512 devices in a mesh: sp: 16 (over z), fs: 4 (over y), tp: 8 (over x, core).
Axes of the slice: x: 4, y: 4, z: 16, core: 2. Of those that a mesh axis runs over, the one named last changes fastest.
Arguments:
- tokens: bfloat16 [4, 16384, 2048], P('fs', ('sp', 'tp')), may hold values from -6 to 6
- input_norm_gain: float32 [2048], replicated, may hold values from 0.1 to 1.9
- earlier_gate: bfloat16 [2048, 1024], P(('sp', 'fs'), 'tp'), may hold values from -0.125 to 0.125
- later_gate: bfloat16 [2048, 1024], P(('sp', 'fs'), 'tp'), may hold values from -0.125 to 0.125
- convolution_input: bfloat16 [2048, 1024], P(('sp', 'fs'), 'tp'), may hold values from -0.125 to 0.125
- convolution_taps: float32 [3, 1024], P(None, 'tp'), may hold values from -3 to 3
- receptance: bfloat16 [2048, 1024], P(('sp', 'fs'), 'tp'), may hold values from -0.125 to 0.125
- key_matrix: bfloat16 [2048, 1024], P(('sp', 'fs'), 'tp'), may hold values from -0.125 to 0.125
- value_matrix: bfloat16 [2048, 1024], P(('sp', 'fs'), 'tp'), may hold values from -0.125 to 0.125
- decay_matrix: bfloat16 [2048, 1024], P(('sp', 'fs'), 'tp'), may hold values from -0.125 to 0.125
- rate_matrix: bfloat16 [2048, 1024], P(('sp', 'fs'), 'tp'), may hold values from -0.125 to 0.125
- decay_floor: float32 [1024], P('tp'), may hold values from -16 to -3.4
- rate_offset: float32 [1024], P('tp'), may hold values from -7.5 to 1
- decay_spike: float32 [4, 16384, 1024], P('fs', 'sp', 'tp'), may hold values from -1.3 to 0
- initial_state: float32 [4, 16, 64, 64], P('fs', 'tp'), may hold values from -768 to 768
- head_norm_gain: float32 [1024], P('tp'), may hold values from 0.1 to 1.9
- convolution_output: bfloat16 [1024, 2048], P('tp', ('sp', 'fs')), may hold values from -0.125 to 0.125
- state_heads_output: bfloat16 [1024, 2048], P('tp', ('sp', 'fs')), may hold values from -0.125 to 0.125
Outputs:
- mixed: bfloat16 [4, 16384, 2048], P('fs', ('sp', 'tp'))
The draws below stay inside these ranges and needn't reach their ends.
All inputs are finite; a program needn't handle non-finite values.
Results may differ from the reference program's by a relative error of at most 0.02.
Values may be sent and summed in bfloat16 or wider, within the bound.
No kernel may reach another device: no remote copies, remote signals or barrier semaphores. Data moves between devices by JAX's collectives and lax.ppermute only.
A program may use at most 64 MiB of HBM per device.

```python
import math
import jax
import jax.numpy as jnp
from jax import lax

D = 2048
HEAD_COUNT = 16
HEAD_WIDTH = 64
KERNEL = 3
TOK_DEV = 1024
SEQUENCE_LENGTH = 16384
SEQS = 4
N_TP = 8


def speed_mask(key, slow_count):
    order = jax.random.permutation(jax.random.fold_in(key, 101), HEAD_COUNT)
    return jnp.repeat(order < slow_count, HEAD_WIDTH)


def draw_decay_floor(key, part):
    slow_count = HEAD_COUNT // 2
    slow_channels = speed_mask(key, slow_count)
    jitter = jax.random.uniform(jax.random.fold_in(key, 102), (HEAD_COUNT * HEAD_WIDTH,), jnp.float32, -0.5, 0.5)
    return jnp.where(slow_channels, math.log(0.1 / SEQUENCE_LENGTH), math.log(0.02)) + jitter


def draw_rate_offset(key, part):
    slow_count = HEAD_COUNT // 2
    slow_channels = speed_mask(key, slow_count)
    slow_values = -7.0 + jax.random.uniform(jax.random.fold_in(key, 103), (HEAD_COUNT * HEAD_WIDTH,), jnp.float32, -0.5, 0.5)
    fast_values = jax.random.uniform(jax.random.fold_in(key, 104), (HEAD_COUNT * HEAD_WIDTH,), jnp.float32, -1.0, 1.0)
    return jnp.where(slow_channels, slow_values, fast_values)


def draw_decay_spike(key, part):
    segments = SEQUENCE_LENGTH // TOK_DEV
    drift = jnp.exp(jax.random.uniform(jax.random.fold_in(key, 105), (SEQS, segments, HEAD_COUNT), jnp.float32, math.log(0.1), math.log(0.6)))
    layer_depth = jax.random.uniform(jax.random.fold_in(key, 107), (SEQS, 2, HEAD_COUNT), jnp.float32, 0.22, 0.6)
    wander_rows = jnp.repeat(-drift / SEQUENCE_LENGTH, TOK_DEV, axis=1)
    spots = jax.random.randint(jax.random.fold_in(key, 106), (SEQS, 2, HEAD_COUNT), 0, SEQUENCE_LENGTH)
    positions = jnp.arange(SEQUENCE_LENGTH, dtype=jnp.int32)[None, :, None, None]
    matches = positions == spots[:, None, :, :]
    spikes = -jnp.sum(jnp.where(matches, layer_depth[:, None, :, :], 0.0), axis=2)
    return jnp.repeat(wander_rows + spikes, HEAD_WIDTH, axis=2).astype(jnp.float32)


def level_of(key, dims, split, smallest, high):
    def one(axis_at, blocks):
        draws = jax.random.uniform(jax.random.fold_in(jax.random.fold_in(key, 6), axis_at), (blocks,), jnp.float32, smallest / len(split), high / len(split))
        return jnp.repeat(jnp.exp(draws), dims[axis_at] // blocks).reshape((-1,) + (1,) * (len(dims) - axis_at - 1))

    factor_of = one(*split[0])
    for cut in split[1:]:
        factor_of = factor_of * one(*cut)
    return factor_of


def bell_draw(key, dims, width, limit, split=(), held_as=jnp.bfloat16):
    loudness = level_of(key, dims, split, -0.22, 0.18) if split else 1.0
    values = jax.random.normal(key, dims, jnp.float32) * width * loudness
    return jnp.minimum(jnp.maximum(values, -limit), limit).astype(held_as)


def setup_inputs(seed: int = 0) -> dict:
    key_of = jax.random.split(jax.random.key(seed), 19)
    return {
        "tokens": bell_draw(key_of[0], (SEQS, SEQUENCE_LENGTH, D), 1.0, 6.0, ((0, 4), (1, 128))),
        "input_norm_gain": jnp.clip(1.0 + 0.18 * jax.random.normal(key_of[1], (D,), jnp.float32), 0.1, 1.9),
        "earlier_gate": bell_draw(key_of[2], (D, HEAD_COUNT * HEAD_WIDTH), D ** -0.5, 0.125, ((0, 64), (1, 8))),
        "later_gate": bell_draw(key_of[3], (D, HEAD_COUNT * HEAD_WIDTH), D ** -0.5, 0.125, ((0, 64), (1, 8))),
        "convolution_input": bell_draw(key_of[4], (D, HEAD_COUNT * HEAD_WIDTH), D ** -0.5, 0.125, ((0, 64), (1, 8))),
        "convolution_taps": bell_draw(key_of[5], (KERNEL, HEAD_COUNT * HEAD_WIDTH), 0.5, 3.0, ((1, 8),), jnp.float32),
        "receptance": bell_draw(key_of[6], (D, HEAD_COUNT * HEAD_WIDTH), D ** -0.5, 0.125, ((0, 64), (1, 8))),
        "key_matrix": bell_draw(key_of[7], (D, HEAD_COUNT * HEAD_WIDTH), D ** -0.5, 0.125, ((0, 64), (1, 8))),
        "value_matrix": bell_draw(key_of[8], (D, HEAD_COUNT * HEAD_WIDTH), D ** -0.5, 0.125, ((0, 64), (1, 8))),
        "decay_matrix": bell_draw(key_of[9], (D, HEAD_COUNT * HEAD_WIDTH), D ** -0.5, 0.125, ((0, 64), (1, 8))),
        "rate_matrix": bell_draw(key_of[10], (D, HEAD_COUNT * HEAD_WIDTH), D ** -0.5, 0.125, ((0, 64), (1, 8))),
        "decay_floor": draw_decay_floor(jax.random.fold_in(key_of[18], 71), 0),
        "rate_offset": draw_rate_offset(jax.random.fold_in(key_of[18], 71), 0),
        "decay_spike": draw_decay_spike(jax.random.fold_in(key_of[18], 71), 0),
        "initial_state": bell_draw(key_of[14], (SEQS, HEAD_COUNT, HEAD_WIDTH, HEAD_WIDTH), (SEQUENCE_LENGTH ** 0.5), 768.0, ((0, 4), (1, 8)), jnp.float32),
        "head_norm_gain": jnp.clip(1.0 + 0.18 * jax.random.normal(key_of[15], (HEAD_COUNT * HEAD_WIDTH,), jnp.float32), 0.1, 1.9),
        "convolution_output": bell_draw(key_of[16], (HEAD_COUNT * HEAD_WIDTH, D), (2 * HEAD_COUNT * HEAD_WIDTH) ** -0.5, 0.125, ((0, 8), (1, 64))),
        "state_heads_output": bell_draw(key_of[17], (HEAD_COUNT * HEAD_WIDTH, D), (2 * HEAD_COUNT * HEAD_WIDTH) ** -0.5, 0.125, ((0, 8), (1, 64))),
    }


norm_eps = 1e-06
key_eps = 1e-06
highest = lax.Precision.HIGHEST

def rms_rows(activations, gain_vector):
    values = activations.astype(jnp.float32)
    inv_scale = lax.rsqrt(lax.optimization_barrier(jnp.mean(values * values, axis=-1, keepdims=True)) + norm_eps)
    return (values * inv_scale * gain_vector).astype(jnp.bfloat16)

def project(activations, weight):
    return jnp.dot(activations, weight, preferred_element_type=jnp.float32).astype(jnp.bfloat16)

def recur(state, inputs):
    queries, key_rows, value_rows, unit_keys, beta_rows, log_rows = inputs
    removed = jnp.einsum('hvk,hk->hv', state, unit_keys, precision=highest)
    state = state * jnp.exp(log_rows)[:, None, :] - removed[:, :, None] * beta_rows[:, None, :] + value_rows[:, :, None] * key_rows[:, None, :]
    return (state, jnp.einsum('hvk,hk->hv', state, queries, precision=highest))

def single_sequence(token_sequence, spike_rows, opening_state, weight_set):
    input_norm_gain, earlier_gate, later_gate, convolution_input, convolution_taps, receptance, key_matrix, value_matrix, decay_matrix, rate_matrix, decay_floor, rate_offset, head_norm_gain, convolution_output, state_heads_output = weight_set
    normed = rms_rows(token_sequence, input_norm_gain)
    product = project(normed, earlier_gate).astype(jnp.float32) * project(normed, convolution_input).astype(jnp.float32)
    padded = jnp.concatenate([jnp.zeros((KERNEL - 1, product.shape[1]), jnp.float32), product], axis=0)
    filtered = jnp.zeros_like(product)
    for offset in range(KERNEL):
        filtered = filtered + convolution_taps[offset] * padded[offset:offset + SEQUENCE_LENGTH]
    conv_mixed = (project(normed, later_gate).astype(jnp.float32) * filtered).astype(jnp.bfloat16)

    def by_heads(array):
        return array.astype(jnp.float32).reshape(SEQUENCE_LENGTH, HEAD_COUNT, HEAD_WIDTH)
    queries = by_heads(project(normed, receptance))
    key_rows = by_heads(project(normed, key_matrix))
    value_rows = by_heads(project(normed, value_matrix))
    logarithm_decay = -jnp.exp(decay_floor.reshape(HEAD_COUNT, HEAD_WIDTH) + jnp.tanh(by_heads(project(normed, decay_matrix))))
    logarithm_decay = logarithm_decay + spike_rows.reshape(SEQUENCE_LENGTH, HEAD_COUNT, HEAD_WIDTH)
    learn_rate = jax.nn.sigmoid(rate_offset.reshape(HEAD_COUNT, HEAD_WIDTH) + by_heads(project(normed, rate_matrix)))
    unit_keys = key_rows * lax.rsqrt(lax.optimization_barrier(jnp.sum(key_rows * key_rows, axis=-1, keepdims=True)) + key_eps)
    beta_rows = learn_rate * unit_keys
    final_state, reads = lax.scan(recur, opening_state, (queries, key_rows, value_rows, unit_keys, beta_rows, logarithm_decay))
    centered = reads - lax.optimization_barrier(jnp.mean(reads, axis=-1, keepdims=True))
    variance = lax.optimization_barrier(jnp.mean(centered * centered, axis=-1, keepdims=True))
    state_mixed = centered * lax.rsqrt(variance + HEAD_WIDTH * 1e-05) * head_norm_gain.reshape(HEAD_COUNT, HEAD_WIDTH)
    state_mixed = state_mixed.reshape(SEQUENCE_LENGTH, HEAD_COUNT * HEAD_WIDTH).astype(jnp.bfloat16)
    group_width = HEAD_COUNT * HEAD_WIDTH // N_TP
    summed = jnp.zeros((SEQUENCE_LENGTH, D), jnp.float32)
    for member in range(N_TP):
        column_start = member * group_width
        column_end = column_start + group_width
        partial_value = jnp.dot(conv_mixed[:, column_start:column_end], convolution_output[column_start:column_end], preferred_element_type=jnp.float32)
        partial_value = partial_value + jnp.dot(state_mixed[:, column_start:column_end], state_heads_output[column_start:column_end], preferred_element_type=jnp.float32)
        summed = summed + lax.optimization_barrier(partial_value.astype(jnp.bfloat16)).astype(jnp.float32)
    return summed.astype(jnp.bfloat16)

def reference(tokens, input_norm_gain, earlier_gate, later_gate, convolution_input, convolution_taps, receptance, key_matrix, value_matrix, decay_matrix, rate_matrix, decay_floor, rate_offset, decay_spike, initial_state, head_norm_gain, convolution_output, state_heads_output):
    weight_set = (input_norm_gain, earlier_gate, later_gate, convolution_input, convolution_taps, receptance, key_matrix, value_matrix, decay_matrix, rate_matrix, decay_floor, rate_offset, head_norm_gain, convolution_output, state_heads_output)

    def apply_single(inputs):
        return single_sequence(inputs[0], inputs[1], inputs[2], weight_set)
    return lax.map(apply_single, (tokens, decay_spike, initial_state))
```

```python
import functools

import jax
import jax.numpy as jnp
from jax import lax
from jax.experimental import pallas as pl
from jax.experimental.pallas import tpu as pltpu
from jax.sharding import PartitionSpec as P

HEAD_WIDTH = 64
CHUNK = 64
BLOCK = 256
norm_eps = 1e-06
key_eps = 1e-06
f32, bf16 = jnp.float32, jnp.bfloat16


def dot(a, b, ca=1, cb=0):
    return lax.dot_general(
        a.astype(bf16), b.astype(bf16), (((ca,), (cb,)), ((), ())), preferred_element_type=f32
    )


def lanes_of(shape):
    return lax.broadcasted_iota(jnp.int32, shape, 1)


def rows_of(shape):
    return lax.broadcasted_iota(jnp.int32, shape, 0)


def spread(z, first):
    z = z.astype(bf16)
    return jnp.concatenate([z * first, z * (1 - first)], axis=0)


def head_sums(z, low):
    a = jnp.sum(jnp.where(low, z, 0.0), axis=1, keepdims=True)
    b = jnp.sum(jnp.where(low, 0.0, z), axis=1, keepdims=True)
    return jnp.where(low, a, b)


def local_kernel(x_ref, w_ref, spike_ref, vec_ref, conv_ref, o_ref, y_ref, agg_ref, edge_ref, st_ref, tail_ref):
    step = pl.program_id(0)
    width = 2 * HEAD_WIDTH
    pairs = BLOCK // CHUNK

    @pl.when(step == 0)
    def _():
        r, l = rows_of((width, width)), lanes_of((width, width))
        eye = (r - HEAD_WIDTH == l % HEAD_WIDTH) & (r >= HEAD_WIDTH)
        st_ref[...] = jnp.where(eye, 1.0, 0.0).astype(f32)
        tail_ref[...] = jnp.zeros_like(tail_ref)

    x = x_ref[...]

    def section(k):
        two = jnp.dot(x, w_ref[:, 2 * k * width : 2 * (k + 1) * width], preferred_element_type=f32)
        two = two.astype(bf16).astype(f32)
        return two[:, :width], two[:, width:]

    pre, post = section(0)
    cvals, q = section(1)
    keys, vals = section(2)
    dpre, rpre = section(3)

    prod = pre * cvals
    tail = tail_ref[...]
    row = rows_of((BLOCK, width))
    last, before = tail[7:8], tail[6:7]
    one = jnp.where(row == 0, last, pltpu.roll(prod, 1, 0))
    two = jnp.where(row == 0, before, jnp.where(row == 1, last, pltpu.roll(prod, 2, 0)))
    filtered = vec_ref[2:3] * two + vec_ref[3:4] * one + vec_ref[4:5] * prod
    conv_ref[...] = (post * filtered).astype(bf16)
    tail_ref[...] = prod[BLOCK - 8 :]

    @pl.when(step == 0)
    def _():
        edge_ref[0:8] = prod[:8]
        edge_ref[8:16] = post[:8]

    @pl.when(step == pl.num_programs(0) - 1)
    def _():
        edge_ref[16:24] = prod[BLOCK - 8 :]

    low = lanes_of((BLOCK, width)) < HEAD_WIDTH
    logd = spike_ref[...] - jnp.exp(vec_ref[0:1] + jnp.tanh(dpre))
    rate = jax.nn.sigmoid(vec_ref[1:2] + rpre)
    unit = keys * lax.rsqrt(head_sums(keys * keys, low) + key_eps)
    beta = rate * unit
    r, c = rows_of((BLOCK, BLOCK)), lanes_of((BLOCK, BLOCK))
    tri = jnp.where((r >= c) & (r // CHUNK == c // CHUNK), 1.0, 0.0).astype(bf16)
    hi = logd.astype(bf16)
    rest = logd - hi.astype(f32)
    mid = rest.astype(bf16)
    lo = (rest - mid.astype(f32)).astype(bf16)
    sums = jnp.dot(tri, jnp.concatenate([hi, mid, lo], axis=1), preferred_element_type=f32)
    cum_all = sums[:, :width] + sums[:, width : 2 * width] + sums[:, 2 * width :]
    prev_all = cum_all - logd

    shape = (CHUNK, width)
    t, s = rows_of(shape), lanes_of(shape) % HEAD_WIDTH
    strict, inclusive = t > s, t >= s
    low_c = lanes_of(shape) < HEAD_WIDTH
    first = jnp.where(lanes_of((1, width)) < HEAD_WIDTH, 1.0, 0.0).astype(bf16)
    fold = functools.partial(spread, first=first)
    same = (rows_of((width, width)) // HEAD_WIDTH) == (lanes_of((width, width)) // HEAD_WIDTH)
    each = range(pairs)

    def part(a):
        return [a[k * CHUNK : (k + 1) * CHUNK] for k in each]

    q, keys, vals, unit, beta = map(part, (q, keys, vals, unit, beta))
    cum, prev = part(cum_all), part(prev_all)
    center = [cum[k][CHUNK // 2 : CHUNK // 2 + 1] for k in each]
    close = [cum[k][CHUNK - 1 : CHUNK] for k in each]
    e_neg = [jnp.exp(center[k] - cum[k]) for k in each]
    ask_k = [unit[k] * jnp.exp(prev[k] - center[k]) for k in each]
    ask_q = [q[k] * jnp.exp(cum[k] - center[k]) for k in each]
    give_k = [keys[k] * e_neg[k] for k in each]
    give_b = [beta[k] * e_neg[k] for k in each]
    e_center = [jnp.exp(center[k]) for k in each]
    e_tail = [jnp.exp(close[k] - center[k]) for k in each]
    e_close = [jnp.exp(close[k]) for k in each]
    grams = [
        dot(
            jnp.concatenate([ask_k[k], ask_q[k]], axis=0),
            jnp.concatenate([fold(give_k[k]), fold(give_b[k])], axis=0),
            1,
            1,
        )
        for k in each
    ]
    key_ask = [jnp.where(strict, g[:CHUNK, :width], 0.0) for g in grams]
    beta_ask = [jnp.where(strict, g[:CHUNK, width:], 0.0) for g in grams]
    key_read = [jnp.where(inclusive, g[CHUNK:, :width], 0.0) for g in grams]
    beta_read = [jnp.where(inclusive, g[CHUNK:, width:], 0.0) for g in grams]
    both_v = [dot(jnp.concatenate([key_ask[k], key_read[k]], axis=0), fold(vals[k])) for k in each]

    inv = [jnp.where(t == s, 1.0, jnp.where(t // 2 == s // 2, -beta_ask[k], 0.0)) for k in each]
    size = 2
    while size < CHUNK:
        here = (t // (2 * size) == s // (2 * size)) & (t // size != s // size)
        mixed = [dot(inv[k], fold(jnp.where(here, beta_ask[k], 0.0))) for k in each]
        inv = [inv[k] - dot(mixed[k], fold(inv[k])) for k in each]
        size *= 2

    wu = [
        dot(
            inv[k],
            jnp.concatenate([fold(ask_k[k] * e_center[k]), fold(both_v[k][:CHUNK])], axis=1),
        )
        for k in each
    ]
    back = [
        dot(
            beta_read[k],
            jnp.concatenate([fold(wu[k][:, :width]), fold(wu[k][:, width:])], axis=1),
        )
        for k in each
    ]
    q_eff = [ask_q[k] * e_center[k] - back[k][:, :width] for k in each]
    o_loc = [both_v[k][CHUNK:] - back[k][:, width:] for k in each]
    outer = [dot(wu[k], give_b[k] * e_tail[k], 0, 0) for k in each]
    outer_v = [dot(vals[k], give_k[k] * e_tail[k], 0, 0) for k in each]
    step_map = [jnp.where(same, -outer[k][:width], 0.0).astype(bf16) for k in each]
    source_full = [outer_v[k] - outer[k][width:] for k in each]
    source = [jnp.where(low_c, f[:HEAD_WIDTH], f[HEAD_WIDTH:]) for f in source_full]

    state = st_ref[...]
    for k in each:
        got = dot(
            q_eff[k],
            jnp.concatenate([fold(state[:HEAD_WIDTH]), fold(state[HEAD_WIDTH:])], axis=0),
            1,
            1,
        )
        o_ref[k * CHUNK : (k + 1) * CHUNK] = o_loc[k] + got[:, :width]
        y_ref[k * CHUNK : (k + 1) * CHUNK] = got[:, width:].astype(bf16)
        state = state * e_close[k] + dot(state, step_map[k])
        state = jnp.concatenate([state[:HEAD_WIDTH] + source[k], state[HEAD_WIDTH:]], axis=0)
    st_ref[...] = state

    @pl.when(step == pl.num_programs(0) - 1)
    def _():
        agg_ref[...] = state.astype(bf16)


def local_call(x, w, spike, vec):
    rows, depth = x.shape
    width = 2 * HEAD_WIDTH
    whole = lambda *shape: pl.BlockSpec(shape, lambda i: (0,) * len(shape))
    tile = pl.BlockSpec((BLOCK, width), lambda i: (i, 0))
    return pl.pallas_call(
        local_kernel,
        grid=(rows // BLOCK,),
        in_specs=[
            pl.BlockSpec((BLOCK, depth), lambda i: (i, 0)),
            pl.BlockSpec((depth, 8 * width), lambda i: (0, 0)),
            tile,
            whole(8, width),
        ],
        out_specs=[tile, tile, tile, whole(width, width), whole(24, width)],
        out_shape=[
            jax.ShapeDtypeStruct((rows, width), bf16),
            jax.ShapeDtypeStruct((rows, width), f32),
            jax.ShapeDtypeStruct((rows, width), bf16),
            jax.ShapeDtypeStruct((width, width), bf16),
            jax.ShapeDtypeStruct((24, width), f32),
        ],
        scratch_shapes=[pltpu.VMEM((width, width), f32), pltpu.VMEM((8, width), f32)],
        compiler_params=pltpu.CompilerParams(
            dimension_semantics=("arbitrary",), vmem_limit_bytes=50 * 2**20
        ),
        name="local_mix",
    )(x, w, spike, vec)


def finish_kernel(pos_ref, agg_ref, init_ref, o_ref, y_ref, conv_ref, edge_ref, prior_ref, vec_ref, w_ref, out_ref, s_ref):
    step = pl.program_id(0)
    width = 2 * HEAD_WIDTH
    first = jnp.where(lanes_of((1, width)) < HEAD_WIDTH, 1.0, 0.0).astype(bf16)

    @pl.when(step == 0)
    def _():
        def advance(i, state):
            piece = agg_ref[i]
            hi = state.astype(bf16)
            lo = (state - hi.astype(f32)).astype(bf16)
            got = dot(jnp.concatenate([hi, lo], axis=0), spread(piece[HEAD_WIDTH:], first))
            return got[:HEAD_WIDTH] + got[HEAD_WIDTH:] + piece[:HEAD_WIDTH].astype(f32)

        state = lax.fori_loop(0, pos_ref[0], advance, init_ref[...])
        s_ref[...] = spread(state, first)

    low = lanes_of((BLOCK, width)) < HEAD_WIDTH
    reads = o_ref[...] + dot(y_ref[...], s_ref[...], 1, 1)
    centered = reads - head_sums(reads, low) * (1.0 / HEAD_WIDTH)
    variance = head_sums(centered * centered, low) * (1.0 / HEAD_WIDTH)
    mixed = centered * lax.rsqrt(variance + HEAD_WIDTH * 1e-05) * vec_ref[5:6]

    prod, post = edge_ref[0:8], edge_ref[8:16]
    last, before = prior_ref[1:2], prior_ref[0:1]
    row = rows_of((8, width))
    one = jnp.where(row == 0, last, pltpu.roll(prod, 1, 0))
    two = jnp.where(row == 0, before, jnp.where(row == 1, last, pltpu.roll(prod, 2, 0)))
    fixed = post * (vec_ref[2:3] * two + vec_ref[3:4] * one + vec_ref[4:5] * prod)
    conv = conv_ref[...]
    head = jnp.where((step == 0) & (rows_of((16, width)) < 2), jnp.concatenate([fixed, fixed], axis=0), conv[:16].astype(f32))
    conv = jnp.concatenate([head.astype(bf16), conv[16:]], axis=0)
    both = jnp.concatenate([conv, mixed.astype(bf16)], axis=1)
    out_ref[...] = dot(both, w_ref[...], 1, 1).astype(bf16)


def finish_call(pos, agg, init, o, y, conv, edge, prior, vec, w):
    rows, width = o.shape
    whole = lambda a: pl.BlockSpec(a.shape, lambda i, p: (0,) * a.ndim)
    tile = pl.BlockSpec((BLOCK, width), lambda i, p: (i, 0))
    return pl.pallas_call(
        finish_kernel,
        grid_spec=pltpu.PrefetchScalarGridSpec(
            num_scalar_prefetch=1,
            grid=(rows // BLOCK,),
            in_specs=[
                whole(agg), whole(init), tile, tile, tile, whole(edge), whole(prior), whole(vec),
                pl.BlockSpec((w.shape[0], 2 * width), lambda i, p: (0, 4)),
            ],
            out_specs=pl.BlockSpec((BLOCK, w.shape[0]), lambda i, p: (i, 0)),
            scratch_shapes=[pltpu.VMEM((width, width), bf16)],
        ),
        out_shape=jax.ShapeDtypeStruct((rows, w.shape[0]), bf16),
        compiler_params=pltpu.CompilerParams(
            dimension_semantics=("arbitrary",), vmem_limit_bytes=50 * 2**20
        ),
        name="finish_mix",
    )(pos, agg, init, o, y, conv, edge, prior, vec, w)


def pack_kernel(*refs):
    *parts, out_ref = refs
    for k, ref in enumerate(parts):
        piece = ref[...]
        if piece.shape[0] > piece.shape[1]:
            piece = piece.astype(f32).T.astype(bf16)
        out_ref[:, k * 128 : (k + 1) * 128] = piece


def packed(*shards):
    rows, width = shards[0].shape
    return pl.pallas_call(
        pack_kernel,
        out_shape=jax.ShapeDtypeStruct((rows, len(shards) * width), bf16),
        name="pack_shards",
    )(*shards)


def passed_along(block, axis, distance):
    devices = range(lax.axis_size(axis))
    route = [(i - distance, i) for i in devices if i - distance in devices]
    return lax.ppermute(block, axis, route)


def from_everyone(x, axis):
    devices = lax.axis_size(axis)
    return lax.all_to_all(jnp.broadcast_to(x[None], (devices, *x.shape)), axis, 0, 0, tiled=True)


def rms_rows(activations, gain_vector):
    values = activations.astype(f32)
    inv_scale = lax.rsqrt(jnp.mean(values * values, axis=-1, keepdims=True) + norm_eps)
    return (values * inv_scale * gain_vector).astype(bf16)


def on_device(
    tokens,
    input_norm_gain,
    earlier_gate,
    later_gate,
    convolution_input,
    convolution_taps,
    receptance,
    key_matrix,
    value_matrix,
    decay_matrix,
    rate_matrix,
    decay_floor,
    rate_offset,
    decay_spike,
    initial_state,
    head_norm_gain,
    convolution_output,
    state_heads_output,
):
    normed = rms_rows(tokens[0], input_norm_gain)
    channels = earlier_gate.shape[1]
    heads = channels // HEAD_WIDTH
    both = packed(
        earlier_gate,
        later_gate,
        convolution_input,
        receptance,
        key_matrix,
        value_matrix,
        decay_matrix,
        rate_matrix,
        convolution_output,
        state_heads_output,
    )
    weights = lax.all_gather(both, "fs", axis=0, tiled=True)
    weights = lax.all_gather(weights, "sp", axis=0, tiled=True)
    piece = from_everyone(normed, "tp").reshape(-1, normed.shape[1])
    vec = jnp.concatenate(
        [
            decay_floor[None],
            rate_offset[None],
            convolution_taps,
            head_norm_gain[None],
            jnp.zeros((2, channels), f32),
        ],
        axis=0,
    )
    conv, o, y, agg, edge = local_call(piece, weights, decay_spike[0], vec)
    pieces = from_everyone(agg, "sp")
    prior = passed_along(edge[22:24], "sp", 1)
    init = jnp.moveaxis(initial_state[0], 0, 1).reshape(HEAD_WIDTH, heads * HEAD_WIDTH)
    pos = lax.axis_index("sp").astype(jnp.int32)[None]
    partial = finish_call(pos, pieces, init, o, y, conv, edge, prior, vec, weights)
    mixed = lax.psum_scatter(partial, "tp", scatter_dimension=0, tiled=True)
    return mixed[None]


def solution(mesh):
    placed = (
        P("fs", ("sp", "tp"), None),
        P(),
        P(("sp", "fs"), "tp"),
        P(("sp", "fs"), "tp"),
        P(("sp", "fs"), "tp"),
        P(None, "tp"),
        P(("sp", "fs"), "tp"),
        P(("sp", "fs"), "tp"),
        P(("sp", "fs"), "tp"),
        P(("sp", "fs"), "tp"),
        P(("sp", "fs"), "tp"),
        P("tp"),
        P("tp"),
        P("fs", "sp", "tp"),
        P("fs", "tp", None, None),
        P("tp"),
        P("tp", ("sp", "fs")),
        P("tp", ("sp", "fs")),
    )
    return jax.shard_map(
        on_device,
        mesh=mesh,
        in_specs=placed,
        out_specs=P("fs", ("sp", "tp"), None),
        check_vma=False,
    )
```

```python
import functools

import jax
import jax.numpy as jnp
from jax import lax
from jax.experimental import pallas as pl
from jax.experimental.pallas import tpu as pltpu
from jax.sharding import PartitionSpec as P


HEAD_WIDTH = 64
CHUNK = 64
BLOCK = 256
norm_eps = 1e-06
key_eps = 1e-06
f32, bf16 = jnp.float32, jnp.bfloat16


def dot(a, b, ca=1, cb=0):
    return lax.dot_general(
        a.astype(bf16), b.astype(bf16), (((ca,), (cb,)), ((), ())), preferred_element_type=f32
    )


def lanes_of(shape):
    return lax.broadcasted_iota(jnp.int32, shape, 1)


def rows_of(shape):
    return lax.broadcasted_iota(jnp.int32, shape, 0)


def spread(z, first):
    z = z.astype(bf16)
    return jnp.concatenate([z * first, z * (1 - first)], axis=0)


def head_sums(z, low):
    a = jnp.sum(jnp.where(low, z, 0.0), axis=1, keepdims=True)
    b = jnp.sum(jnp.where(low, 0.0, z), axis=1, keepdims=True)
    return jnp.where(low, a, b)


def local_kernel(x_ref, w_ref, spike_ref, vec_ref, conv_ref, o_ref, y_ref, agg_ref, edge_ref, st_ref, tail_ref):
    step = pl.program_id(0)
    width = 2 * HEAD_WIDTH
    pairs = BLOCK // CHUNK

    @pl.when(step == 0)
    def _():
        r, l = rows_of((width, width)), lanes_of((width, width))
        eye = (r - HEAD_WIDTH == l % HEAD_WIDTH) & (r >= HEAD_WIDTH)
        st_ref[...] = jnp.where(eye, 1.0, 0.0).astype(f32)
        tail_ref[...] = jnp.zeros_like(tail_ref)

    x = x_ref[...]

    def section(k):
        two = jnp.dot(x, w_ref[:, 2 * k * width : 2 * (k + 1) * width], preferred_element_type=f32)
        two = two.astype(bf16).astype(f32)
        return two[:, :width], two[:, width:]

    pre, post = section(0)
    cvals, q = section(1)
    keys, vals = section(2)
    dpre, rpre = section(3)

    prod = pre * cvals
    tail = tail_ref[...]
    row = rows_of((BLOCK, width))
    last, before = tail[7:8], tail[6:7]
    one = jnp.where(row == 0, last, pltpu.roll(prod, 1, 0))
    two = jnp.where(row == 0, before, jnp.where(row == 1, last, pltpu.roll(prod, 2, 0)))
    filtered = vec_ref[2:3] * two + vec_ref[3:4] * one + vec_ref[4:5] * prod
    conv_ref[...] = (post * filtered).astype(bf16)
    tail_ref[...] = prod[BLOCK - 8 :]

    @pl.when(step == 0)
    def _():
        edge_ref[0:8] = prod[:8]
        edge_ref[8:16] = post[:8]

    @pl.when(step == pl.num_programs(0) - 1)
    def _():
        edge_ref[16:24] = prod[BLOCK - 8 :]

    low = lanes_of((BLOCK, width)) < HEAD_WIDTH
    logd = spike_ref[...] - jnp.exp(vec_ref[0:1] + jnp.tanh(dpre))
    rate = jax.nn.sigmoid(vec_ref[1:2] + rpre)
    unit = keys * lax.rsqrt(head_sums(keys * keys, low) + key_eps)
    beta = rate * unit
    r, c = rows_of((BLOCK, BLOCK)), lanes_of((BLOCK, BLOCK))
    tri = jnp.where((r >= c) & (r // CHUNK == c // CHUNK), 1.0, 0.0).astype(bf16)
    hi = logd.astype(bf16)
    rest = logd - hi.astype(f32)
    mid = rest.astype(bf16)
    lo = (rest - mid.astype(f32)).astype(bf16)
    sums = jnp.dot(tri, jnp.concatenate([hi, mid, lo], axis=1), preferred_element_type=f32)
    cum_all = sums[:, :width] + sums[:, width : 2 * width] + sums[:, 2 * width :]
    prev_all = cum_all - logd

    shape = (CHUNK, width)
    t, s = rows_of(shape), lanes_of(shape) % HEAD_WIDTH
    strict, inclusive = t > s, t >= s
    low_c = lanes_of(shape) < HEAD_WIDTH
    first = jnp.where(lanes_of((1, width)) < HEAD_WIDTH, 1.0, 0.0).astype(bf16)
    fold = functools.partial(spread, first=first)
    same = (rows_of((width, width)) // HEAD_WIDTH) == (lanes_of((width, width)) // HEAD_WIDTH)
    each = range(pairs)

    def part(a):
        return [a[k * CHUNK : (k + 1) * CHUNK] for k in each]

    q, keys, vals, unit, beta = map(part, (q, keys, vals, unit, beta))
    cum, prev = part(cum_all), part(prev_all)
    center = [cum[k][CHUNK // 2 : CHUNK // 2 + 1] for k in each]
    close = [cum[k][CHUNK - 1 : CHUNK] for k in each]
    e_neg = [jnp.exp(center[k] - cum[k]) for k in each]
    ask_k = [unit[k] * jnp.exp(prev[k] - center[k]) for k in each]
    ask_q = [q[k] * jnp.exp(cum[k] - center[k]) for k in each]
    give_k = [keys[k] * e_neg[k] for k in each]
    give_b = [beta[k] * e_neg[k] for k in each]
    e_center = [jnp.exp(center[k]) for k in each]
    e_tail = [jnp.exp(close[k] - center[k]) for k in each]
    e_close = [jnp.exp(close[k]) for k in each]
    grams = [
        dot(
            jnp.concatenate([ask_k[k], ask_q[k]], axis=0),
            jnp.concatenate([fold(give_k[k]), fold(give_b[k])], axis=0),
            1,
            1,
        )
        for k in each
    ]
    key_ask = [jnp.where(strict, g[:CHUNK, :width], 0.0) for g in grams]
    beta_ask = [jnp.where(strict, g[:CHUNK, width:], 0.0) for g in grams]
    key_read = [jnp.where(inclusive, g[CHUNK:, :width], 0.0) for g in grams]
    beta_read = [jnp.where(inclusive, g[CHUNK:, width:], 0.0) for g in grams]
    both_v = [dot(jnp.concatenate([key_ask[k], key_read[k]], axis=0), fold(vals[k])) for k in each]

    inv = [jnp.where(t == s, 1.0, jnp.where(t // 2 == s // 2, -beta_ask[k], 0.0)) for k in each]
    size = 2
    while size < CHUNK:
        here = (t // (2 * size) == s // (2 * size)) & (t // size != s // size)
        mixed = [dot(inv[k], fold(jnp.where(here, beta_ask[k], 0.0))) for k in each]
        inv = [inv[k] - dot(mixed[k], fold(inv[k])) for k in each]
        size *= 2

    wu = [
        dot(
            inv[k],
            jnp.concatenate([fold(ask_k[k] * e_center[k]), fold(both_v[k][:CHUNK])], axis=1),
        )
        for k in each
    ]
    back = [
        dot(
            beta_read[k],
            jnp.concatenate([fold(wu[k][:, :width]), fold(wu[k][:, width:])], axis=1),
        )
        for k in each
    ]
    q_eff = [ask_q[k] * e_center[k] - back[k][:, :width] for k in each]
    o_loc = [both_v[k][CHUNK:] - back[k][:, width:] for k in each]
    outer = [dot(wu[k], give_b[k] * e_tail[k], 0, 0) for k in each]
    outer_v = [dot(vals[k], give_k[k] * e_tail[k], 0, 0) for k in each]
    step_map = [jnp.where(same, -outer[k][:width], 0.0).astype(bf16) for k in each]
    source_full = [outer_v[k] - outer[k][width:] for k in each]
    source = [jnp.where(low_c, f[:HEAD_WIDTH], f[HEAD_WIDTH:]) for f in source_full]

    state = st_ref[...]
    for k in each:
        got = dot(
            q_eff[k],
            jnp.concatenate([fold(state[:HEAD_WIDTH]), fold(state[HEAD_WIDTH:])], axis=0),
            1,
            1,
        )
        o_ref[k * CHUNK : (k + 1) * CHUNK] = o_loc[k] + got[:, :width]
        y_ref[k * CHUNK : (k + 1) * CHUNK] = got[:, width:].astype(bf16)
        state = state * e_close[k] + dot(state, step_map[k])
        state = jnp.concatenate([state[:HEAD_WIDTH] + source[k], state[HEAD_WIDTH:]], axis=0)
    st_ref[...] = state

    @pl.when(step == pl.num_programs(0) - 1)
    def _():
        agg_ref[...] = state.astype(bf16)


def local_call(x, w, spike, vec):
    rows, depth = x.shape
    width = 2 * HEAD_WIDTH
    whole = lambda *shape: pl.BlockSpec(shape, lambda i: (0,) * len(shape))
    tile = pl.BlockSpec((BLOCK, width), lambda i: (i, 0))
    return pl.pallas_call(
        local_kernel,
        grid=(rows // BLOCK,),
        in_specs=[
            pl.BlockSpec((BLOCK, depth), lambda i: (i, 0)),
            pl.BlockSpec((depth, 8 * width), lambda i: (0, 0)),
            tile,
            whole(8, width),
        ],
        out_specs=[tile, tile, tile, whole(width, width), whole(24, width)],
        out_shape=[
            jax.ShapeDtypeStruct((rows, width), bf16),
            jax.ShapeDtypeStruct((rows, width), f32),
            jax.ShapeDtypeStruct((rows, width), bf16),
            jax.ShapeDtypeStruct((width, width), bf16),
            jax.ShapeDtypeStruct((24, width), f32),
        ],
        scratch_shapes=[pltpu.VMEM((width, width), f32), pltpu.VMEM((8, width), f32)],
        compiler_params=pltpu.CompilerParams(
            dimension_semantics=("arbitrary",), vmem_limit_bytes=50 * 2**20
        ),
        name="local_mix",
    )(x, w, spike, vec)


def finish_kernel(pos_ref, agg_ref, init_ref, o_ref, y_ref, conv_ref, edge_ref, prior_ref, vec_ref, out_ref, s_ref):
    step = pl.program_id(0)
    width = 2 * HEAD_WIDTH
    first = jnp.where(lanes_of((1, width)) < HEAD_WIDTH, 1.0, 0.0).astype(bf16)

    @pl.when(step == 0)
    def _():
        def advance(i, state):
            piece = agg_ref[i]
            hi = state.astype(bf16)
            lo = (state - hi.astype(f32)).astype(bf16)
            got = dot(jnp.concatenate([hi, lo], axis=0), spread(piece[HEAD_WIDTH:], first))
            return got[:HEAD_WIDTH] + got[HEAD_WIDTH:] + piece[:HEAD_WIDTH].astype(f32)

        state = lax.fori_loop(0, pos_ref[0], advance, init_ref[...])
        s_ref[...] = spread(state, first)

    low = lanes_of((BLOCK, width)) < HEAD_WIDTH
    reads = o_ref[...] + dot(y_ref[...], s_ref[...], 1, 1)
    centered = reads - head_sums(reads, low) * (1.0 / HEAD_WIDTH)
    variance = head_sums(centered * centered, low) * (1.0 / HEAD_WIDTH)
    mixed = centered * lax.rsqrt(variance + HEAD_WIDTH * 1e-05) * vec_ref[5:6]

    prod, post = edge_ref[0:8], edge_ref[8:16]
    last, before = prior_ref[1:2], prior_ref[0:1]
    row = rows_of((8, width))
    one = jnp.where(row == 0, last, pltpu.roll(prod, 1, 0))
    two = jnp.where(row == 0, before, jnp.where(row == 1, last, pltpu.roll(prod, 2, 0)))
    fixed = post * (vec_ref[2:3] * two + vec_ref[3:4] * one + vec_ref[4:5] * prod)
    conv = conv_ref[...]
    head = jnp.where((step == 0) & (rows_of((16, width)) < 2), jnp.concatenate([fixed, fixed], axis=0), conv[:16].astype(f32))
    conv = jnp.concatenate([head.astype(bf16), conv[16:]], axis=0)
    out_ref[:, :width] = conv
    out_ref[:, width:] = mixed.astype(bf16)


def finish_call(pos, agg, init, o, y, conv, edge, prior, vec):
    rows, width = o.shape
    whole = lambda a: pl.BlockSpec(a.shape, lambda i, p: (0,) * a.ndim)
    tile = pl.BlockSpec((BLOCK, width), lambda i, p: (i, 0))
    return pl.pallas_call(
        finish_kernel,
        grid_spec=pltpu.PrefetchScalarGridSpec(
            num_scalar_prefetch=1,
            grid=(rows // BLOCK,),
            in_specs=[whole(agg), whole(init), tile, tile, tile, whole(edge), whole(prior), whole(vec)],
            out_specs=pl.BlockSpec((BLOCK, 2 * width), lambda i, p: (i, 0)),
            scratch_shapes=[pltpu.VMEM((width, width), bf16)],
        ),
        out_shape=jax.ShapeDtypeStruct((rows, 2 * width), bf16),
        compiler_params=pltpu.CompilerParams(
            dimension_semantics=("arbitrary",), vmem_limit_bytes=50 * 2**20
        ),
        name="finish_mix",
    )(pos, agg, init, o, y, conv, edge, prior, vec)


def outward_kernel(pick_ref, m_ref, *refs):
    *weights, out_ref = refs
    rows = out_ref.shape[0]
    at = pl.multiple_of(pick_ref[0], rows)
    total = None
    for k, w_ref in enumerate(weights):
        got = dot(m_ref[pick_ref[1 + k], pl.ds(at, rows), :], w_ref[...], 1, 1)
        total = got if total is None else total + got
    out_ref[...] = total.astype(out_ref.dtype)


def outward_call(pick, gathered, weights, dtype):
    _, rows, depth = gathered.shape
    columns = weights[0].shape[0]
    step = 512
    return pl.pallas_call(
        outward_kernel,
        grid_spec=pltpu.PrefetchScalarGridSpec(
            num_scalar_prefetch=1,
            grid=(columns // step,),
            in_specs=[pl.BlockSpec(gathered.shape, lambda i, p: (0, 0, 0))]
            + [pl.BlockSpec((step, depth), lambda i, p: (i, 0)) for _ in weights],
            out_specs=pl.BlockSpec((rows // 2, step), lambda i, p: (0, i)),
        ),
        out_shape=jax.ShapeDtypeStruct((rows // 2, columns), dtype),
        compiler_params=pltpu.CompilerParams(dimension_semantics=("arbitrary",)),
        name="outward",
    )(pick, gathered, *weights)


def pack_kernel(*refs):
    *parts, out_ref = refs
    for k, ref in enumerate(parts):
        width = ref.shape[1]
        out_ref[:, k * width : (k + 1) * width] = ref[...]


def packed(*shards):
    rows, width = shards[0].shape
    return pl.pallas_call(
        pack_kernel,
        out_shape=jax.ShapeDtypeStruct((rows, len(shards) * width), bf16),
        name="pack_shards",
    )(*shards)


def passed_along(block, axis, distance):
    devices = range(lax.axis_size(axis))
    route = [(i - distance, i) for i in devices if i - distance in devices]
    return lax.ppermute(block, axis, route)


def turned(x, distance):
    devices = lax.axis_size("tp")
    return lax.ppermute(x, "tp", [(i, (i + distance) % devices) for i in range(devices)])


def from_everyone(x, axis):
    devices = lax.axis_size(axis)
    return lax.all_to_all(jnp.broadcast_to(x[None], (devices, *x.shape)), axis, 0, 0, tiled=True)


def rms_rows(activations, gain_vector):
    values = activations.astype(f32)
    inv_scale = lax.rsqrt(jnp.mean(values * values, axis=-1, keepdims=True) + norm_eps)
    return (values * inv_scale * gain_vector).astype(bf16)


def mixing(
    tokens,
    input_norm_gain,
    earlier_gate,
    later_gate,
    convolution_input,
    convolution_taps,
    receptance,
    key_matrix,
    value_matrix,
    decay_matrix,
    rate_matrix,
    decay_floor,
    rate_offset,
    decay_spike,
    initial_state,
    head_norm_gain,
    convolution_output,
    state_heads_output,
):
    normed = rms_rows(tokens[0], input_norm_gain)
    channels = earlier_gate.shape[1]
    heads = channels // HEAD_WIDTH
    both = packed(
        earlier_gate,
        later_gate,
        convolution_input,
        receptance,
        key_matrix,
        value_matrix,
        decay_matrix,
        rate_matrix,
    )
    outer = from_everyone(from_everyone(packed(convolution_output.T, state_heads_output.T), "sp"), "fs")
    outer = jnp.swapaxes(outer, 0, 1).reshape(-1, 2 * channels)
    weights = lax.all_gather(both, "fs", axis=0, tiled=True)
    weights = lax.all_gather(weights, "sp", axis=0, tiled=True)
    piece = from_everyone(normed, "tp").reshape(-1, normed.shape[1])
    piece, outer = lax.optimization_barrier((piece, outer))
    half = outer.shape[0] // 2
    before, after = turned(outer, 2), turned(outer, -2)
    across = jnp.concatenate([turned(before[:half], 2), turned(after[half:], -2)], axis=0)
    vec = jnp.concatenate(
        [
            decay_floor[None],
            rate_offset[None],
            convolution_taps,
            head_norm_gain[None],
            jnp.zeros((2, channels), f32),
        ],
        axis=0,
    )
    conv, o, y, agg, edge = local_call(piece, weights, decay_spike[0], vec)
    pieces = from_everyone(agg, "sp")
    prior = passed_along(edge[22:24], "sp", 1)
    init = jnp.moveaxis(initial_state[0], 0, 1).reshape(HEAD_WIDTH, heads * HEAD_WIDTH)
    pos = lax.axis_index("sp").astype(jnp.int32)[None]
    mixed = finish_call(pos, pieces, init, o, y, conv, edge, prior, vec)
    devices = lax.axis_size("tp")
    chips = devices // 2
    groups = [list(range(core, devices, 2)) for core in range(2)]
    gathered = lax.all_to_all(
        mixed.reshape(chips, -1, 2 * channels), "tp", 0, 0, tiled=True, axis_index_groups=groups
    )
    me = lax.axis_index("tp").astype(jnp.int32)
    chip, core = lax.shift_right_logical(me, 1), me & 1
    near = [(chip + k) & (chips - 1) for k in (0, chips - 1, 1, 2)]
    own = gathered.shape[1] // 2
    weights = (outer, before, after, across)
    given = outward_call(jnp.stack([(1 - core) * own, *near]), gathered, weights, bf16)
    taken = lax.ppermute(given, "tp", [(i, i ^ 1) for i in range(devices)])
    kept = outward_call(jnp.stack([core * own, *near]), gathered, weights, f32)
    return (kept + taken.astype(f32)).astype(bf16)[None]


def solution(mesh):
    placed = (
        P("fs", ("sp", "tp"), None),
        P(),
        P(("sp", "fs"), "tp"),
        P(("sp", "fs"), "tp"),
        P(("sp", "fs"), "tp"),
        P(None, "tp"),
        P(("sp", "fs"), "tp"),
        P(("sp", "fs"), "tp"),
        P(("sp", "fs"), "tp"),
        P(("sp", "fs"), "tp"),
        P(("sp", "fs"), "tp"),
        P("tp"),
        P("tp"),
        P("fs", "sp", "tp"),
        P("fs", "tp", None, None),
        P("tp"),
        P("tp", ("sp", "fs")),
        P("tp", ("sp", "fs")),
    )
    return jax.shard_map(
        mixing,
        mesh=mesh,
        in_specs=placed,
        out_specs=P("fs", ("sp", "tp"), None),
        check_vma=False,
    )
```

```python
import functools

import jax
import jax.numpy as jnp
from jax import lax
from jax.experimental import pallas as pl
from jax.experimental.pallas import tpu as pltpu
from jax.sharding import PartitionSpec as P


HEAD_WIDTH = 64
CHUNK = 64
BLOCK = 256
norm_eps = 1e-06
key_eps = 1e-06
f32, bf16 = jnp.float32, jnp.bfloat16


def dot(a, b, ca=1, cb=0):
    return lax.dot_general(
        a.astype(bf16), b.astype(bf16), (((ca,), (cb,)), ((), ())), preferred_element_type=f32
    )


def lanes_of(shape):
    return lax.broadcasted_iota(jnp.int32, shape, 1)


def rows_of(shape):
    return lax.broadcasted_iota(jnp.int32, shape, 0)


def spread(z, first):
    z = z.astype(bf16)
    return jnp.concatenate([z * first, z * (1 - first)], axis=0)


def head_sums(z, low):
    a = jnp.sum(jnp.where(low, z, 0.0), axis=1, keepdims=True)
    b = jnp.sum(jnp.where(low, 0.0, z), axis=1, keepdims=True)
    return jnp.where(low, a, b)


def local_kernel(x_ref, w_ref, spike_ref, vec_ref, o_ref, y_ref, agg_ref, st_ref):
    step = pl.program_id(0)
    width = 2 * HEAD_WIDTH
    pairs = BLOCK // CHUNK

    @pl.when(step == 0)
    def _():
        r, l = rows_of((width, width)), lanes_of((width, width))
        eye = (r - HEAD_WIDTH == l % HEAD_WIDTH) & (r >= HEAD_WIDTH)
        st_ref[...] = jnp.where(eye, 1.0, 0.0).astype(f32)

    x = x_ref[...]

    def section(first, last):
        out = jnp.dot(x, w_ref[:, first * width : last * width], preferred_element_type=f32)
        out = out.astype(bf16).astype(f32)
        return [out[:, k * width : (k + 1) * width] for k in range(last - first)]

    keys, vals = section(0, 2)
    dpre, rpre = section(2, 4)
    (q,) = section(4, 5)

    low = lanes_of((BLOCK, width)) < HEAD_WIDTH
    logd = spike_ref[...] - jnp.exp(vec_ref[0:1] + jnp.tanh(dpre))
    rate = jax.nn.sigmoid(vec_ref[1:2] + rpre)
    unit = keys * lax.rsqrt(head_sums(keys * keys, low) + key_eps)
    beta = rate * unit
    r, c = rows_of((BLOCK, BLOCK)), lanes_of((BLOCK, BLOCK))
    tri = jnp.where((r >= c) & (r // CHUNK == c // CHUNK), 1.0, 0.0).astype(bf16)
    hi = logd.astype(bf16)
    rest = logd - hi.astype(f32)
    mid = rest.astype(bf16)
    lo = (rest - mid.astype(f32)).astype(bf16)
    sums = jnp.dot(tri, jnp.concatenate([hi, mid, lo], axis=1), preferred_element_type=f32)
    cum_all = sums[:, :width] + sums[:, width : 2 * width] + sums[:, 2 * width :]
    prev_all = cum_all - logd

    shape = (CHUNK, width)
    t, s = rows_of(shape), lanes_of(shape) % HEAD_WIDTH
    strict, inclusive = t > s, t >= s
    low_c = lanes_of(shape) < HEAD_WIDTH
    first = jnp.where(lanes_of((1, width)) < HEAD_WIDTH, 1.0, 0.0).astype(bf16)
    fold = functools.partial(spread, first=first)
    same = (rows_of((width, width)) // HEAD_WIDTH) == (lanes_of((width, width)) // HEAD_WIDTH)
    each = range(pairs)

    def part(a):
        return [a[k * CHUNK : (k + 1) * CHUNK] for k in each]

    q, keys, vals, unit, beta = map(part, (q, keys, vals, unit, beta))
    cum, prev = part(cum_all), part(prev_all)
    center = [cum[k][CHUNK // 2 : CHUNK // 2 + 1] for k in each]
    close = [cum[k][CHUNK - 1 : CHUNK] for k in each]
    e_neg = [jnp.exp(center[k] - cum[k]) for k in each]
    ask_k = [unit[k] * jnp.exp(prev[k] - center[k]) for k in each]
    ask_q = [q[k] * jnp.exp(cum[k] - center[k]) for k in each]
    give_k = [keys[k] * e_neg[k] for k in each]
    give_b = [beta[k] * e_neg[k] for k in each]
    e_center = [jnp.exp(center[k]) for k in each]
    e_tail = [jnp.exp(close[k] - center[k]) for k in each]
    e_close = [jnp.exp(close[k]) for k in each]
    grams = [
        dot(
            jnp.concatenate([ask_k[k], ask_q[k]], axis=0),
            jnp.concatenate([fold(give_k[k]), fold(give_b[k])], axis=0),
            1,
            1,
        )
        for k in each
    ]
    key_ask = [jnp.where(strict, g[:CHUNK, :width], 0.0) for g in grams]
    beta_ask = [jnp.where(strict, g[:CHUNK, width:], 0.0) for g in grams]
    key_read = [jnp.where(inclusive, g[CHUNK:, :width], 0.0) for g in grams]
    beta_read = [jnp.where(inclusive, g[CHUNK:, width:], 0.0) for g in grams]
    both_v = [dot(jnp.concatenate([key_ask[k], key_read[k]], axis=0), fold(vals[k])) for k in each]

    inv = [jnp.where(t == s, 1.0, jnp.where(t // 2 == s // 2, -beta_ask[k], 0.0)) for k in each]
    size = 2
    while size < CHUNK:
        here = (t // (2 * size) == s // (2 * size)) & (t // size != s // size)
        mixed = [dot(inv[k], fold(jnp.where(here, beta_ask[k], 0.0))) for k in each]
        inv = [inv[k] - dot(mixed[k], fold(inv[k])) for k in each]
        size *= 2

    wu = [
        dot(
            inv[k],
            jnp.concatenate([fold(ask_k[k] * e_center[k]), fold(both_v[k][:CHUNK])], axis=1),
        )
        for k in each
    ]
    back = [
        dot(
            beta_read[k],
            jnp.concatenate([fold(wu[k][:, :width]), fold(wu[k][:, width:])], axis=1),
        )
        for k in each
    ]
    q_eff = [ask_q[k] * e_center[k] - back[k][:, :width] for k in each]
    o_loc = [both_v[k][CHUNK:] - back[k][:, width:] for k in each]
    outer = [dot(wu[k], give_b[k] * e_tail[k], 0, 0) for k in each]
    outer_v = [dot(vals[k], give_k[k] * e_tail[k], 0, 0) for k in each]
    step_map = [jnp.where(same, -outer[k][:width], 0.0).astype(bf16) for k in each]
    source_full = [outer_v[k] - outer[k][width:] for k in each]
    source = [jnp.where(low_c, f[:HEAD_WIDTH], f[HEAD_WIDTH:]) for f in source_full]

    state = st_ref[...]
    for k in each:
        got = dot(
            q_eff[k],
            jnp.concatenate([fold(state[:HEAD_WIDTH]), fold(state[HEAD_WIDTH:])], axis=0),
            1,
            1,
        )
        o_ref[k * CHUNK : (k + 1) * CHUNK] = o_loc[k] + got[:, :width]
        y_ref[k * CHUNK : (k + 1) * CHUNK] = got[:, width:].astype(bf16)
        state = state * e_close[k] + dot(state, step_map[k])
        state = jnp.concatenate([state[:HEAD_WIDTH] + source[k], state[HEAD_WIDTH:]], axis=0)
    st_ref[...] = state

    @pl.when(step == pl.num_programs(0) - 1)
    def _():
        agg_ref[...] = state.astype(bf16)


def local_call(x, w, spike, vec):
    rows, depth = x.shape
    width = 2 * HEAD_WIDTH
    whole = lambda *shape: pl.BlockSpec(shape, lambda i: (0,) * len(shape))
    tile = pl.BlockSpec((BLOCK, width), lambda i: (i, 0))
    return pl.pallas_call(
        local_kernel,
        grid=(rows // BLOCK,),
        in_specs=[pl.BlockSpec((BLOCK, depth), lambda i: (i, 0)), whole(*w.shape), tile, whole(8, width)],
        out_specs=[tile, tile, whole(width, width)],
        out_shape=[
            jax.ShapeDtypeStruct((rows, width), f32),
            jax.ShapeDtypeStruct((rows, width), bf16),
            jax.ShapeDtypeStruct((width, width), bf16),
        ],
        scratch_shapes=[pltpu.VMEM((width, width), f32)],
        compiler_params=pltpu.CompilerParams(
            dimension_semantics=("arbitrary",), vmem_limit_bytes=50 * 2**20
        ),
        name="local_mix",
    )(x, w, spike, vec)


def conv_kernel(x_ref, w_ref, halo_ref, vec_ref, out_ref, tail_ref):
    width = vec_ref.shape[1]

    def project(x):
        out = jnp.dot(x, w_ref[...], preferred_element_type=f32).astype(bf16).astype(f32)
        return out[:, :width] * out[:, width : 2 * width], out[:, 2 * width :]

    @pl.when(pl.program_id(0) == 0)
    def _():
        tail_ref[...] = project(halo_ref[...])[0]

    prod, post = project(x_ref[...])
    rows = prod.shape[0]
    tail = tail_ref[...]
    row = rows_of((rows, width))
    last, before = tail[-1:], tail[-2:-1]
    one = jnp.where(row == 0, last, pltpu.roll(prod, 1, 0))
    two = jnp.where(row == 0, before, jnp.where(row == 1, last, pltpu.roll(prod, 2, 0)))
    filtered = vec_ref[2:3] * two + vec_ref[3:4] * one + vec_ref[4:5] * prod
    out_ref[...] = (post * filtered).astype(bf16)
    tail_ref[...] = prod[rows - tail_ref.shape[0] :]


def conv_call(x, w, halo, vec):
    rows, depth = x.shape
    width = vec.shape[1]
    whole = lambda a: pl.BlockSpec(a.shape, lambda i: (0,) * a.ndim)
    return pl.pallas_call(
        conv_kernel,
        grid=(rows // BLOCK,),
        in_specs=[pl.BlockSpec((BLOCK, depth), lambda i: (i, 0)), whole(w), whole(halo), whole(vec)],
        out_specs=pl.BlockSpec((BLOCK, width), lambda i: (i, 0)),
        out_shape=jax.ShapeDtypeStruct((rows, width), bf16),
        scratch_shapes=[pltpu.VMEM((halo.shape[0], width), f32)],
        compiler_params=pltpu.CompilerParams(
            dimension_semantics=("arbitrary",), vmem_limit_bytes=40 * 2**20
        ),
        name="conv_mix",
    )(x, w, halo, vec)


def finish_kernel(pos_ref, agg_ref, init_ref, o_ref, y_ref, conv_ref, vec_ref, out_ref, s_ref):
    step = pl.program_id(0)
    width = 2 * HEAD_WIDTH
    first = jnp.where(lanes_of((1, width)) < HEAD_WIDTH, 1.0, 0.0).astype(bf16)

    @pl.when(step == 0)
    def _():
        def advance(i, state):
            piece = agg_ref[i]
            hi = state.astype(bf16)
            lo = (state - hi.astype(f32)).astype(bf16)
            got = dot(jnp.concatenate([hi, lo], axis=0), spread(piece[HEAD_WIDTH:], first))
            return got[:HEAD_WIDTH] + got[HEAD_WIDTH:] + piece[:HEAD_WIDTH].astype(f32)

        state = lax.fori_loop(0, pos_ref[0], advance, init_ref[...])
        s_ref[...] = spread(state, first)

    low = lanes_of((BLOCK, width)) < HEAD_WIDTH
    reads = o_ref[...] + dot(y_ref[...], s_ref[...], 1, 1)
    centered = reads - head_sums(reads, low) * (1.0 / HEAD_WIDTH)
    variance = head_sums(centered * centered, low) * (1.0 / HEAD_WIDTH)
    mixed = centered * lax.rsqrt(variance + HEAD_WIDTH * 1e-05) * vec_ref[5:6]
    out_ref[:, :width] = conv_ref[...]
    out_ref[:, width:] = mixed.astype(bf16)


def finish_call(pos, agg, init, o, y, conv, vec):
    rows, width = o.shape
    whole = lambda a: pl.BlockSpec(a.shape, lambda i, p: (0,) * a.ndim)
    tile = pl.BlockSpec((BLOCK, width), lambda i, p: (i, 0))
    return pl.pallas_call(
        finish_kernel,
        grid_spec=pltpu.PrefetchScalarGridSpec(
            num_scalar_prefetch=1,
            grid=(rows // BLOCK,),
            in_specs=[whole(agg), whole(init), tile, tile, tile, whole(vec)],
            out_specs=pl.BlockSpec((BLOCK, 2 * width), lambda i, p: (i, 0)),
            scratch_shapes=[pltpu.VMEM((width, width), bf16)],
        ),
        out_shape=jax.ShapeDtypeStruct((rows, 2 * width), bf16),
        compiler_params=pltpu.CompilerParams(
            dimension_semantics=("arbitrary",), vmem_limit_bytes=50 * 2**20
        ),
        name="finish_mix",
    )(pos, agg, init, o, y, conv, vec)


def outward_kernel(pick_ref, m_ref, *refs):
    *weights, out_ref = refs
    rows = out_ref.shape[0]
    at = pl.multiple_of(pick_ref[0], rows)
    total = None
    for k, w_ref in enumerate(weights):
        got = dot(m_ref[pick_ref[1 + k], pl.ds(at, rows), :], w_ref[...])
        total = got if total is None else total + got
    out_ref[...] = total.astype(out_ref.dtype)


def outward_call(pick, gathered, weights, dtype):
    _, rows, depth = gathered.shape
    columns = weights[0].shape[1]
    step = 512
    return pl.pallas_call(
        outward_kernel,
        grid_spec=pltpu.PrefetchScalarGridSpec(
            num_scalar_prefetch=1,
            grid=(columns // step,),
            in_specs=[pl.BlockSpec(gathered.shape, lambda i, p: (0, 0, 0))]
            + [pl.BlockSpec((depth, step), lambda i, p: (0, i)) for _ in weights],
            out_specs=pl.BlockSpec((rows // 2, step), lambda i, p: (0, i)),
        ),
        out_shape=jax.ShapeDtypeStruct((rows // 2, columns), dtype),
        compiler_params=pltpu.CompilerParams(dimension_semantics=("arbitrary",)),
        name="outward",
    )(pick, gathered, *weights)


def pack_kernel(*refs):
    *parts, out_ref = refs
    for k, ref in enumerate(parts):
        width = ref.shape[1]
        out_ref[:, k * width : (k + 1) * width] = ref[...]


def packed(*shards):
    rows, width = shards[0].shape
    return pl.pallas_call(
        pack_kernel,
        out_shape=jax.ShapeDtypeStruct((rows, len(shards) * width), bf16),
        name="pack_shards",
    )(*shards)


def passed_along(block, axis, distance):
    devices = range(lax.axis_size(axis))
    route = [(i - distance, i) for i in devices if i - distance in devices]
    return lax.ppermute(block, axis, route)


def turned(x, axis, distance):
    devices = lax.axis_size(axis)
    return lax.ppermute(x, axis, [(i, (i + distance) % devices) for i in range(devices)])


def from_everyone(x, axis):
    devices = lax.axis_size(axis)
    return lax.all_to_all(jnp.broadcast_to(x[None], (devices, *x.shape)), axis, 0, 0, tiled=True)


def rms_rows(activations, gain_vector):
    values = activations.astype(f32)
    inv_scale = lax.rsqrt(jnp.mean(values * values, axis=-1, keepdims=True) + norm_eps)
    return (values * inv_scale * gain_vector).astype(bf16)


def mixing(
    tokens,
    input_norm_gain,
    earlier_gate,
    later_gate,
    convolution_input,
    convolution_taps,
    receptance,
    key_matrix,
    value_matrix,
    decay_matrix,
    rate_matrix,
    decay_floor,
    rate_offset,
    decay_spike,
    initial_state,
    head_norm_gain,
    convolution_output,
    state_heads_output,
):
    channels = earlier_gate.shape[1]
    heads = channels // HEAD_WIDTH
    vec = jnp.concatenate(
        [
            decay_floor[None],
            rate_offset[None],
            convolution_taps,
            head_norm_gain[None],
            jnp.zeros((2, channels), f32),
        ],
        axis=0,
    )
    init = jnp.moveaxis(initial_state[0], 0, 1).reshape(HEAD_WIDTH, heads * HEAD_WIDTH)
    pos = lax.axis_index("sp").astype(jnp.int32)[None]

    def rows_whole(shards):
        return lax.all_gather(shards, "fs", axis=1, tiled=True).reshape(-1, shards.shape[2])

    early = from_everyone(packed(key_matrix, value_matrix, decay_matrix, rate_matrix, receptance), "sp")
    normed = rms_rows(tokens[0], input_norm_gain)
    piece = lax.all_gather(normed, "tp", axis=0, tiled=True)
    early = rows_whole(early)
    halo = passed_along(piece[-16:], "sp", 1)
    outer = packed(convolution_output.T, state_heads_output.T)
    late = packed(earlier_gate, convolution_input, later_gate)
    outer = from_everyone(outer, "sp")
    late = from_everyone(late, "sp")
    others = [turned(outer, "fs", -k) for k in (1, 2, 3)]
    outer = jnp.roll(jnp.stack([outer, *others], axis=1), lax.axis_index("fs"), axis=1)
    outer = outer.reshape(-1, 2 * channels).T
    before, after = turned(outer, "tp", 2), turned(outer, "tp", -2)
    far = turned(before[:channels], "tp", 2), turned(after[channels:], "tp", -2)
    across = jnp.concatenate(far, axis=0)
    o, y, agg = local_call(piece, early, decay_spike[0], vec)
    pieces = from_everyone(agg, "sp")
    late = rows_whole(late)
    conv = conv_call(piece, late, halo, vec)
    mixed = finish_call(pos, pieces, init, o, y, conv, vec)
    devices = lax.axis_size("tp")
    chips = devices // 2
    groups = [list(range(core, devices, 2)) for core in range(2)]
    gathered = lax.all_to_all(
        mixed.reshape(chips, -1, 2 * channels), "tp", 0, 0, tiled=True, axis_index_groups=groups
    )
    me = lax.axis_index("tp").astype(jnp.int32)
    chip, core = lax.shift_right_logical(me, 1), me & 1
    near = [(chip + k) & (chips - 1) for k in (0, chips - 1, 1, 2)]
    own = gathered.shape[1] // 2
    weights = (outer, before, after, across)
    given = outward_call(jnp.stack([(1 - core) * own, *near]), gathered, weights, bf16)
    taken = lax.ppermute(given, "tp", [(i, i ^ 1) for i in range(devices)])
    kept = outward_call(jnp.stack([core * own, *near]), gathered, weights, f32)
    return (kept + taken.astype(f32)).astype(bf16)[None]


def solution(mesh):
    placed = (
        P("fs", ("sp", "tp"), None),
        P(),
        P(("sp", "fs"), "tp"),
        P(("sp", "fs"), "tp"),
        P(("sp", "fs"), "tp"),
        P(None, "tp"),
        P(("sp", "fs"), "tp"),
        P(("sp", "fs"), "tp"),
        P(("sp", "fs"), "tp"),
        P(("sp", "fs"), "tp"),
        P(("sp", "fs"), "tp"),
        P("tp"),
        P("tp"),
        P("fs", "sp", "tp"),
        P("fs", "tp", None, None),
        P("tp"),
        P("tp", ("sp", "fs")),
        P("tp", ("sp", "fs")),
    )
    return jax.shard_map(
        mixing,
        mesh=mesh,
        in_specs=placed,
        out_specs=P("fs", ("sp", "tp"), None),
        check_vma=False,
    )
```

```python
import functools

import jax
import jax.numpy as jnp
from jax import lax
from jax.experimental import pallas as pl
from jax.experimental.pallas import tpu as pltpu
from jax.sharding import PartitionSpec as P


HEAD_WIDTH = 64
CHUNK = 64
BLOCK = 256
norm_eps = 1e-06
key_eps = 1e-06
f32, bf16 = jnp.float32, jnp.bfloat16


def dot(a, b, ca=1, cb=0):
    return lax.dot_general(
        a.astype(bf16), b.astype(bf16), (((ca,), (cb,)), ((), ())), preferred_element_type=f32
    )


def lanes_of(shape):
    return lax.broadcasted_iota(jnp.int32, shape, 1)


def rows_of(shape):
    return lax.broadcasted_iota(jnp.int32, shape, 0)


def spread(z, first):
    z = z.astype(bf16)
    return jnp.concatenate([z * first, z * (1 - first)], axis=0)


def head_sums(z, low):
    a = jnp.sum(jnp.where(low, z, 0.0), axis=1, keepdims=True)
    b = jnp.sum(jnp.where(low, 0.0, z), axis=1, keepdims=True)
    return jnp.where(low, a, b)


def local_kernel(place_ref, same_ref, other_ref, w_ref, spike_ref, vec_ref, conv_ref, o_ref, y_ref, agg_ref, edge_ref, st_ref, tail_ref):
    step = pl.program_id(0)
    width = 2 * HEAD_WIDTH
    pairs = BLOCK // CHUNK

    @pl.when(step == 0)
    def _():
        r, l = rows_of((width, width)), lanes_of((width, width))
        eye = (r - HEAD_WIDTH == l % HEAD_WIDTH) & (r >= HEAD_WIDTH)
        st_ref[...] = jnp.where(eye, 1.0, 0.0).astype(f32)
        tail_ref[...] = jnp.zeros_like(tail_ref)

    mine, theirs = same_ref[0], other_ref[0]
    low_core = place_ref[1] == 0
    x = jnp.concatenate([jnp.where(low_core, mine, theirs), jnp.where(low_core, theirs, mine)], axis=0)

    def section(k):
        two = jnp.dot(x, w_ref[:, 2 * k * width : 2 * (k + 1) * width], preferred_element_type=f32)
        two = two.astype(bf16).astype(f32)
        return two[:, :width], two[:, width:]

    pre, post = section(0)
    cvals, q = section(1)
    keys, vals = section(2)
    dpre, rpre = section(3)

    prod = pre * cvals
    tail = tail_ref[...]
    row = rows_of((BLOCK, width))
    last, before = tail[7:8], tail[6:7]
    one = jnp.where(row == 0, last, pltpu.roll(prod, 1, 0))
    two = jnp.where(row == 0, before, jnp.where(row == 1, last, pltpu.roll(prod, 2, 0)))
    filtered = vec_ref[2:3] * two + vec_ref[3:4] * one + vec_ref[4:5] * prod
    conv_ref[...] = (post * filtered).astype(bf16)
    tail_ref[...] = prod[BLOCK - 8 :]

    @pl.when(step == 0)
    def _():
        edge_ref[0:8] = prod[:8]
        edge_ref[8:16] = post[:8]

    @pl.when(step == pl.num_programs(0) - 1)
    def _():
        edge_ref[16:24] = prod[BLOCK - 8 :]

    low = lanes_of((BLOCK, width)) < HEAD_WIDTH
    logd = spike_ref[...] - jnp.exp(vec_ref[0:1] + jnp.tanh(dpre))
    rate = jax.nn.sigmoid(vec_ref[1:2] + rpre)
    unit = keys * lax.rsqrt(head_sums(keys * keys, low) + key_eps)
    beta = rate * unit
    r, c = rows_of((BLOCK, BLOCK)), lanes_of((BLOCK, BLOCK))
    tri = jnp.where((r >= c) & (r // CHUNK == c // CHUNK), 1.0, 0.0).astype(bf16)
    hi = logd.astype(bf16)
    rest = logd - hi.astype(f32)
    mid = rest.astype(bf16)
    lo = (rest - mid.astype(f32)).astype(bf16)
    sums = jnp.dot(tri, jnp.concatenate([hi, mid, lo], axis=1), preferred_element_type=f32)
    cum_all = sums[:, :width] + sums[:, width : 2 * width] + sums[:, 2 * width :]
    prev_all = cum_all - logd

    shape = (CHUNK, width)
    t, s = rows_of(shape), lanes_of(shape) % HEAD_WIDTH
    strict, inclusive = t > s, t >= s
    low_c = lanes_of(shape) < HEAD_WIDTH
    first = jnp.where(lanes_of((1, width)) < HEAD_WIDTH, 1.0, 0.0).astype(bf16)
    fold = functools.partial(spread, first=first)
    same = (rows_of((width, width)) // HEAD_WIDTH) == (lanes_of((width, width)) // HEAD_WIDTH)
    each = range(pairs)

    def part(a):
        return [a[k * CHUNK : (k + 1) * CHUNK] for k in each]

    q, keys, vals, unit, beta = map(part, (q, keys, vals, unit, beta))
    cum, prev = part(cum_all), part(prev_all)
    center = [cum[k][CHUNK // 2 : CHUNK // 2 + 1] for k in each]
    close = [cum[k][CHUNK - 1 : CHUNK] for k in each]
    e_neg = [jnp.exp(center[k] - cum[k]) for k in each]
    ask_k = [unit[k] * jnp.exp(prev[k] - center[k]) for k in each]
    ask_q = [q[k] * jnp.exp(cum[k] - center[k]) for k in each]
    give_k = [keys[k] * e_neg[k] for k in each]
    give_b = [beta[k] * e_neg[k] for k in each]
    e_center = [jnp.exp(center[k]) for k in each]
    e_tail = [jnp.exp(close[k] - center[k]) for k in each]
    e_close = [jnp.exp(close[k]) for k in each]
    grams = [
        dot(
            jnp.concatenate([ask_k[k], ask_q[k]], axis=0),
            jnp.concatenate([fold(give_k[k]), fold(give_b[k])], axis=0),
            1,
            1,
        )
        for k in each
    ]
    key_ask = [jnp.where(strict, g[:CHUNK, :width], 0.0) for g in grams]
    beta_ask = [jnp.where(strict, g[:CHUNK, width:], 0.0) for g in grams]
    key_read = [jnp.where(inclusive, g[CHUNK:, :width], 0.0) for g in grams]
    beta_read = [jnp.where(inclusive, g[CHUNK:, width:], 0.0) for g in grams]
    both_v = [dot(jnp.concatenate([key_ask[k], key_read[k]], axis=0), fold(vals[k])) for k in each]

    inv = [jnp.where(t == s, 1.0, jnp.where(t // 2 == s // 2, -beta_ask[k], 0.0)) for k in each]
    size = 2
    while size < CHUNK:
        here = (t // (2 * size) == s // (2 * size)) & (t // size != s // size)
        mixed = [dot(inv[k], fold(jnp.where(here, beta_ask[k], 0.0))) for k in each]
        inv = [inv[k] - dot(mixed[k], fold(inv[k])) for k in each]
        size *= 2

    wu = [
        dot(
            inv[k],
            jnp.concatenate([fold(ask_k[k] * e_center[k]), fold(both_v[k][:CHUNK])], axis=1),
        )
        for k in each
    ]
    back = [
        dot(
            beta_read[k],
            jnp.concatenate([fold(wu[k][:, :width]), fold(wu[k][:, width:])], axis=1),
        )
        for k in each
    ]
    q_eff = [ask_q[k] * e_center[k] - back[k][:, :width] for k in each]
    o_loc = [both_v[k][CHUNK:] - back[k][:, width:] for k in each]
    outer = [dot(wu[k], give_b[k] * e_tail[k], 0, 0) for k in each]
    outer_v = [dot(vals[k], give_k[k] * e_tail[k], 0, 0) for k in each]
    step_map = [jnp.where(same, -outer[k][:width], 0.0).astype(bf16) for k in each]
    source_full = [outer_v[k] - outer[k][width:] for k in each]
    source = [jnp.where(low_c, f[:HEAD_WIDTH], f[HEAD_WIDTH:]) for f in source_full]

    state = st_ref[...]
    for k in each:
        got = dot(
            q_eff[k],
            jnp.concatenate([fold(state[:HEAD_WIDTH]), fold(state[HEAD_WIDTH:])], axis=0),
            1,
            1,
        )
        o_ref[k * CHUNK : (k + 1) * CHUNK] = o_loc[k] + got[:, :width]
        y_ref[k * CHUNK : (k + 1) * CHUNK] = got[:, width:].astype(bf16)
        state = state * e_close[k] + dot(state, step_map[k])
        state = jnp.concatenate([state[:HEAD_WIDTH] + source[k], state[HEAD_WIDTH:]], axis=0)
    st_ref[...] = state

    @pl.when(step == pl.num_programs(0) - 1)
    def _():
        agg_ref[...] = state.astype(bf16)


def local_call(place, same, other, w, spike, vec):
    chips, part, depth = same.shape
    rows, width = spike.shape
    whole = lambda *shape: pl.BlockSpec(shape, lambda i, p: (0,) * len(shape))
    tile = pl.BlockSpec((BLOCK, width), lambda i, p: (i, 0))
    tokens = pl.BlockSpec((1, part, depth), lambda i, p: ((i - p[0]) & (chips - 1), 0, 0))
    return pl.pallas_call(
        local_kernel,
        grid_spec=pltpu.PrefetchScalarGridSpec(
            num_scalar_prefetch=1,
            grid=(rows // BLOCK,),
            in_specs=[tokens, tokens, whole(depth, 8 * width), tile, whole(8, width)],
            out_specs=[tile, tile, tile, whole(width, width), whole(24, width)],
            scratch_shapes=[pltpu.VMEM((width, width), f32), pltpu.VMEM((8, width), f32)],
        ),
        out_shape=[
            jax.ShapeDtypeStruct((rows, width), bf16),
            jax.ShapeDtypeStruct((rows, width), f32),
            jax.ShapeDtypeStruct((rows, width), bf16),
            jax.ShapeDtypeStruct((width, width), bf16),
            jax.ShapeDtypeStruct((24, width), f32),
        ],
        compiler_params=pltpu.CompilerParams(
            dimension_semantics=("arbitrary",), vmem_limit_bytes=50 * 2**20
        ),
        name="local_mix",
    )(place, same, other, w, spike, vec)


def finish_kernel(pos_ref, agg_ref, init_ref, o_ref, y_ref, conv_ref, edge_ref, prior_ref, vec_ref, out_ref, s_ref):
    step = pl.program_id(0)
    width = 2 * HEAD_WIDTH
    first = jnp.where(lanes_of((1, width)) < HEAD_WIDTH, 1.0, 0.0).astype(bf16)

    @pl.when(step == 0)
    def _():
        def advance(i, state):
            piece = agg_ref[i]
            hi = state.astype(bf16)
            lo = (state - hi.astype(f32)).astype(bf16)
            got = dot(jnp.concatenate([hi, lo], axis=0), spread(piece[HEAD_WIDTH:], first))
            return got[:HEAD_WIDTH] + got[HEAD_WIDTH:] + piece[:HEAD_WIDTH].astype(f32)

        state = lax.fori_loop(0, pos_ref[0], advance, init_ref[...])
        s_ref[...] = spread(state, first)

    low = lanes_of((BLOCK, width)) < HEAD_WIDTH
    reads = o_ref[...] + dot(y_ref[...], s_ref[...], 1, 1)
    centered = reads - head_sums(reads, low) * (1.0 / HEAD_WIDTH)
    variance = head_sums(centered * centered, low) * (1.0 / HEAD_WIDTH)
    mixed = centered * lax.rsqrt(variance + HEAD_WIDTH * 1e-05) * vec_ref[5:6]

    prod, post = edge_ref[0:8], edge_ref[8:16]
    last, before = prior_ref[1:2], prior_ref[0:1]
    row = rows_of((8, width))
    one = jnp.where(row == 0, last, pltpu.roll(prod, 1, 0))
    two = jnp.where(row == 0, before, jnp.where(row == 1, last, pltpu.roll(prod, 2, 0)))
    fixed = post * (vec_ref[2:3] * two + vec_ref[3:4] * one + vec_ref[4:5] * prod)
    conv = conv_ref[...]
    head = jnp.where((step == 0) & (rows_of((16, width)) < 2), jnp.concatenate([fixed, fixed], axis=0), conv[:16].astype(f32))
    conv = jnp.concatenate([head.astype(bf16), conv[16:]], axis=0)
    out_ref[:, :width] = conv
    out_ref[:, width:] = mixed.astype(bf16)


def finish_call(pos, agg, init, o, y, conv, edge, prior, vec):
    rows, width = o.shape
    whole = lambda a: pl.BlockSpec(a.shape, lambda i, p: (0,) * a.ndim)
    tile = pl.BlockSpec((BLOCK, width), lambda i, p: (i, 0))
    return pl.pallas_call(
        finish_kernel,
        grid_spec=pltpu.PrefetchScalarGridSpec(
            num_scalar_prefetch=1,
            grid=(rows // BLOCK,),
            in_specs=[whole(agg), whole(init), tile, tile, tile, whole(edge), whole(prior), whole(vec)],
            out_specs=pl.BlockSpec((BLOCK, 2 * width), lambda i, p: (i, 0)),
            scratch_shapes=[pltpu.VMEM((width, width), bf16)],
        ),
        out_shape=jax.ShapeDtypeStruct((rows, 2 * width), bf16),
        compiler_params=pltpu.CompilerParams(
            dimension_semantics=("arbitrary",), vmem_limit_bytes=50 * 2**20
        ),
        name="finish_mix",
    )(pos, agg, init, o, y, conv, edge, prior, vec)


def outward_kernel(pick_ref, m_ref, *refs):
    *weights, keep_ref, give_ref = refs
    total = None
    for k, w_ref in enumerate(weights):
        got = dot(m_ref[pick_ref[1 + k]], w_ref[...])
        total = got if total is None else total + got
    total = total.astype(bf16)
    rows = keep_ref.shape[0]
    first = pick_ref[0] == 0
    keep_ref[...] = jnp.where(first, total[:rows], total[rows:])
    give_ref[...] = jnp.where(first, total[rows:], total[:rows])


def outward_call(pick, gathered, weights):
    _, rows, depth = gathered.shape
    columns = weights[0].shape[1]
    step = 512
    tile = pl.BlockSpec((rows // 2, step), lambda i, p: (0, i))
    return pl.pallas_call(
        outward_kernel,
        grid_spec=pltpu.PrefetchScalarGridSpec(
            num_scalar_prefetch=1,
            grid=(columns // step,),
            in_specs=[pl.BlockSpec(gathered.shape, lambda i, p: (0, 0, 0))]
            + [pl.BlockSpec((depth, step), lambda i, p: (0, i)) for _ in weights],
            out_specs=[tile, tile],
        ),
        out_shape=[jax.ShapeDtypeStruct((rows // 2, columns), bf16)] * 2,
        compiler_params=pltpu.CompilerParams(dimension_semantics=("arbitrary",)),
        name="outward",
    )(pick, gathered, *weights)


def pack_kernel(*refs):
    *parts, out_ref = refs
    for k, ref in enumerate(parts):
        width = ref.shape[1]
        out_ref[:, k * width : (k + 1) * width] = ref[...]


def packed(*shards):
    rows, width = shards[0].shape
    return pl.pallas_call(
        pack_kernel,
        out_shape=jax.ShapeDtypeStruct((rows, len(shards) * width), bf16),
        name="pack_shards",
    )(*shards)


def passed_along(block, axis, distance):
    devices = range(lax.axis_size(axis))
    route = [(i - distance, i) for i in devices if i - distance in devices]
    return lax.ppermute(block, axis, route)


def turned(x, distance):
    devices = lax.axis_size("tp")
    return lax.ppermute(x, "tp", [(i, (i + distance) % devices) for i in range(devices)])


def from_everyone(x, axis):
    devices = lax.axis_size(axis)
    return lax.all_to_all(jnp.broadcast_to(x[None], (devices, *x.shape)), axis, 0, 0, tiled=True)


def rms_rows(activations, gain_vector):
    values = activations.astype(f32)
    inv_scale = lax.rsqrt(jnp.mean(values * values, axis=-1, keepdims=True) + norm_eps)
    return (values * inv_scale * gain_vector).astype(bf16)


def mixing(
    tokens,
    input_norm_gain,
    earlier_gate,
    later_gate,
    convolution_input,
    convolution_taps,
    receptance,
    key_matrix,
    value_matrix,
    decay_matrix,
    rate_matrix,
    decay_floor,
    rate_offset,
    decay_spike,
    initial_state,
    head_norm_gain,
    convolution_output,
    state_heads_output,
):
    channels = earlier_gate.shape[1]
    heads = channels // HEAD_WIDTH
    devices = lax.axis_size("tp")
    chips = devices // 2
    me = lax.axis_index("tp").astype(jnp.int32)
    chip, core = lax.shift_right_logical(me, 1), me & 1

    def core_swap(x):
        return lax.ppermute(x, "tp", [(i, i ^ 1) for i in range(devices)])

    both = packed(
        earlier_gate,
        later_gate,
        convolution_input,
        receptance,
        key_matrix,
        value_matrix,
        decay_matrix,
        rate_matrix,
    )
    weights = lax.all_gather(both, "fs", axis=0, tiled=True)
    weights = lax.all_gather(weights, "sp", axis=0, tiled=True)
    outer = from_everyone(packed(convolution_output.T, state_heads_output.T), "sp")
    outer = from_everyone(outer, "fs")
    outer = jnp.swapaxes(outer, 0, 1).reshape(-1, 2 * channels).T

    normed = rms_rows(tokens[0], input_norm_gain)
    behind, ahead = turned(normed, 2), turned(normed, -2)
    cut = normed.shape[0] // 2
    far = turned(behind[:cut], 2), turned(ahead[cut:], -2)
    same = jnp.stack([normed, ahead, jnp.concatenate(far, axis=0), behind])
    other = core_swap(same)

    before, after = turned(outer, 2), turned(outer, -2)
    far = turned(before[:channels], 2), turned(after[channels:], -2)
    across = jnp.concatenate(far, axis=0)
    vec = jnp.concatenate(
        [
            decay_floor[None],
            rate_offset[None],
            convolution_taps,
            head_norm_gain[None],
            jnp.zeros((2, channels), f32),
        ],
        axis=0,
    )
    conv, o, y, agg, edge = local_call(
        jnp.stack([chip, core]), same, other, weights, decay_spike[0], vec
    )
    pieces = from_everyone(agg, "sp")
    prior = passed_along(edge[22:24], "sp", 1)
    init = jnp.moveaxis(initial_state[0], 0, 1).reshape(HEAD_WIDTH, heads * HEAD_WIDTH)
    pos = lax.axis_index("sp").astype(jnp.int32)[None]
    mixed = finish_call(pos, pieces, init, o, y, conv, edge, prior, vec)
    groups = [list(range(side, devices, 2)) for side in range(2)]
    gathered = lax.all_to_all(
        mixed.reshape(chips, -1, 2 * channels), "tp", 0, 0, tiled=True, axis_index_groups=groups
    )
    near = [(chip + k) & (chips - 1) for k in (0, chips - 1, 1, 2)]
    kept, given = outward_call(jnp.stack([core, *near]), gathered, (outer, before, after, across))
    taken = core_swap(given)
    return (kept.astype(f32) + taken.astype(f32)).astype(bf16)[None]


def solution(mesh):
    placed = (
        P("fs", ("sp", "tp"), None),
        P(),
        P(("sp", "fs"), "tp"),
        P(("sp", "fs"), "tp"),
        P(("sp", "fs"), "tp"),
        P(None, "tp"),
        P(("sp", "fs"), "tp"),
        P(("sp", "fs"), "tp"),
        P(("sp", "fs"), "tp"),
        P(("sp", "fs"), "tp"),
        P(("sp", "fs"), "tp"),
        P("tp"),
        P("tp"),
        P("fs", "sp", "tp"),
        P("fs", "tp", None, None),
        P("tp"),
        P("tp", ("sp", "fs")),
        P("tp", ("sp", "fs")),
    )
    return jax.shard_map(
        mixing,
        mesh=mesh,
        in_specs=placed,
        out_specs=P("fs", ("sp", "tp"), None),
        check_vma=False,
    )
```

```python
import functools

import jax
import jax.numpy as jnp
from jax import lax
from jax.experimental import pallas as pl
from jax.experimental.pallas import tpu as pltpu
from jax.sharding import PartitionSpec as P


HEAD_WIDTH = 64
CHUNK = 64
BLOCK = 256
norm_eps = 1e-06
key_eps = 1e-06
f32, bf16 = jnp.float32, jnp.bfloat16


def dot(a, b, ca=1, cb=0):
    return lax.dot_general(
        a.astype(bf16), b.astype(bf16), (((ca,), (cb,)), ((), ())), preferred_element_type=f32
    )


def lanes_of(shape):
    return lax.broadcasted_iota(jnp.int32, shape, 1)


def rows_of(shape):
    return lax.broadcasted_iota(jnp.int32, shape, 0)


def spread(z, first):
    z = z.astype(bf16)
    return jnp.concatenate([z * first, z * (1 - first)], axis=0)


def head_sums(z, low):
    a = jnp.sum(jnp.where(low, z, 0.0), axis=1, keepdims=True)
    b = jnp.sum(jnp.where(low, 0.0, z), axis=1, keepdims=True)
    return jnp.where(low, a, b)


def own_block(place_ref, same_ref, other_ref):
    mine, theirs = same_ref[0], other_ref[0]
    low_core = place_ref[1] == 0
    return jnp.concatenate([jnp.where(low_core, mine, theirs), jnp.where(low_core, theirs, mine)], axis=0)


def chunk_masks():
    shape = (CHUNK, 2 * HEAD_WIDTH)
    return rows_of(shape), lanes_of(shape) % HEAD_WIDTH, lanes_of(shape) < HEAD_WIDTH


def first_lanes():
    return jnp.where(lanes_of((1, 2 * HEAD_WIDTH)) < HEAD_WIDTH, 1.0, 0.0).astype(bf16)


def cut(a):
    return [a[k * CHUNK : (k + 1) * CHUNK] for k in range(a.shape[0] // CHUNK)]


def maps_kernel(
    place_ref,
    same_ref,
    other_ref,
    w_ref,
    spike_ref,
    vec_ref,
    gk_ref,
    gb_ref,
    wu_ref,
    v_ref,
    pos_ref,
    full_ref,
    states_ref,
    agg_ref,
    st_ref,
):
    step = pl.program_id(0)
    width = 2 * HEAD_WIDTH
    each = range(BLOCK // CHUNK)

    @pl.when(step == 0)
    def _():
        r, l = rows_of((width, width)), lanes_of((width, width))
        eye = (r - HEAD_WIDTH == l % HEAD_WIDTH) & (r >= HEAD_WIDTH)
        st_ref[...] = jnp.where(eye, 1.0, 0.0).astype(f32)

    x = own_block(place_ref, same_ref, other_ref)

    def section(k):
        two = jnp.dot(x, w_ref[:, 2 * k * width : 2 * (k + 1) * width], preferred_element_type=f32)
        two = two.astype(bf16)
        return two[:, :width], two[:, width:]

    dpre, rpre = (a.astype(f32) for a in section(1))
    keys, vals = section(0)
    v_ref[...] = vals
    keys = keys.astype(f32)

    low = lanes_of((BLOCK, width)) < HEAD_WIDTH
    logd = spike_ref[...] - jnp.exp(vec_ref[0:1] + jnp.tanh(dpre))
    rate = jax.nn.sigmoid(vec_ref[1:2] + rpre)
    unit = keys * lax.rsqrt(head_sums(keys * keys, low) + key_eps)
    beta = rate * unit
    r, c = rows_of((BLOCK, BLOCK)), lanes_of((BLOCK, BLOCK))
    tri = jnp.where((r >= c) & (r // CHUNK == c // CHUNK), 1.0, 0.0).astype(bf16)
    hi = logd.astype(bf16)
    rest = logd - hi.astype(f32)
    mid = rest.astype(bf16)
    lo = (rest - mid.astype(f32)).astype(bf16)
    sums = jnp.dot(tri, jnp.concatenate([hi, mid, lo], axis=1), preferred_element_type=f32)
    cum_all = sums[:, :width] + sums[:, width : 2 * width] + sums[:, 2 * width :]
    prev_all = cum_all - logd

    t, s, low_c = chunk_masks()
    strict = t > s
    fold = functools.partial(spread, first=first_lanes())
    same = (rows_of((width, width)) // HEAD_WIDTH) == (lanes_of((width, width)) // HEAD_WIDTH)

    keys, vals, unit, beta, cum, prev = map(cut, (keys, vals, unit, beta, cum_all, prev_all))
    center = [cum[k][CHUNK // 2 : CHUNK // 2 + 1] for k in each]
    close = [cum[k][CHUNK - 1 : CHUNK] for k in each]
    e_neg = [jnp.exp(center[k] - cum[k]) for k in each]
    ask_k = [unit[k] * jnp.exp(prev[k] - center[k]) for k in each]
    give_k = [keys[k] * e_neg[k] for k in each]
    give_b = [beta[k] * e_neg[k] for k in each]
    e_center = [jnp.exp(center[k]) for k in each]
    e_tail = [jnp.exp(close[k] - center[k]) for k in each]
    e_close = [jnp.exp(close[k]) for k in each]
    grams = [dot(ask_k[k], jnp.concatenate([fold(give_k[k]), fold(give_b[k])], axis=0), 1, 1) for k in each]
    key_ask = [jnp.where(strict, g[:, :width], 0.0) for g in grams]
    beta_ask = [jnp.where(strict, g[:, width:], 0.0) for g in grams]
    asked = [dot(key_ask[k], fold(vals[k])) for k in each]

    inv = [jnp.where(t == s, 1.0, jnp.where(t // 2 == s // 2, -beta_ask[k], 0.0)) for k in each]
    size = 2
    while size < CHUNK:
        here = (t // (2 * size) == s // (2 * size)) & (t // size != s // size)
        mixed = [dot(inv[k], fold(jnp.where(here, beta_ask[k], 0.0))) for k in each]
        inv = [inv[k] - dot(mixed[k], fold(inv[k])) for k in each]
        size *= 2

    wu = [
        dot(inv[k], jnp.concatenate([fold(ask_k[k] * e_center[k]), fold(asked[k])], axis=1))
        for k in each
    ]
    outer = [dot(wu[k], give_b[k] * e_tail[k], 0, 0) for k in each]
    outer_v = [dot(vals[k], give_k[k] * e_tail[k], 0, 0) for k in each]
    step_map = [jnp.where(same, -outer[k][:width], 0.0).astype(bf16) for k in each]
    source_full = [outer_v[k] - outer[k][width:] for k in each]
    source = [jnp.where(low_c, f[:HEAD_WIDTH], f[HEAD_WIDTH:]) for f in source_full]

    state = st_ref[...]
    for k in each:
        rounded = state.astype(bf16)
        states_ref[k] = rounded
        state = state * e_close[k] + dot(rounded, step_map[k])
        state = jnp.concatenate([state[:HEAD_WIDTH] + source[k], state[HEAD_WIDTH:]], axis=0)
    st_ref[...] = state

    for k in each:
        at = slice(k * CHUNK, (k + 1) * CHUNK)
        gk_ref[at] = give_k[k].astype(bf16)
        gb_ref[at] = give_b[k].astype(bf16)
        wu_ref[at] = wu[k].astype(bf16)
        pos_ref[at] = jnp.exp(cum[k] - center[k])
        full_ref[at] = jnp.exp(cum[k])

    @pl.when(step == pl.num_programs(0) - 1)
    def _():
        for k in range(agg_ref.shape[0]):
            agg_ref[k] = state.astype(bf16)


def token_specs(same):
    chips, part, depth = same.shape
    tokens = pl.BlockSpec((1, part, depth), lambda i, p: ((i - p[0]) & (chips - 1), 0, 0))
    return [tokens, tokens]


def maps_call(place, same, other, w, spike, vec, copies):
    rows, width = spike.shape
    depth = w.shape[0]
    tile = pl.BlockSpec((BLOCK, width), lambda i, p: (i, 0))
    wide = pl.BlockSpec((BLOCK, 2 * width), lambda i, p: (i, 0))
    pairs = BLOCK // CHUNK
    like = lambda n, t: jax.ShapeDtypeStruct((rows, n), t)
    return pl.pallas_call(
        maps_kernel,
        grid_spec=pltpu.PrefetchScalarGridSpec(
            num_scalar_prefetch=1,
            grid=(rows // BLOCK,),
            in_specs=token_specs(same)
            + [
                pl.BlockSpec((depth, 4 * width), lambda i, p: (0, 0)),
                tile,
                pl.BlockSpec(vec.shape, lambda i, p: (0, 0)),
            ],
            out_specs=[
                tile,
                tile,
                wide,
                tile,
                tile,
                tile,
                pl.BlockSpec((pairs, width, width), lambda i, p: (i, 0, 0)),
                pl.BlockSpec((copies, width, width), lambda i, p: (0, 0, 0)),
            ],
            scratch_shapes=[pltpu.VMEM((width, width), f32)],
        ),
        out_shape=[
            like(width, bf16),
            like(width, bf16),
            like(2 * width, bf16),
            like(width, bf16),
            like(width, f32),
            like(width, f32),
            jax.ShapeDtypeStruct((rows // CHUNK, width, width), bf16),
            jax.ShapeDtypeStruct((copies, width, width), bf16),
        ],
        compiler_params=pltpu.CompilerParams(
            dimension_semantics=("arbitrary",), vmem_limit_bytes=50 * 2**20
        ),
        name="state_maps",
    )(place, same, other, w, spike, vec)


def conv_kernel(place_ref, same_ref, other_ref, w_ref, halo_ref, vec_ref, q_ref, out_ref, tail_ref):
    width = vec_ref.shape[1]

    def project(x, first, last):
        out = jnp.dot(x, w_ref[:, first * width : last * width], preferred_element_type=f32)
        return out.astype(bf16)

    @pl.when(pl.program_id(0) == 0)
    def _():
        two = project(halo_ref[...], 1, 3).astype(f32)
        tail_ref[...] = two[:, :width] * two[:, width:]

    x = own_block(place_ref, same_ref, other_ref)
    two = project(x, 0, 2)
    q_ref[...] = two[:, :width]
    rest = project(x, 2, 4).astype(f32)
    prod, post = two[:, width:].astype(f32) * rest[:, :width], rest[:, width:]
    rows = prod.shape[0]
    tail = tail_ref[...]
    row = rows_of((rows, width))
    last, before = tail[-1:], tail[-2:-1]
    one = jnp.where(row == 0, last, pltpu.roll(prod, 1, 0))
    two = jnp.where(row == 0, before, jnp.where(row == 1, last, pltpu.roll(prod, 2, 0)))
    filtered = vec_ref[2:3] * two + vec_ref[3:4] * one + vec_ref[4:5] * prod
    out_ref[...] = (post * filtered).astype(bf16)
    tail_ref[...] = prod[rows - tail_ref.shape[0] :]


def conv_call(place, same, other, w, halo, vec):
    rows, width = same.shape[0] * same.shape[1] * 2, vec.shape[1]
    depth = w.shape[0]
    tile = pl.BlockSpec((BLOCK, width), lambda i, p: (i, 0))
    whole = lambda a: pl.BlockSpec(a.shape, lambda i, p: (0,) * a.ndim)
    return pl.pallas_call(
        conv_kernel,
        grid_spec=pltpu.PrefetchScalarGridSpec(
            num_scalar_prefetch=1,
            grid=(rows // BLOCK,),
            in_specs=token_specs(same)
            + [pl.BlockSpec((depth, 4 * width), lambda i, p: (0, 1)), whole(halo), whole(vec)],
            out_specs=[tile, tile],
            scratch_shapes=[pltpu.VMEM((halo.shape[0], width), f32)],
        ),
        out_shape=[jax.ShapeDtypeStruct((rows, width), bf16)] * 2,
        compiler_params=pltpu.CompilerParams(
            dimension_semantics=("arbitrary",), vmem_limit_bytes=40 * 2**20
        ),
        name="conv_mix",
    )(place, same, other, w, halo, vec)


def reads_kernel(q_ref, gk_ref, gb_ref, wu_ref, v_ref, pos_ref, full_ref, states_ref, o_ref, y_ref):
    width = 2 * HEAD_WIDTH
    each = range(BLOCK // CHUNK)
    t, s, _ = chunk_masks()
    inclusive = t >= s
    fold = functools.partial(spread, first=first_lanes())
    q_all = q_ref[...].astype(f32)
    ask, full = cut(q_all * pos_ref[...]), cut(q_all * full_ref[...])
    gk, gb, wu, v = map(cut, (gk_ref[...], gb_ref[...], wu_ref[...], v_ref[...]))
    grams = [dot(ask[k], jnp.concatenate([fold(gk[k]), fold(gb[k])], axis=0), 1, 1) for k in each]
    key_read = [jnp.where(inclusive, g[:, :width], 0.0) for g in grams]
    beta_read = [jnp.where(inclusive, g[:, width:], 0.0) for g in grams]
    forward = [dot(key_read[k], fold(v[k])) for k in each]
    back = [
        dot(beta_read[k], jnp.concatenate([fold(wu[k][:, :width]), fold(wu[k][:, width:])], axis=1))
        for k in each
    ]
    for k in each:
        start = states_ref[k]
        got = dot(
            full[k] - back[k][:, :width],
            jnp.concatenate([fold(start[:HEAD_WIDTH]), fold(start[HEAD_WIDTH:])], axis=0),
            1,
            1,
        )
        at = slice(k * CHUNK, (k + 1) * CHUNK)
        o_ref[at] = forward[k] - back[k][:, width:] + got[:, :width]
        y_ref[at] = got[:, width:].astype(bf16)


def reads_call(q, gk, gb, wu, v, pos, full, states):
    rows, width = q.shape
    tile = pl.BlockSpec((BLOCK, width), lambda i: (i, 0))
    wide = pl.BlockSpec((BLOCK, 2 * width), lambda i: (i, 0))
    starts = pl.BlockSpec((BLOCK // CHUNK, width, width), lambda i: (i, 0, 0))
    return pl.pallas_call(
        reads_kernel,
        grid=(rows // BLOCK,),
        in_specs=[tile, tile, tile, wide, tile, tile, tile, starts],
        out_specs=[tile, tile],
        out_shape=[jax.ShapeDtypeStruct((rows, width), f32), jax.ShapeDtypeStruct((rows, width), bf16)],
        compiler_params=pltpu.CompilerParams(
            dimension_semantics=("arbitrary",), vmem_limit_bytes=40 * 2**20
        ),
        name="local_reads",
    )(q, gk, gb, wu, v, pos, full, states)


def moved(state, piece, first):
    hi = state.astype(bf16)
    lo = (state - hi.astype(f32)).astype(bf16)
    got = dot(jnp.concatenate([hi, lo], axis=0), spread(piece[HEAD_WIDTH:], first))
    return got[: state.shape[0]] + got[state.shape[0] :]


def group_kernel(pieces_ref, out_ref):
    first = first_lanes()
    total = pieces_ref[0].astype(f32)
    for k in range(1, pieces_ref.shape[0]):
        piece = pieces_ref[k]
        total = moved(total, piece, first)
        total = jnp.concatenate(
            [total[:HEAD_WIDTH] + piece[:HEAD_WIDTH].astype(f32), total[HEAD_WIDTH:]], axis=0
        )
    for k in range(out_ref.shape[0]):
        out_ref[k] = total.astype(bf16)


def finish_kernel(at_ref, near_ref, far_ref, init_ref, o_ref, y_ref, conv_ref, vec_ref, out_ref, s_ref):
    width = 2 * HEAD_WIDTH
    first = first_lanes()

    @pl.when(pl.program_id(0) == 0)
    def _():
        def through(ref):
            def advance(i, state):
                piece = ref[i]
                return moved(state, piece, first) + piece[:HEAD_WIDTH].astype(f32)

            return advance

        state = lax.fori_loop(0, at_ref[0], through(far_ref), init_ref[...])
        state = lax.fori_loop(0, at_ref[1], through(near_ref), state)
        s_ref[...] = spread(state, first)

    low = lanes_of((BLOCK, width)) < HEAD_WIDTH
    reads = o_ref[...] + dot(y_ref[...], s_ref[...], 1, 1)
    centered = reads - head_sums(reads, low) * (1.0 / HEAD_WIDTH)
    variance = head_sums(centered * centered, low) * (1.0 / HEAD_WIDTH)
    mixed = centered * lax.rsqrt(variance + HEAD_WIDTH * 1e-05) * vec_ref[5:6]
    out_ref[:, :width] = conv_ref[...]
    out_ref[:, width:] = mixed.astype(bf16)


def finish_call(at, near, far, init, o, y, conv, vec):
    rows, width = o.shape
    whole = lambda a: pl.BlockSpec(a.shape, lambda i, p: (0,) * a.ndim)
    tile = pl.BlockSpec((BLOCK, width), lambda i, p: (i, 0))
    return pl.pallas_call(
        finish_kernel,
        grid_spec=pltpu.PrefetchScalarGridSpec(
            num_scalar_prefetch=1,
            grid=(rows // BLOCK,),
            in_specs=[whole(near), whole(far), whole(init), tile, tile, tile, whole(vec)],
            out_specs=pl.BlockSpec((BLOCK, 2 * width), lambda i, p: (i, 0)),
            scratch_shapes=[pltpu.VMEM((width, width), bf16)],
        ),
        out_shape=jax.ShapeDtypeStruct((rows, 2 * width), bf16),
        compiler_params=pltpu.CompilerParams(
            dimension_semantics=("arbitrary",), vmem_limit_bytes=50 * 2**20
        ),
        name="finish_mix",
    )(at, near, far, init, o, y, conv, vec)


def outward_kernel(pick_ref, m_ref, *refs):
    *weights, keep_ref, give_ref = refs
    total = None
    for k, w_ref in enumerate(weights):
        got = dot(m_ref[pick_ref[1 + k]], w_ref[...])
        total = got if total is None else total + got
    total = total.astype(bf16)
    rows = keep_ref.shape[0]
    first = pick_ref[0] == 0
    keep_ref[...] = jnp.where(first, total[:rows], total[rows:])
    give_ref[...] = jnp.where(first, total[rows:], total[:rows])


def outward_call(pick, gathered, weights):
    _, rows, depth = gathered.shape
    columns = weights[0].shape[1]
    step = 512
    tile = pl.BlockSpec((rows // 2, step), lambda i, p: (0, i))
    return pl.pallas_call(
        outward_kernel,
        grid_spec=pltpu.PrefetchScalarGridSpec(
            num_scalar_prefetch=1,
            grid=(columns // step,),
            in_specs=[pl.BlockSpec(gathered.shape, lambda i, p: (0, 0, 0))]
            + [pl.BlockSpec((depth, step), lambda i, p: (0, i)) for _ in weights],
            out_specs=[tile, tile],
        ),
        out_shape=[jax.ShapeDtypeStruct((rows // 2, columns), bf16)] * 2,
        compiler_params=pltpu.CompilerParams(dimension_semantics=("arbitrary",)),
        name="outward",
    )(pick, gathered, *weights)


def pack_kernel(*refs):
    *parts, out_ref = refs
    for k, ref in enumerate(parts):
        width = ref.shape[1]
        for n in range(out_ref.shape[0]):
            out_ref[n, :, k * width : (k + 1) * width] = ref[...]


def packed(copies, *shards):
    rows, width = shards[0].shape
    return pl.pallas_call(
        pack_kernel,
        out_shape=jax.ShapeDtypeStruct((copies, rows, len(shards) * width), bf16),
        name="pack_shards",
    )(*shards)


def passed_along(block, axis, distance):
    devices = range(lax.axis_size(axis))
    route = [(i - distance, i) for i in devices if i - distance in devices]
    return lax.ppermute(block, axis, route)


def turned(x, distance):
    devices = lax.axis_size("tp")
    return lax.ppermute(x, "tp", [(i, (i + distance) % devices) for i in range(devices)])


def from_everyone(copies, axis, groups=None):
    return lax.all_to_all(copies, axis, 0, 0, tiled=True, axis_index_groups=groups)


def rms_rows(activations, gain_vector):
    values = activations.astype(f32)
    inv_scale = lax.rsqrt(jnp.mean(values * values, axis=-1, keepdims=True) + norm_eps)
    return (values * inv_scale * gain_vector).astype(bf16)


def mixing(
    tokens,
    input_norm_gain,
    earlier_gate,
    later_gate,
    convolution_input,
    convolution_taps,
    receptance,
    key_matrix,
    value_matrix,
    decay_matrix,
    rate_matrix,
    decay_floor,
    rate_offset,
    decay_spike,
    initial_state,
    head_norm_gain,
    convolution_output,
    state_heads_output,
):
    channels = earlier_gate.shape[1]
    heads = channels // HEAD_WIDTH
    devices = lax.axis_size("tp")
    chips = devices // 2
    me = lax.axis_index("tp").astype(jnp.int32)
    chip, core = lax.shift_right_logical(me, 1), me & 1

    def core_swap(x):
        return lax.ppermute(x, "tp", [(i, i ^ 1) for i in range(devices)])

    blocks, seqs = lax.axis_size("sp"), lax.axis_size("fs")
    weights = from_everyone(
        packed(
            seqs,
            key_matrix,
            value_matrix,
            decay_matrix,
            rate_matrix,
            receptance,
            earlier_gate,
            convolution_input,
            later_gate,
        ),
        "fs",
    )
    weights = weights.reshape(-1, 8 * channels)
    weights = lax.all_gather(weights, "sp", axis=0, tiled=True)
    outer = from_everyone(packed(blocks, convolution_output.T, state_heads_output.T), "sp")
    outer = from_everyone(jnp.broadcast_to(outer[None], (seqs, *outer.shape)), "fs")
    outer = jnp.swapaxes(outer, 0, 1).reshape(-1, 2 * channels).T

    normed = rms_rows(tokens[0], input_norm_gain)
    behind, ahead = turned(normed, 2), turned(normed, -2)
    cut = normed.shape[0] // 2
    far = turned(behind[:cut], 2), turned(ahead[cut:], -2)
    same = jnp.stack([normed, ahead, jnp.concatenate(far, axis=0), behind])
    other = core_swap(same)

    before, after = turned(outer, 2), turned(outer, -2)
    far = turned(before[:channels], 2), turned(after[channels:], -2)
    across = jnp.concatenate(far, axis=0)
    vec = jnp.concatenate(
        [
            decay_floor[None],
            rate_offset[None],
            convolution_taps,
            head_norm_gain[None],
            jnp.zeros((2, channels), f32),
        ],
        axis=0,
    )
    place = jnp.stack([chip, core])
    last_rows = jnp.where(core == 0, other[:, -16:], same[:, -16:])
    last_rows = lax.dynamic_index_in_dim(last_rows, (chips - 1 - chip) & (chips - 1), 0, keepdims=False)
    halo = passed_along(last_rows, "sp", 1)
    few = 4
    near_blocks = [list(range(k, k + few)) for k in range(0, blocks, few)]
    far_blocks = [list(range(k, blocks, few)) for k in range(few)]
    *kept, agg = maps_call(place, same, other, weights, decay_spike[0], vec, few)
    near_maps = from_everyone(agg, "sp", near_blocks)
    q, conv = conv_call(place, same, other, weights, halo, vec)
    total = pl.pallas_call(
        group_kernel,
        out_shape=jax.ShapeDtypeStruct((blocks // few, *agg.shape[1:]), bf16),
        name="group_map",
    )(near_maps)
    far_maps = from_everyone(total, "sp", far_blocks)
    o, y = reads_call(q, *kept)
    init = jnp.moveaxis(initial_state[0], 0, 1).reshape(HEAD_WIDTH, heads * HEAD_WIDTH)
    block = lax.axis_index("sp").astype(jnp.int32)
    at = jnp.stack([lax.shift_right_logical(block, 2), block & (few - 1)])
    mixed = finish_call(at, near_maps, far_maps, init, o, y, conv, vec)
    groups = [list(range(side, devices, 2)) for side in range(2)]
    gathered = lax.all_to_all(
        mixed.reshape(chips, -1, 2 * channels), "tp", 0, 0, tiled=True, axis_index_groups=groups
    )
    near = [(chip + k) & (chips - 1) for k in (0, chips - 1, 1, 2)]
    kept, given = outward_call(jnp.stack([core, *near]), gathered, (outer, before, after, across))
    taken = core_swap(given)
    return (kept.astype(f32) + taken.astype(f32)).astype(bf16)[None]


def solution(mesh):
    placed = (
        P("fs", ("sp", "tp"), None),
        P(),
        P(("sp", "fs"), "tp"),
        P(("sp", "fs"), "tp"),
        P(("sp", "fs"), "tp"),
        P(None, "tp"),
        P(("sp", "fs"), "tp"),
        P(("sp", "fs"), "tp"),
        P(("sp", "fs"), "tp"),
        P(("sp", "fs"), "tp"),
        P(("sp", "fs"), "tp"),
        P("tp"),
        P("tp"),
        P("fs", "sp", "tp"),
        P("fs", "tp", None, None),
        P("tp"),
        P("tp", ("sp", "fs")),
        P("tp", ("sp", "fs")),
    )
    return jax.shard_map(
        mixing,
        mesh=mesh,
        in_specs=placed,
        out_specs=P("fs", ("sp", "tp"), None),
        check_vma=False,
    )
```

```python
import functools

import jax
import jax.numpy as jnp
from jax import lax
from jax.experimental import pallas as pl
from jax.experimental.pallas import tpu as pltpu
from jax.sharding import PartitionSpec as P


HEAD_WIDTH = 64
CHUNK = 64
BLOCK = 256
MAPS_BLOCK = 512
norm_eps = 1e-06
key_eps = 1e-06
f32, bf16 = jnp.float32, jnp.bfloat16


def array(shape, dtype):
    return pltpu.HBM(tuple(shape), dtype)


def in_hbm(*arrays):
    return [pltpu.with_memory_space_constraint(a, pltpu.HBM) for a in arrays]


def dot(a, b, ca=1, cb=0):
    return lax.dot_general(
        a.astype(bf16), b.astype(bf16), (((ca,), (cb,)), ((), ())), preferred_element_type=f32
    )


def lanes_of(shape):
    return lax.broadcasted_iota(jnp.int32, shape, 1)


def rows_of(shape):
    return lax.broadcasted_iota(jnp.int32, shape, 0)


def spread(z, first):
    z = z.astype(bf16)
    return jnp.concatenate([z * first, z * (1 - first)], axis=0)


def head_sums(z, low):
    a = jnp.sum(jnp.where(low, z, 0.0), axis=1, keepdims=True)
    b = jnp.sum(jnp.where(low, 0.0, z), axis=1, keepdims=True)
    return jnp.where(low, a, b)


def own_block(place_ref, *token_refs):
    low_core = place_ref[1] == 0
    rows = []
    for k in range(0, len(token_refs), 2):
        mine, theirs = token_refs[k][0], token_refs[k + 1][0]
        rows += [jnp.where(low_core, mine, theirs), jnp.where(low_core, theirs, mine)]
    return jnp.concatenate(rows, axis=0)


def chunk_masks():
    shape = (CHUNK, 2 * HEAD_WIDTH)
    return rows_of(shape), lanes_of(shape) % HEAD_WIDTH, lanes_of(shape) < HEAD_WIDTH


def first_lanes():
    return jnp.where(lanes_of((1, 2 * HEAD_WIDTH)) < HEAD_WIDTH, 1.0, 0.0).astype(bf16)


def cut(a):
    return [a[k * CHUNK : (k + 1) * CHUNK] for k in range(a.shape[0] // CHUNK)]


def maps_kernel(place_ref, *refs):
    *token_refs, w_ref, spike_ref, vec_ref = refs[:-9]
    gk_ref, gb_ref, wu_ref, v_ref, pos_ref, full_ref, states_ref, agg_ref, st_ref = refs[-9:]
    step = pl.program_id(0)
    width = 2 * HEAD_WIDTH
    each = range(MAPS_BLOCK // CHUNK)

    @pl.when(step == 0)
    def _():
        r, l = rows_of((width, width)), lanes_of((width, width))
        eye = (r - HEAD_WIDTH == l % HEAD_WIDTH) & (r >= HEAD_WIDTH)
        st_ref[...] = jnp.where(eye, 1.0, 0.0).astype(f32)

    x = own_block(place_ref, *token_refs)

    def section(k):
        two = jnp.dot(x, w_ref[:, 2 * k * width : 2 * (k + 1) * width], preferred_element_type=f32)
        two = two.astype(bf16)
        return two[:, :width], two[:, width:]

    dpre, rpre = (a.astype(f32) for a in section(1))
    keys, vals = section(0)
    v_ref[...] = vals
    keys = keys.astype(f32)

    low = lanes_of((MAPS_BLOCK, width)) < HEAD_WIDTH
    logd = spike_ref[...] - jnp.exp(vec_ref[0:1] + jnp.tanh(dpre))
    rate = jax.nn.sigmoid(vec_ref[1:2] + rpre)
    unit = keys * lax.rsqrt(head_sums(keys * keys, low) + key_eps)
    beta = rate * unit
    r, c = rows_of((BLOCK, BLOCK)), lanes_of((BLOCK, BLOCK))
    tri = jnp.where((r >= c) & (r // CHUNK == c // CHUNK), 1.0, 0.0).astype(bf16)
    hi = logd.astype(bf16)
    rest = logd - hi.astype(f32)
    mid = rest.astype(bf16)
    lo = (rest - mid.astype(f32)).astype(bf16)
    terms = jnp.concatenate([hi, mid, lo], axis=1)
    sums = jnp.concatenate(
        [
            jnp.dot(tri, terms[k : k + BLOCK], preferred_element_type=f32)
            for k in range(0, MAPS_BLOCK, BLOCK)
        ],
        axis=0,
    )
    cum_all = sums[:, :width] + sums[:, width : 2 * width] + sums[:, 2 * width :]
    prev_all = cum_all - logd

    t, s, low_c = chunk_masks()
    strict = t > s
    fold = functools.partial(spread, first=first_lanes())
    same = (rows_of((width, width)) // HEAD_WIDTH) == (lanes_of((width, width)) // HEAD_WIDTH)

    keys, vals, unit, beta, cum, prev = map(cut, (keys, vals, unit, beta, cum_all, prev_all))
    center = [cum[k][CHUNK // 2 : CHUNK // 2 + 1] for k in each]
    close = [cum[k][CHUNK - 1 : CHUNK] for k in each]
    e_neg = [jnp.exp(center[k] - cum[k]) for k in each]
    ask_k = [unit[k] * jnp.exp(prev[k] - center[k]) for k in each]
    give_k = [keys[k] * e_neg[k] for k in each]
    give_b = [beta[k] * e_neg[k] for k in each]
    e_center = [jnp.exp(center[k]) for k in each]
    e_tail = [jnp.exp(close[k] - center[k]) for k in each]
    e_close = [jnp.exp(close[k]) for k in each]
    grams = [dot(ask_k[k], jnp.concatenate([fold(give_k[k]), fold(give_b[k])], axis=0), 1, 1) for k in each]
    key_ask = [jnp.where(strict, g[:, :width], 0.0) for g in grams]
    beta_ask = [jnp.where(strict, g[:, width:], 0.0) for g in grams]
    asked = [dot(key_ask[k], fold(vals[k])) for k in each]

    inv = [jnp.where(t == s, 1.0, jnp.where(t // 2 == s // 2, -beta_ask[k], 0.0)) for k in each]
    size = 2
    while size < CHUNK:
        here = (t // (2 * size) == s // (2 * size)) & (t // size != s // size)
        mixed = [dot(inv[k], fold(jnp.where(here, beta_ask[k], 0.0))) for k in each]
        inv = [inv[k] - dot(mixed[k], fold(inv[k])) for k in each]
        size *= 2

    wu = [
        dot(inv[k], jnp.concatenate([fold(ask_k[k] * e_center[k]), fold(asked[k])], axis=1))
        for k in each
    ]
    outer = [dot(wu[k], give_b[k] * e_tail[k], 0, 0) for k in each]
    outer_v = [dot(vals[k], give_k[k] * e_tail[k], 0, 0) for k in each]
    step_map = [jnp.where(same, -outer[k][:width], 0.0).astype(bf16) for k in each]
    source_full = [outer_v[k] - outer[k][width:] for k in each]
    source = [jnp.where(low_c, f[:HEAD_WIDTH], f[HEAD_WIDTH:]) for f in source_full]

    state = st_ref[...]
    for k in each:
        rounded = state.astype(bf16)
        states_ref[k] = rounded
        state = state * e_close[k] + dot(rounded, step_map[k])
        state = jnp.concatenate([state[:HEAD_WIDTH] + source[k], state[HEAD_WIDTH:]], axis=0)
    st_ref[...] = state

    for k in each:
        at = slice(k * CHUNK, (k + 1) * CHUNK)
        gk_ref[at] = give_k[k].astype(bf16)
        gb_ref[at] = give_b[k].astype(bf16)
        wu_ref[at] = wu[k].astype(bf16)
        pos_ref[at] = jnp.exp(cum[k] - center[k])
        full_ref[at] = jnp.exp(cum[k])

    @pl.when(step == pl.num_programs(0) - 1)
    def _():
        for k in range(agg_ref.shape[0]):
            agg_ref[k] = state.astype(bf16)


def token_specs(same, pairs=1):
    chips, part, depth = same.shape
    specs = []
    for k in range(pairs):
        place = lambda i, p, k=k: ((pairs * i + k - p[0]) & (chips - 1), 0, 0)
        specs += [pl.BlockSpec((1, part, depth), place)] * 2
    return specs


def maps_call(place, same, other, w, spike, vec, copies):
    rows, width = spike.shape
    depth = w.shape[0]
    tile = pl.BlockSpec((MAPS_BLOCK, width), lambda i, p: (i, 0))
    wide = pl.BlockSpec((MAPS_BLOCK, 2 * width), lambda i, p: (i, 0))
    pairs = MAPS_BLOCK // CHUNK
    like = lambda n, t: array((rows, n), t)
    return pl.pallas_call(
        maps_kernel,
        grid_spec=pltpu.PrefetchScalarGridSpec(
            num_scalar_prefetch=1,
            grid=(rows // MAPS_BLOCK,),
            in_specs=token_specs(same, MAPS_BLOCK // BLOCK)
            + [
                pl.BlockSpec((depth, 4 * width), lambda i, p: (0, 0)),
                tile,
                pl.BlockSpec(vec.shape, lambda i, p: (0, 0)),
            ],
            out_specs=[
                tile,
                tile,
                wide,
                tile,
                tile,
                tile,
                pl.BlockSpec((pairs, width, width), lambda i, p: (i, 0, 0)),
                pl.BlockSpec((copies, width, width), lambda i, p: (0, 0, 0)),
            ],
            scratch_shapes=[pltpu.VMEM((width, width), f32)],
        ),
        out_shape=[
            like(width, bf16),
            like(width, bf16),
            like(2 * width, bf16),
            like(width, bf16),
            like(width, f32),
            like(width, f32),
            array((rows // CHUNK, width, width), bf16),
            array((copies, width, width), bf16),
        ],
        compiler_params=pltpu.CompilerParams(
            dimension_semantics=("arbitrary",), vmem_limit_bytes=28 * 2**20
        ),
        name="state_maps",
    )(place, *(in_hbm(same, other) * (MAPS_BLOCK // BLOCK)), *in_hbm(w), spike, vec)


def conv_kernel(place_ref, same_ref, other_ref, w_ref, halo_ref, vec_ref, q_ref, out_ref, tail_ref):
    width = vec_ref.shape[1]

    def project(x, first, last):
        out = jnp.dot(x, w_ref[:, first * width : last * width], preferred_element_type=f32)
        return out.astype(bf16)

    @pl.when(pl.program_id(0) == 0)
    def _():
        two = project(halo_ref[...], 1, 3).astype(f32)
        tail_ref[...] = two[:, :width] * two[:, width:]

    x = own_block(place_ref, same_ref, other_ref)
    two = project(x, 0, 2)
    q_ref[...] = two[:, :width]
    rest = project(x, 2, 4).astype(f32)
    prod, post = two[:, width:].astype(f32) * rest[:, :width], rest[:, width:]
    rows = prod.shape[0]
    tail = tail_ref[...]
    row = rows_of((rows, width))
    last, before = tail[-1:], tail[-2:-1]
    one = jnp.where(row == 0, last, pltpu.roll(prod, 1, 0))
    two = jnp.where(row == 0, before, jnp.where(row == 1, last, pltpu.roll(prod, 2, 0)))
    filtered = vec_ref[2:3] * two + vec_ref[3:4] * one + vec_ref[4:5] * prod
    out_ref[...] = (post * filtered).astype(bf16)
    tail_ref[...] = prod[rows - tail_ref.shape[0] :]


def conv_call(place, same, other, w, halo, vec):
    rows, width = same.shape[0] * same.shape[1] * 2, vec.shape[1]
    depth = w.shape[0]
    tile = pl.BlockSpec((BLOCK, width), lambda i, p: (i, 0))
    whole = lambda a: pl.BlockSpec(a.shape, lambda i, p: (0,) * a.ndim)
    return pl.pallas_call(
        conv_kernel,
        grid_spec=pltpu.PrefetchScalarGridSpec(
            num_scalar_prefetch=1,
            grid=(rows // BLOCK,),
            in_specs=token_specs(same)
            + [pl.BlockSpec((depth, 4 * width), lambda i, p: (0, 1)), whole(halo), whole(vec)],
            out_specs=[tile, tile],
            scratch_shapes=[pltpu.VMEM((halo.shape[0], width), f32)],
        ),
        out_shape=[array((rows, width), bf16)] * 2,
        compiler_params=pltpu.CompilerParams(
            dimension_semantics=("arbitrary",), vmem_limit_bytes=20 * 2**20
        ),
        name="conv_mix",
    )(place, *in_hbm(same, other, w), halo, vec)


def reads_kernel(q_ref, gk_ref, gb_ref, wu_ref, v_ref, pos_ref, full_ref, states_ref, o_ref, y_ref):
    width = 2 * HEAD_WIDTH
    each = range(BLOCK // CHUNK)
    t, s, _ = chunk_masks()
    inclusive = t >= s
    fold = functools.partial(spread, first=first_lanes())
    q_all = q_ref[...].astype(f32)
    ask, full = cut(q_all * pos_ref[...]), cut(q_all * full_ref[...])
    gk, gb, wu, v = map(cut, (gk_ref[...], gb_ref[...], wu_ref[...], v_ref[...]))
    grams = [dot(ask[k], jnp.concatenate([fold(gk[k]), fold(gb[k])], axis=0), 1, 1) for k in each]
    key_read = [jnp.where(inclusive, g[:, :width], 0.0) for g in grams]
    beta_read = [jnp.where(inclusive, g[:, width:], 0.0) for g in grams]
    forward = [dot(key_read[k], fold(v[k])) for k in each]
    back = [
        dot(beta_read[k], jnp.concatenate([fold(wu[k][:, :width]), fold(wu[k][:, width:])], axis=1))
        for k in each
    ]
    for k in each:
        start = states_ref[k]
        got = dot(
            full[k] - back[k][:, :width],
            jnp.concatenate([fold(start[:HEAD_WIDTH]), fold(start[HEAD_WIDTH:])], axis=0),
            1,
            1,
        )
        at = slice(k * CHUNK, (k + 1) * CHUNK)
        o_ref[at] = forward[k] - back[k][:, width:] + got[:, :width]
        y_ref[at] = got[:, width:].astype(bf16)


def reads_call(q, gk, gb, wu, v, pos, full, states):
    rows, width = q.shape
    tile = pl.BlockSpec((BLOCK, width), lambda i: (i, 0))
    wide = pl.BlockSpec((BLOCK, 2 * width), lambda i: (i, 0))
    starts = pl.BlockSpec((BLOCK // CHUNK, width, width), lambda i: (i, 0, 0))
    return pl.pallas_call(
        reads_kernel,
        grid=(rows // BLOCK,),
        in_specs=[tile, tile, tile, wide, tile, tile, tile, starts],
        out_specs=[tile, tile],
        out_shape=[array((rows, width), f32), array((rows, width), bf16)],
        compiler_params=pltpu.CompilerParams(
            dimension_semantics=("arbitrary",), vmem_limit_bytes=20 * 2**20
        ),
        name="local_reads",
    )(*in_hbm(q, gk, gb, wu, v, pos, full, states))


def moved(state, piece, first):
    hi = state.astype(bf16)
    lo = (state - hi.astype(f32)).astype(bf16)
    got = dot(jnp.concatenate([hi, lo], axis=0), spread(piece[HEAD_WIDTH:], first))
    return got[: state.shape[0]] + got[state.shape[0] :]


def group_kernel(pieces_ref, out_ref):
    first = first_lanes()
    total = pieces_ref[0].astype(f32)
    for k in range(1, pieces_ref.shape[0]):
        piece = pieces_ref[k]
        total = moved(total, piece, first)
        total = jnp.concatenate(
            [total[:HEAD_WIDTH] + piece[:HEAD_WIDTH].astype(f32), total[HEAD_WIDTH:]], axis=0
        )
    for k in range(out_ref.shape[0]):
        out_ref[k] = total.astype(bf16)


def finish_kernel(at_ref, near_ref, far_ref, init_ref, o_ref, y_ref, conv_ref, vec_ref, out_ref, s_ref):
    width = 2 * HEAD_WIDTH
    first = first_lanes()

    @pl.when(pl.program_id(0) == 0)
    def _():
        def through(ref):
            def advance(i, state):
                piece = ref[i]
                return moved(state, piece, first) + piece[:HEAD_WIDTH].astype(f32)

            return advance

        state = lax.fori_loop(0, at_ref[0], through(far_ref), init_ref[...])
        state = lax.fori_loop(0, at_ref[1], through(near_ref), state)
        s_ref[...] = spread(state, first)

    low = lanes_of((BLOCK, width)) < HEAD_WIDTH
    reads = o_ref[...] + dot(y_ref[...], s_ref[...], 1, 1)
    centered = reads - head_sums(reads, low) * (1.0 / HEAD_WIDTH)
    variance = head_sums(centered * centered, low) * (1.0 / HEAD_WIDTH)
    mixed = centered * lax.rsqrt(variance + HEAD_WIDTH * 1e-05) * vec_ref[5:6]
    out_ref[:, :width] = conv_ref[...]
    out_ref[:, width:] = mixed.astype(bf16)


def finish_call(at, near, far, init, o, y, conv, vec):
    rows, width = o.shape
    whole = lambda a: pl.BlockSpec(a.shape, lambda i, p: (0,) * a.ndim)
    tile = pl.BlockSpec((BLOCK, width), lambda i, p: (i, 0))
    return pl.pallas_call(
        finish_kernel,
        grid_spec=pltpu.PrefetchScalarGridSpec(
            num_scalar_prefetch=1,
            grid=(rows // BLOCK,),
            in_specs=[whole(near), whole(far), whole(init), tile, tile, tile, whole(vec)],
            out_specs=pl.BlockSpec((BLOCK, 2 * width), lambda i, p: (i, 0)),
            scratch_shapes=[pltpu.VMEM((width, width), bf16)],
        ),
        out_shape=array((rows, 2 * width), bf16),
        compiler_params=pltpu.CompilerParams(
            dimension_semantics=("arbitrary",), vmem_limit_bytes=12 * 2**20
        ),
        name="finish_mix",
    )(at, near, far, init, *in_hbm(o, y, conv), vec)


def outward_kernel(pick_ref, m_ref, *refs):
    *weights, keep_ref, give_ref = refs
    rows, columns = keep_ref.shape
    first = pick_ref[0] == 0
    step = 512
    for at in range(0, columns, step):
        total = None
        for k, w_ref in enumerate(weights):
            got = dot(m_ref[pick_ref[1 + k]], w_ref[:, at : at + step])
            total = got if total is None else total + got
        total = total.astype(bf16)
        keep_ref[:, at : at + step] = jnp.where(first, total[:rows], total[rows:])
        give_ref[:, at : at + step] = jnp.where(first, total[rows:], total[:rows])


def outward_call(pick, gathered, weights):
    rows, columns = gathered.shape[1] // 2, weights[0].shape[1]
    here = pl.BlockSpec(memory_space=pltpu.VMEM)
    return pl.pallas_call(
        outward_kernel,
        in_specs=[pl.BlockSpec(memory_space=pltpu.SMEM)] + [here] * (1 + len(weights)),
        out_specs=[here, here],
        out_shape=[jax.ShapeDtypeStruct((rows, columns), bf16)] * 2,
        compiler_params=pltpu.CompilerParams(vmem_limit_bytes=24 * 2**20),
        name="outward",
    )(pick, gathered, *weights)


def pack_kernel(*refs):
    *parts, out_ref = refs
    for k, ref in enumerate(parts):
        width = ref.shape[1]
        for n in range(out_ref.shape[0]):
            out_ref[n, :, k * width : (k + 1) * width] = ref[...]


def packed(copies, *shards):
    rows, width = shards[0].shape
    return pl.pallas_call(
        pack_kernel,
        out_shape=jax.ShapeDtypeStruct((copies, rows, len(shards) * width), bf16),
        name="pack_shards",
    )(*shards)


def passed_along(block, axis, distance):
    devices = range(lax.axis_size(axis))
    route = [(i - distance, i) for i in devices if i - distance in devices]
    return lax.ppermute(block, axis, route)


def turned(x, distance):
    devices = lax.axis_size("tp")
    return lax.ppermute(x, "tp", [(i, (i + distance) % devices) for i in range(devices)])


def from_everyone(copies, axis, groups=None):
    return lax.all_to_all(copies, axis, 0, 0, tiled=True, axis_index_groups=groups)


def rms_rows(activations, gain_vector):
    values = activations.astype(f32)
    inv_scale = lax.rsqrt(jnp.mean(values * values, axis=-1, keepdims=True) + norm_eps)
    return (values * inv_scale * gain_vector).astype(bf16)


def mixing(
    tokens,
    input_norm_gain,
    earlier_gate,
    later_gate,
    convolution_input,
    convolution_taps,
    receptance,
    key_matrix,
    value_matrix,
    decay_matrix,
    rate_matrix,
    decay_floor,
    rate_offset,
    decay_spike,
    initial_state,
    head_norm_gain,
    convolution_output,
    state_heads_output,
):
    channels = earlier_gate.shape[1]
    heads = channels // HEAD_WIDTH
    devices = lax.axis_size("tp")
    chips = devices // 2
    me = lax.axis_index("tp").astype(jnp.int32)
    chip, core = lax.shift_right_logical(me, 1), me & 1

    def core_swap(x):
        return lax.ppermute(x, "tp", [(i, i ^ 1) for i in range(devices)])

    blocks, seqs = lax.axis_size("sp"), lax.axis_size("fs")
    weights = from_everyone(
        packed(
            seqs,
            key_matrix,
            value_matrix,
            decay_matrix,
            rate_matrix,
            receptance,
            earlier_gate,
            convolution_input,
            later_gate,
        ),
        "fs",
    )
    weights = weights.reshape(-1, 8 * channels)
    weights = lax.all_gather(weights, "sp", axis=0, tiled=True)
    outer = from_everyone(packed(blocks, convolution_output.T, state_heads_output.T), "sp")
    outer = from_everyone(jnp.broadcast_to(outer[None], (seqs, *outer.shape)), "fs")
    outer = jnp.swapaxes(outer, 0, 1).reshape(-1, 2 * channels).T

    normed = rms_rows(tokens[0], input_norm_gain)
    others = [turned(normed, -2), turned(normed, 4), turned(normed, 2)]
    same = jnp.stack([normed, *others])
    other = core_swap(same)
    after, across, before = [turned(outer, k) for k in (-2, 4, 2)]
    vec = jnp.concatenate(
        [
            decay_floor[None],
            rate_offset[None],
            convolution_taps,
            head_norm_gain[None],
            jnp.zeros((2, channels), f32),
        ],
        axis=0,
    )
    place = jnp.stack([chip, core])
    last_rows = jnp.where(core == 0, other[:, -16:], same[:, -16:])
    last_rows = lax.dynamic_index_in_dim(last_rows, (chips - 1 - chip) & (chips - 1), 0, keepdims=False)
    halo = passed_along(last_rows, "sp", 1)
    few = 4
    near_blocks = [list(range(k, k + few)) for k in range(0, blocks, few)]
    far_blocks = [list(range(k, blocks, few)) for k in range(few)]
    *kept, agg = maps_call(place, same, other, weights, decay_spike[0], vec, few)
    near_maps = from_everyone(agg, "sp", near_blocks)
    q, conv = conv_call(place, same, other, weights, halo, vec)
    total = pl.pallas_call(
        group_kernel,
        out_shape=array((blocks // few, *agg.shape[1:]), bf16),
        name="group_map",
    )(near_maps)
    far_maps = from_everyone(total, "sp", far_blocks)
    o, y = reads_call(q, *kept)
    init = jnp.moveaxis(initial_state[0], 0, 1).reshape(HEAD_WIDTH, heads * HEAD_WIDTH)
    block = lax.axis_index("sp").astype(jnp.int32)
    at = jnp.stack([lax.shift_right_logical(block, 2), block & (few - 1)])
    mixed = finish_call(at, near_maps, far_maps, init, o, y, conv, vec)
    groups = [list(range(side, devices, 2)) for side in range(2)]
    gathered = lax.all_to_all(
        mixed.reshape(chips, -1, 2 * channels), "tp", 0, 0, tiled=True, axis_index_groups=groups
    )
    near = [(chip + k) & (chips - 1) for k in (0, 1, 2, chips - 1)]
    kept, given = outward_call(jnp.stack([core, *near]), gathered, (outer, after, across, before))
    taken = core_swap(given)
    return (kept.astype(f32) + taken.astype(f32)).astype(bf16)[None]


def solution(mesh):
    placed = (
        P("fs", ("sp", "tp"), None),
        P(),
        P(("sp", "fs"), "tp"),
        P(("sp", "fs"), "tp"),
        P(("sp", "fs"), "tp"),
        P(None, "tp"),
        P(("sp", "fs"), "tp"),
        P(("sp", "fs"), "tp"),
        P(("sp", "fs"), "tp"),
        P(("sp", "fs"), "tp"),
        P(("sp", "fs"), "tp"),
        P("tp"),
        P("tp"),
        P("fs", "sp", "tp"),
        P("fs", "tp", None, None),
        P("tp"),
        P("tp", ("sp", "fs")),
        P("tp", ("sp", "fs")),
    )
    return jax.shard_map(
        mixing,
        mesh=mesh,
        in_specs=placed,
        out_specs=P("fs", ("sp", "tp"), None),
        check_vma=False,
    )
```

```python
import functools

import jax
import jax.numpy as jnp
from jax import lax
from jax.experimental import pallas as pl
from jax.experimental.pallas import tpu as pltpu
from jax.sharding import PartitionSpec as P


HEAD_WIDTH = 64
CHUNK = 64
BLOCK = 256
MAPS_BLOCK = 512
norm_eps = 1e-06
key_eps = 1e-06
f32, bf16 = jnp.float32, jnp.bfloat16


def array(shape, dtype):
    return pltpu.HBM(tuple(shape), dtype)


def in_hbm(*arrays):
    return [pltpu.with_memory_space_constraint(a, pltpu.HBM) for a in arrays]


def dot(a, b, ca=1, cb=0):
    return lax.dot_general(
        a.astype(bf16), b.astype(bf16), (((ca,), (cb,)), ((), ())), preferred_element_type=f32
    )


def lanes_of(shape):
    return lax.broadcasted_iota(jnp.int32, shape, 1)


def rows_of(shape):
    return lax.broadcasted_iota(jnp.int32, shape, 0)


def spread(z, first):
    z = z.astype(bf16)
    return jnp.concatenate([z * first, z * (1 - first)], axis=0)


def head_sums(z, low):
    a = jnp.sum(jnp.where(low, z, 0.0), axis=1, keepdims=True)
    b = jnp.sum(jnp.where(low, 0.0, z), axis=1, keepdims=True)
    return jnp.where(low, a, b)


def own_block(place_ref, *token_refs):
    low_core = place_ref[1] == 0
    rows = []
    for k in range(0, len(token_refs), 2):
        mine, theirs = token_refs[k][0], token_refs[k + 1][0]
        rows += [jnp.where(low_core, mine, theirs), jnp.where(low_core, theirs, mine)]
    return jnp.concatenate(rows, axis=0)


def chunk_masks():
    shape = (CHUNK, 2 * HEAD_WIDTH)
    return rows_of(shape), lanes_of(shape) % HEAD_WIDTH, lanes_of(shape) < HEAD_WIDTH


def first_lanes():
    return jnp.where(lanes_of((1, 2 * HEAD_WIDTH)) < HEAD_WIDTH, 1.0, 0.0).astype(bf16)


def cut(a):
    return [a[k * CHUNK : (k + 1) * CHUNK] for k in range(a.shape[0] // CHUNK)]


def maps_kernel(place_ref, *refs):
    *token_refs, w_ref, spike_ref, vec_ref = refs[:-9]
    gk_ref, gb_ref, wu_ref, v_ref, pos_ref, full_ref, states_ref, agg_ref, st_ref = refs[-9:]
    step = pl.program_id(0)
    width = 2 * HEAD_WIDTH
    each = range(MAPS_BLOCK // CHUNK)

    @pl.when(step == 0)
    def _():
        r, l = rows_of((width, width)), lanes_of((width, width))
        eye = (r - HEAD_WIDTH == l % HEAD_WIDTH) & (r >= HEAD_WIDTH)
        st_ref[...] = jnp.where(eye, 1.0, 0.0).astype(f32)

    x = own_block(place_ref, *token_refs)

    def section(k):
        two = jnp.dot(x, w_ref[:, 2 * k * width : 2 * (k + 1) * width], preferred_element_type=f32)
        two = two.astype(bf16)
        return two[:, :width], two[:, width:]

    dpre, rpre = (a.astype(f32) for a in section(1))
    keys, vals = section(0)
    v_ref[...] = vals
    keys = keys.astype(f32)

    low = lanes_of((MAPS_BLOCK, width)) < HEAD_WIDTH
    logd = spike_ref[...] - jnp.exp(vec_ref[0:1] + jnp.tanh(dpre))
    rate = jax.nn.sigmoid(vec_ref[1:2] + rpre)
    unit = keys * lax.rsqrt(head_sums(keys * keys, low) + key_eps)
    beta = rate * unit
    r, c = rows_of((BLOCK, BLOCK)), lanes_of((BLOCK, BLOCK))
    tri = jnp.where((r >= c) & (r // CHUNK == c // CHUNK), 1.0, 0.0).astype(bf16)
    hi = logd.astype(bf16)
    rest = logd - hi.astype(f32)
    mid = rest.astype(bf16)
    lo = (rest - mid.astype(f32)).astype(bf16)
    terms = jnp.concatenate([hi, mid, lo], axis=1)
    sums = jnp.concatenate(
        [
            jnp.dot(tri, terms[k : k + BLOCK], preferred_element_type=f32)
            for k in range(0, MAPS_BLOCK, BLOCK)
        ],
        axis=0,
    )
    cum_all = sums[:, :width] + sums[:, width : 2 * width] + sums[:, 2 * width :]
    prev_all = cum_all - logd

    t, s, low_c = chunk_masks()
    strict = t > s
    fold = functools.partial(spread, first=first_lanes())
    same = (rows_of((width, width)) // HEAD_WIDTH) == (lanes_of((width, width)) // HEAD_WIDTH)

    keys, vals, unit, beta, cum, prev = map(cut, (keys, vals, unit, beta, cum_all, prev_all))
    center = [cum[k][CHUNK // 2 : CHUNK // 2 + 1] for k in each]
    close = [cum[k][CHUNK - 1 : CHUNK] for k in each]
    e_neg = [jnp.exp(center[k] - cum[k]) for k in each]
    ask_k = [unit[k] * jnp.exp(prev[k] - center[k]) for k in each]
    give_k = [keys[k] * e_neg[k] for k in each]
    give_b = [beta[k] * e_neg[k] for k in each]
    e_center = [jnp.exp(center[k]) for k in each]
    e_tail = [jnp.exp(close[k] - center[k]) for k in each]
    e_close = [jnp.exp(close[k]) for k in each]
    grams = [dot(ask_k[k], jnp.concatenate([fold(give_k[k]), fold(give_b[k])], axis=0), 1, 1) for k in each]
    key_ask = [jnp.where(strict, g[:, :width], 0.0) for g in grams]
    beta_ask = [jnp.where(strict, g[:, width:], 0.0) for g in grams]
    asked = [dot(key_ask[k], fold(vals[k])) for k in each]

    inv = [jnp.where(t == s, 1.0, jnp.where(t // 2 == s // 2, -beta_ask[k], 0.0)) for k in each]
    size = 2
    while size < CHUNK:
        here = (t // (2 * size) == s // (2 * size)) & (t // size != s // size)
        mixed = [dot(inv[k], fold(jnp.where(here, beta_ask[k], 0.0))) for k in each]
        inv = [inv[k] - dot(mixed[k], fold(inv[k])) for k in each]
        size *= 2

    wu = [
        dot(inv[k], jnp.concatenate([fold(ask_k[k] * e_center[k]), fold(asked[k])], axis=1))
        for k in each
    ]
    outer = [dot(wu[k], give_b[k] * e_tail[k], 0, 0) for k in each]
    outer_v = [dot(vals[k], give_k[k] * e_tail[k], 0, 0) for k in each]
    step_map = [jnp.where(same, -outer[k][:width], 0.0).astype(bf16) for k in each]
    source_full = [outer_v[k] - outer[k][width:] for k in each]
    source = [jnp.where(low_c, f[:HEAD_WIDTH], f[HEAD_WIDTH:]) for f in source_full]

    state = st_ref[...]
    for k in each:
        rounded = state.astype(bf16)
        states_ref[k] = rounded
        state = state * e_close[k] + dot(rounded, step_map[k])
        state = jnp.concatenate([state[:HEAD_WIDTH] + source[k], state[HEAD_WIDTH:]], axis=0)
    st_ref[...] = state

    for k in each:
        at = slice(k * CHUNK, (k + 1) * CHUNK)
        gk_ref[at] = give_k[k].astype(bf16)
        gb_ref[at] = give_b[k].astype(bf16)
        wu_ref[at] = wu[k].astype(bf16)
        pos_ref[at] = jnp.exp(cum[k] - center[k])
        full_ref[at] = jnp.exp(cum[k])

    @pl.when(step == pl.num_programs(0) - 1)
    def _():
        for k in range(agg_ref.shape[0]):
            agg_ref[k] = state.astype(bf16)


def token_specs(same, pairs=1):
    chips, part, depth = same.shape
    specs = []
    for k in range(pairs):
        place = lambda i, p, k=k: ((pairs * i + k - p[0]) & (chips - 1), 0, 0)
        specs += [pl.BlockSpec((1, part, depth), place)] * 2
    return specs


def maps_call(place, same, other, w, spike, vec, copies):
    rows, width = spike.shape
    depth = w.shape[0]
    tile = pl.BlockSpec((MAPS_BLOCK, width), lambda i, p: (i, 0))
    wide = pl.BlockSpec((MAPS_BLOCK, 2 * width), lambda i, p: (i, 0))
    pairs = MAPS_BLOCK // CHUNK
    like = lambda n, t: array((rows, n), t)
    return pl.pallas_call(
        maps_kernel,
        grid_spec=pltpu.PrefetchScalarGridSpec(
            num_scalar_prefetch=1,
            grid=(rows // MAPS_BLOCK,),
            in_specs=token_specs(same, MAPS_BLOCK // BLOCK)
            + [
                pl.BlockSpec((depth, 4 * width), lambda i, p: (0, 0)),
                tile,
                pl.BlockSpec(vec.shape, lambda i, p: (0, 0)),
            ],
            out_specs=[
                tile,
                tile,
                wide,
                tile,
                tile,
                tile,
                pl.BlockSpec((pairs, width, width), lambda i, p: (i, 0, 0)),
                pl.BlockSpec((copies, width, width), lambda i, p: (0, 0, 0)),
            ],
            scratch_shapes=[pltpu.VMEM((width, width), f32)],
        ),
        out_shape=[
            like(width, bf16),
            like(width, bf16),
            like(2 * width, bf16),
            like(width, bf16),
            like(width, f32),
            like(width, f32),
            array((rows // CHUNK, width, width), bf16),
            array((copies, width, width), bf16),
        ],
        compiler_params=pltpu.CompilerParams(
            dimension_semantics=("arbitrary",), vmem_limit_bytes=28 * 2**20
        ),
        name="state_maps",
    )(place, *(in_hbm(same, other) * (MAPS_BLOCK // BLOCK)), *in_hbm(w), spike, vec)


def conv_kernel(place_ref, same_ref, other_ref, w_ref, halo_ref, vec_ref, q_ref, out_ref, tail_ref):
    width = vec_ref.shape[1]

    def project(x, first, last):
        out = jnp.dot(x, w_ref[:, first * width : last * width], preferred_element_type=f32)
        return out.astype(bf16)

    @pl.when(pl.program_id(0) == 0)
    def _():
        two = project(halo_ref[...], 1, 3).astype(f32)
        tail_ref[...] = two[:, :width] * two[:, width:]

    x = own_block(place_ref, same_ref, other_ref)
    two = project(x, 0, 2)
    q_ref[...] = two[:, :width]
    rest = project(x, 2, 4).astype(f32)
    prod, post = two[:, width:].astype(f32) * rest[:, :width], rest[:, width:]
    rows = prod.shape[0]
    tail = tail_ref[...]
    row = rows_of((rows, width))
    last, before = tail[-1:], tail[-2:-1]
    one = jnp.where(row == 0, last, pltpu.roll(prod, 1, 0))
    two = jnp.where(row == 0, before, jnp.where(row == 1, last, pltpu.roll(prod, 2, 0)))
    filtered = vec_ref[2:3] * two + vec_ref[3:4] * one + vec_ref[4:5] * prod
    out_ref[...] = (post * filtered).astype(bf16)
    tail_ref[...] = prod[rows - tail_ref.shape[0] :]


def conv_call(place, same, other, w, halo, vec):
    rows, width = same.shape[0] * same.shape[1] * 2, vec.shape[1]
    depth = w.shape[0]
    tile = pl.BlockSpec((BLOCK, width), lambda i, p: (i, 0))
    whole = lambda a: pl.BlockSpec(a.shape, lambda i, p: (0,) * a.ndim)
    return pl.pallas_call(
        conv_kernel,
        grid_spec=pltpu.PrefetchScalarGridSpec(
            num_scalar_prefetch=1,
            grid=(rows // BLOCK,),
            in_specs=token_specs(same)
            + [pl.BlockSpec((depth, 4 * width), lambda i, p: (0, 1)), whole(halo), whole(vec)],
            out_specs=[tile, tile],
            scratch_shapes=[pltpu.VMEM((halo.shape[0], width), f32)],
        ),
        out_shape=[array((rows, width), bf16)] * 2,
        compiler_params=pltpu.CompilerParams(
            dimension_semantics=("arbitrary",), vmem_limit_bytes=20 * 2**20
        ),
        name="conv_mix",
    )(place, *in_hbm(same, other, w), halo, vec)


def reads_kernel(q_ref, gk_ref, gb_ref, wu_ref, v_ref, pos_ref, full_ref, states_ref, o_ref, y_ref):
    width = 2 * HEAD_WIDTH
    each = range(MAPS_BLOCK // CHUNK)
    t, s, _ = chunk_masks()
    inclusive = t >= s
    fold = functools.partial(spread, first=first_lanes())
    q_all = q_ref[...].astype(f32)
    ask, full = cut(q_all * pos_ref[...]), cut(q_all * full_ref[...])
    gk, gb, wu, v = map(cut, (gk_ref[...], gb_ref[...], wu_ref[...], v_ref[...]))
    grams = [dot(ask[k], jnp.concatenate([fold(gk[k]), fold(gb[k])], axis=0), 1, 1) for k in each]
    key_read = [jnp.where(inclusive, g[:, :width], 0.0) for g in grams]
    beta_read = [jnp.where(inclusive, g[:, width:], 0.0) for g in grams]
    forward = [dot(key_read[k], fold(v[k])) for k in each]
    back = [
        dot(beta_read[k], jnp.concatenate([fold(wu[k][:, :width]), fold(wu[k][:, width:])], axis=1))
        for k in each
    ]
    for k in each:
        start = states_ref[k]
        got = dot(
            full[k] - back[k][:, :width],
            jnp.concatenate([fold(start[:HEAD_WIDTH]), fold(start[HEAD_WIDTH:])], axis=0),
            1,
            1,
        )
        at = slice(k * CHUNK, (k + 1) * CHUNK)
        o_ref[at] = forward[k] - back[k][:, width:] + got[:, :width]
        y_ref[at] = got[:, width:].astype(bf16)


def reads_call(q, gk, gb, wu, v, pos, full, states):
    rows, width = q.shape
    tile = pl.BlockSpec((MAPS_BLOCK, width), lambda i: (i, 0))
    wide = pl.BlockSpec((MAPS_BLOCK, 2 * width), lambda i: (i, 0))
    starts = pl.BlockSpec((MAPS_BLOCK // CHUNK, width, width), lambda i: (i, 0, 0))
    return pl.pallas_call(
        reads_kernel,
        grid=(rows // MAPS_BLOCK,),
        in_specs=[tile, tile, tile, wide, tile, tile, tile, starts],
        out_specs=[tile, tile],
        out_shape=[array((rows, width), f32), array((rows, width), bf16)],
        compiler_params=pltpu.CompilerParams(
            dimension_semantics=("arbitrary",), vmem_limit_bytes=20 * 2**20
        ),
        name="local_reads",
    )(*in_hbm(q, gk, gb, wu, v, pos, full, states))


def moved(state, piece, first):
    hi = state.astype(bf16)
    lo = (state - hi.astype(f32)).astype(bf16)
    got = dot(jnp.concatenate([hi, lo], axis=0), spread(piece[HEAD_WIDTH:], first))
    return got[: state.shape[0]] + got[state.shape[0] :]


def group_kernel(at_ref, pieces_ref, out_ref, before_ref):
    first = first_lanes()

    def join(total, k):
        piece = pieces_ref[k]
        total = moved(total, piece, first)
        source = total[:HEAD_WIDTH] + piece[:HEAD_WIDTH].astype(f32)
        return jnp.concatenate([source, total[HEAD_WIDTH:]], axis=0)

    total = pieces_ref[0].astype(f32)
    r, l = rows_of(total.shape), lanes_of(total.shape) % HEAD_WIDTH
    before = jnp.where(r - HEAD_WIDTH == l, 1.0, 0.0)
    for k in range(1, pieces_ref.shape[0]):
        before = jnp.where(at_ref[1] == k, total, before)
        total = join(total, k)
    before_ref[...] = before
    for k in range(out_ref.shape[0]):
        out_ref[k] = total.astype(bf16)


def group_call(at, pieces, copies):
    here = pl.BlockSpec(memory_space=pltpu.VMEM)
    return pl.pallas_call(
        group_kernel,
        in_specs=[pl.BlockSpec(memory_space=pltpu.SMEM), here],
        out_specs=[here, here],
        out_shape=[
            jax.ShapeDtypeStruct((copies, *pieces.shape[1:]), bf16),
            jax.ShapeDtypeStruct(pieces.shape[1:], f32),
        ],
        name="group_map",
    )(at, pieces)


def finish_kernel(at_ref, before_ref, far_ref, init_ref, o_ref, y_ref, conv_ref, vec_ref, out_ref, s_ref):
    width = 2 * HEAD_WIDTH
    first = first_lanes()

    @pl.when(pl.program_id(0) == 0)
    def _():
        def advance(i, state):
            piece = far_ref[i]
            return moved(state, piece, first) + piece[:HEAD_WIDTH].astype(f32)

        state = lax.fori_loop(0, at_ref[0], advance, init_ref[...])
        before = before_ref[...]
        state = moved(state, before, first) + before[:HEAD_WIDTH]
        s_ref[...] = spread(state, first)

    low = lanes_of((MAPS_BLOCK, width)) < HEAD_WIDTH
    reads = o_ref[...] + dot(y_ref[...], s_ref[...], 1, 1)
    centered = reads - head_sums(reads, low) * (1.0 / HEAD_WIDTH)
    variance = head_sums(centered * centered, low) * (1.0 / HEAD_WIDTH)
    mixed = centered * lax.rsqrt(variance + HEAD_WIDTH * 1e-05) * vec_ref[5:6]
    out_ref[:, :width] = conv_ref[...]
    out_ref[:, width:] = mixed.astype(bf16)


def finish_call(at, before, far, init, o, y, conv, vec):
    rows, width = o.shape
    whole = lambda a: pl.BlockSpec(a.shape, lambda i, p: (0,) * a.ndim)
    tile = pl.BlockSpec((MAPS_BLOCK, width), lambda i, p: (i, 0))
    return pl.pallas_call(
        finish_kernel,
        grid_spec=pltpu.PrefetchScalarGridSpec(
            num_scalar_prefetch=1,
            grid=(rows // MAPS_BLOCK,),
            in_specs=[whole(before), whole(far), whole(init), tile, tile, tile, whole(vec)],
            out_specs=pl.BlockSpec((MAPS_BLOCK, 2 * width), lambda i, p: (i, 0)),
            scratch_shapes=[pltpu.VMEM((width, width), bf16)],
        ),
        out_shape=array((rows, 2 * width), bf16),
        compiler_params=pltpu.CompilerParams(
            dimension_semantics=("arbitrary",), vmem_limit_bytes=12 * 2**20
        ),
        name="finish_mix",
    )(at, before, far, init, *in_hbm(o, y, conv), vec)


def outward_kernel(pick_ref, m_ref, *refs):
    *weights, keep_ref, give_ref = refs
    rows, columns = keep_ref.shape
    first = pick_ref[0] == 0
    step = 512
    for at in range(0, columns, step):
        total = None
        for k, w_ref in enumerate(weights):
            got = dot(m_ref[pick_ref[1 + k]], w_ref[:, at : at + step])
            total = got if total is None else total + got
        total = total.astype(bf16)
        keep_ref[:, at : at + step] = jnp.where(first, total[:rows], total[rows:])
        give_ref[:, at : at + step] = jnp.where(first, total[rows:], total[:rows])


def outward_call(pick, gathered, weights):
    rows, columns = gathered.shape[1] // 2, weights[0].shape[1]
    here = pl.BlockSpec(memory_space=pltpu.VMEM)
    return pl.pallas_call(
        outward_kernel,
        in_specs=[pl.BlockSpec(memory_space=pltpu.SMEM)] + [here] * (1 + len(weights)),
        out_specs=[here, here],
        out_shape=[jax.ShapeDtypeStruct((rows, columns), bf16)] * 2,
        compiler_params=pltpu.CompilerParams(vmem_limit_bytes=24 * 2**20),
        name="outward",
    )(pick, gathered, *weights)


def pack_kernel(*refs):
    *parts, out_ref = refs
    for k, ref in enumerate(parts):
        width = ref.shape[1]
        for n in range(out_ref.shape[0]):
            out_ref[n, :, k * width : (k + 1) * width] = ref[...]


def packed(copies, *shards):
    rows, width = shards[0].shape
    return pl.pallas_call(
        pack_kernel,
        out_shape=jax.ShapeDtypeStruct((copies, rows, len(shards) * width), bf16),
        name="pack_shards",
    )(*shards)


def passed_along(block, axis, distance):
    devices = range(lax.axis_size(axis))
    route = [(i - distance, i) for i in devices if i - distance in devices]
    return lax.ppermute(block, axis, route)


def turned(x, distance):
    devices = lax.axis_size("tp")
    return lax.ppermute(x, "tp", [(i, (i + distance) % devices) for i in range(devices)])


def from_everyone(copies, axis, groups=None):
    return lax.all_to_all(copies, axis, 0, 0, tiled=True, axis_index_groups=groups)


def rms_rows(activations, gain_vector):
    values = activations.astype(f32)
    inv_scale = lax.rsqrt(jnp.mean(values * values, axis=-1, keepdims=True) + norm_eps)
    return (values * inv_scale * gain_vector).astype(bf16)


def mixing(
    tokens,
    input_norm_gain,
    earlier_gate,
    later_gate,
    convolution_input,
    convolution_taps,
    receptance,
    key_matrix,
    value_matrix,
    decay_matrix,
    rate_matrix,
    decay_floor,
    rate_offset,
    decay_spike,
    initial_state,
    head_norm_gain,
    convolution_output,
    state_heads_output,
):
    channels = earlier_gate.shape[1]
    heads = channels // HEAD_WIDTH
    devices = lax.axis_size("tp")
    chips = devices // 2
    me = lax.axis_index("tp").astype(jnp.int32)
    chip, core = lax.shift_right_logical(me, 1), me & 1

    def core_swap(x):
        return lax.ppermute(x, "tp", [(i, i ^ 1) for i in range(devices)])

    blocks, seqs = lax.axis_size("sp"), lax.axis_size("fs")
    weights = from_everyone(
        packed(
            seqs,
            key_matrix,
            value_matrix,
            decay_matrix,
            rate_matrix,
            receptance,
            earlier_gate,
            convolution_input,
            later_gate,
        ),
        "fs",
    )
    weights = weights.reshape(-1, 8 * channels)
    weights = lax.all_gather(weights, "sp", axis=0, tiled=True)
    outer = from_everyone(packed(blocks, convolution_output.T, state_heads_output.T), "sp")
    outer = from_everyone(jnp.broadcast_to(outer[None], (seqs, *outer.shape)), "fs")
    outer = jnp.swapaxes(outer, 0, 1).reshape(-1, 2 * channels).T

    normed = rms_rows(tokens[0], input_norm_gain)
    others = [turned(normed, -2), turned(normed, 4), turned(normed, 2)]
    same = jnp.stack([normed, *others])
    other = core_swap(same)
    after, across, before = [turned(outer, k) for k in (-2, 4, 2)]
    vec = jnp.concatenate(
        [
            decay_floor[None],
            rate_offset[None],
            convolution_taps,
            head_norm_gain[None],
            jnp.zeros((2, channels), f32),
        ],
        axis=0,
    )
    place = jnp.stack([chip, core])
    last_rows = jnp.where(core == 0, other[:, -16:], same[:, -16:])
    last_rows = lax.dynamic_index_in_dim(last_rows, (chips - 1 - chip) & (chips - 1), 0, keepdims=False)
    halo = passed_along(last_rows, "sp", 1)
    few = 4
    near_blocks = [list(range(k, k + few)) for k in range(0, blocks, few)]
    far_blocks = [list(range(k, blocks, few)) for k in range(few)]
    *kept, agg = maps_call(place, same, other, weights, decay_spike[0], vec, few)
    near_maps = from_everyone(agg, "sp", near_blocks)
    block = lax.axis_index("sp").astype(jnp.int32)
    at = jnp.stack([lax.shift_right_logical(block, 2), block & (few - 1)])
    total, earlier = group_call(at, near_maps, blocks // few)
    far_maps = from_everyone(total, "sp", far_blocks)
    q, conv = conv_call(place, same, other, weights, halo, vec)
    o, y = reads_call(q, *kept)
    init = jnp.moveaxis(initial_state[0], 0, 1).reshape(HEAD_WIDTH, heads * HEAD_WIDTH)
    mixed = finish_call(at, earlier, far_maps, init, o, y, conv, vec)
    groups = [list(range(side, devices, 2)) for side in range(2)]
    gathered = lax.all_to_all(
        mixed.reshape(chips, -1, 2 * channels), "tp", 0, 0, tiled=True, axis_index_groups=groups
    )
    near = [(chip + k) & (chips - 1) for k in (0, 1, 2, chips - 1)]
    kept, given = outward_call(jnp.stack([core, *near]), gathered, (outer, after, across, before))
    taken = core_swap(given)
    return (kept.astype(f32) + taken.astype(f32)).astype(bf16)[None]


def solution(mesh):
    placed = (
        P("fs", ("sp", "tp"), None),
        P(),
        P(("sp", "fs"), "tp"),
        P(("sp", "fs"), "tp"),
        P(("sp", "fs"), "tp"),
        P(None, "tp"),
        P(("sp", "fs"), "tp"),
        P(("sp", "fs"), "tp"),
        P(("sp", "fs"), "tp"),
        P(("sp", "fs"), "tp"),
        P(("sp", "fs"), "tp"),
        P("tp"),
        P("tp"),
        P("fs", "sp", "tp"),
        P("fs", "tp", None, None),
        P("tp"),
        P("tp", ("sp", "fs")),
        P("tp", ("sp", "fs")),
    )
    return jax.shard_map(
        mixing,
        mesh=mesh,
        in_specs=placed,
        out_specs=P("fs", ("sp", "tp"), None),
        check_vma=False,
    )
```

```python
import functools

import jax
import jax.numpy as jnp
from jax import lax
from jax.experimental import pallas as pl
from jax.experimental.pallas import tpu as pltpu
from jax.sharding import PartitionSpec as P


HEAD_WIDTH = 64
CHUNK = 64
BLOCK = 256
MAPS_BLOCK = 1024
READS_BLOCK = 512
CONV_BLOCK = 1024
norm_eps = 1e-06
key_eps = 1e-06
f32, bf16 = jnp.float32, jnp.bfloat16


def array(shape, dtype):
    return pltpu.HBM(tuple(shape), dtype)


def in_hbm(*arrays):
    return [pltpu.with_memory_space_constraint(a, pltpu.HBM) for a in arrays]


def dot(a, b, ca=1, cb=0):
    return lax.dot_general(
        a.astype(bf16), b.astype(bf16), (((ca,), (cb,)), ((), ())), preferred_element_type=f32
    )


def lanes_of(shape):
    return lax.broadcasted_iota(jnp.int32, shape, 1)


def rows_of(shape):
    return lax.broadcasted_iota(jnp.int32, shape, 0)


def spread(z, first):
    z = z.astype(bf16)
    return jnp.concatenate([z * first, z * (1 - first)], axis=0)


def head_sums(z, low):
    a = jnp.sum(jnp.where(low, z, 0.0), axis=1, keepdims=True)
    b = jnp.sum(jnp.where(low, 0.0, z), axis=1, keepdims=True)
    return jnp.where(low, a, b)


def own_block(place_ref, same_ref, other_ref, first, pairs=1):
    chips = same_ref.shape[0]
    low_core = place_ref[1] == 0
    rows = []
    for k in range(pairs):
        at = (first + k - place_ref[0]) & (chips - 1)
        mine, theirs = same_ref[at], other_ref[at]
        rows += [jnp.where(low_core, mine, theirs), jnp.where(low_core, theirs, mine)]
    return jnp.concatenate(rows, axis=0)


def chunk_masks():
    shape = (CHUNK, 2 * HEAD_WIDTH)
    return rows_of(shape), lanes_of(shape) % HEAD_WIDTH, lanes_of(shape) < HEAD_WIDTH


def first_lanes():
    return jnp.where(lanes_of((1, 2 * HEAD_WIDTH)) < HEAD_WIDTH, 1.0, 0.0).astype(bf16)


def cut(a):
    return [a[k * CHUNK : (k + 1) * CHUNK] for k in range(a.shape[0] // CHUNK)]


def maps_kernel(
    place_ref,
    same_ref,
    other_ref,
    w_ref,
    spike_ref,
    vec_ref,
    gk_ref,
    gb_ref,
    wu_ref,
    v_ref,
    pos_ref,
    full_ref,
    states_ref,
    agg_ref,
    st_ref,
):
    step = pl.program_id(0)
    width = 2 * HEAD_WIDTH
    each = range(MAPS_BLOCK // CHUNK)

    @pl.when(step == 0)
    def _():
        r, l = rows_of((width, width)), lanes_of((width, width))
        eye = (r - HEAD_WIDTH == l % HEAD_WIDTH) & (r >= HEAD_WIDTH)
        st_ref[...] = jnp.where(eye, 1.0, 0.0).astype(f32)

    pairs = MAPS_BLOCK // BLOCK
    x = own_block(place_ref, same_ref, other_ref, step * pairs, pairs)

    def section(k):
        two = jnp.dot(x, w_ref[:, 2 * k * width : 2 * (k + 1) * width], preferred_element_type=f32)
        two = two.astype(bf16)
        return two[:, :width], two[:, width:]

    dpre, rpre = (a.astype(f32) for a in section(1))
    keys, vals = section(0)
    v_ref[...] = vals
    keys = keys.astype(f32)

    low = lanes_of((MAPS_BLOCK, width)) < HEAD_WIDTH
    logd = spike_ref[...] - jnp.exp(vec_ref[0:1] + jnp.tanh(dpre))
    rate = jax.nn.sigmoid(vec_ref[1:2] + rpre)
    unit = keys * lax.rsqrt(head_sums(keys * keys, low) + key_eps)
    beta = rate * unit
    r, c = rows_of((BLOCK, BLOCK)), lanes_of((BLOCK, BLOCK))
    tri = jnp.where((r >= c) & (r // CHUNK == c // CHUNK), 1.0, 0.0).astype(bf16)
    hi = logd.astype(bf16)
    rest = logd - hi.astype(f32)
    mid = rest.astype(bf16)
    lo = (rest - mid.astype(f32)).astype(bf16)
    terms = jnp.concatenate([hi, mid, lo], axis=1)
    sums = jnp.concatenate(
        [
            jnp.dot(tri, terms[k : k + BLOCK], preferred_element_type=f32)
            for k in range(0, MAPS_BLOCK, BLOCK)
        ],
        axis=0,
    )
    cum_all = sums[:, :width] + sums[:, width : 2 * width] + sums[:, 2 * width :]
    prev_all = cum_all - logd

    t, s, low_c = chunk_masks()
    strict = t > s
    fold = functools.partial(spread, first=first_lanes())
    same = (rows_of((width, width)) // HEAD_WIDTH) == (lanes_of((width, width)) // HEAD_WIDTH)

    keys, vals, unit, beta, cum, prev = map(cut, (keys, vals, unit, beta, cum_all, prev_all))
    center = [cum[k][CHUNK // 2 : CHUNK // 2 + 1] for k in each]
    close = [cum[k][CHUNK - 1 : CHUNK] for k in each]
    e_neg = [jnp.exp(center[k] - cum[k]) for k in each]
    ask_k = [unit[k] * jnp.exp(prev[k] - center[k]) for k in each]
    give_k = [keys[k] * e_neg[k] for k in each]
    give_b = [beta[k] * e_neg[k] for k in each]
    e_center = [jnp.exp(center[k]) for k in each]
    e_tail = [jnp.exp(close[k] - center[k]) for k in each]
    e_close = [jnp.exp(close[k]) for k in each]
    grams = [dot(ask_k[k], jnp.concatenate([fold(give_k[k]), fold(give_b[k])], axis=0), 1, 1) for k in each]
    key_ask = [jnp.where(strict, g[:, :width], 0.0) for g in grams]
    beta_ask = [jnp.where(strict, g[:, width:], 0.0) for g in grams]
    asked = [dot(key_ask[k], fold(vals[k])) for k in each]

    inv = [jnp.where(t == s, 1.0, jnp.where(t // 2 == s // 2, -beta_ask[k], 0.0)) for k in each]
    size = 2
    while size < CHUNK:
        here = (t // (2 * size) == s // (2 * size)) & (t // size != s // size)
        mixed = [dot(inv[k], fold(jnp.where(here, beta_ask[k], 0.0))) for k in each]
        inv = [inv[k] - dot(mixed[k], fold(inv[k])) for k in each]
        size *= 2

    wu = [
        dot(inv[k], jnp.concatenate([fold(ask_k[k] * e_center[k]), fold(asked[k])], axis=1))
        for k in each
    ]
    outer = [dot(wu[k], give_b[k] * e_tail[k], 0, 0) for k in each]
    outer_v = [dot(vals[k], give_k[k] * e_tail[k], 0, 0) for k in each]
    step_map = [jnp.where(same, -outer[k][:width], 0.0).astype(bf16) for k in each]
    source_full = [outer_v[k] - outer[k][width:] for k in each]
    source = [jnp.where(low_c, f[:HEAD_WIDTH], f[HEAD_WIDTH:]) for f in source_full]

    state = st_ref[...]
    for k in each:
        rounded = state.astype(bf16)
        states_ref[k] = rounded
        state = state * e_close[k] + dot(rounded, step_map[k])
        state = jnp.concatenate([state[:HEAD_WIDTH] + source[k], state[HEAD_WIDTH:]], axis=0)
    st_ref[...] = state

    for k in each:
        at = slice(k * CHUNK, (k + 1) * CHUNK)
        gk_ref[at] = give_k[k].astype(bf16)
        gb_ref[at] = give_b[k].astype(bf16)
        wu_ref[at] = wu[k].astype(bf16)
        pos_ref[at] = jnp.exp(cum[k] - center[k])
        full_ref[at] = jnp.exp(cum[k])

    @pl.when(step == pl.num_programs(0) - 1)
    def _():
        for k in range(agg_ref.shape[0]):
            agg_ref[k] = state.astype(bf16)


def token_specs():
    return [pl.BlockSpec(memory_space=pltpu.VMEM)] * 2


def maps_call(place, same, other, w, spike, vec, copies):
    rows, width = spike.shape
    depth = w.shape[0]
    tile = pl.BlockSpec((MAPS_BLOCK, width), lambda i, p: (i, 0))
    wide = pl.BlockSpec((MAPS_BLOCK, 2 * width), lambda i, p: (i, 0))
    pairs = MAPS_BLOCK // CHUNK
    like = lambda n, t: array((rows, n), t)
    return pl.pallas_call(
        maps_kernel,
        grid_spec=pltpu.PrefetchScalarGridSpec(
            num_scalar_prefetch=1,
            grid=(rows // MAPS_BLOCK,),
            in_specs=token_specs()
            + [
                pl.BlockSpec((depth, 4 * width), lambda i, p: (0, 0)),
                tile,
                pl.BlockSpec(vec.shape, lambda i, p: (0, 0)),
            ],
            out_specs=[
                tile,
                tile,
                wide,
                tile,
                tile,
                tile,
                pl.BlockSpec((pairs, width, width), lambda i, p: (i, 0, 0)),
                pl.BlockSpec((copies, width, width), lambda i, p: (0, 0, 0)),
            ],
            scratch_shapes=[pltpu.VMEM((width, width), f32)],
        ),
        out_shape=[
            like(width, bf16),
            like(width, bf16),
            like(2 * width, bf16),
            like(width, bf16),
            like(width, f32),
            like(width, f32),
            array((rows // CHUNK, width, width), bf16),
            array((copies, width, width), bf16),
        ],
        compiler_params=pltpu.CompilerParams(
            dimension_semantics=("arbitrary",), vmem_limit_bytes=28 * 2**20
        ),
        name="state_maps",
    )(place, same, other, *in_hbm(w), spike, vec)


def conv_kernel(place_ref, same_ref, other_ref, w_ref, halo_ref, vec_ref, q_ref, out_ref, tail_ref):
    width = vec_ref.shape[1]

    def project(x, first, last):
        out = jnp.dot(x, w_ref[:, first * width : last * width], preferred_element_type=f32)
        return out.astype(bf16)

    @pl.when(pl.program_id(0) == 0)
    def _():
        two = project(halo_ref[...], 1, 3).astype(f32)
        tail_ref[...] = two[:, :width] * two[:, width:]

    pairs = CONV_BLOCK // BLOCK
    x = own_block(place_ref, same_ref, other_ref, pl.program_id(0) * pairs, pairs)
    two = project(x, 0, 2)
    q_ref[...] = two[:, :width]
    rest = project(x, 2, 4).astype(f32)
    prod, post = two[:, width:].astype(f32) * rest[:, :width], rest[:, width:]
    rows = prod.shape[0]
    tail = tail_ref[...]
    row = rows_of((rows, width))
    last, before = tail[-1:], tail[-2:-1]
    one = jnp.where(row == 0, last, pltpu.roll(prod, 1, 0))
    two = jnp.where(row == 0, before, jnp.where(row == 1, last, pltpu.roll(prod, 2, 0)))
    filtered = vec_ref[2:3] * two + vec_ref[3:4] * one + vec_ref[4:5] * prod
    out_ref[...] = (post * filtered).astype(bf16)
    tail_ref[...] = prod[rows - tail_ref.shape[0] :]


def conv_call(place, same, other, w, halo, vec):
    rows, width = same.shape[0] * same.shape[1] * 2, vec.shape[1]
    depth = w.shape[0]
    tile = pl.BlockSpec((CONV_BLOCK, width), lambda i, p: (i, 0))
    whole = lambda a: pl.BlockSpec(a.shape, lambda i, p: (0,) * a.ndim)
    return pl.pallas_call(
        conv_kernel,
        grid_spec=pltpu.PrefetchScalarGridSpec(
            num_scalar_prefetch=1,
            grid=(rows // CONV_BLOCK,),
            in_specs=token_specs()
            + [pl.BlockSpec((depth, 4 * width), lambda i, p: (0, 1)), whole(halo), whole(vec)],
            out_specs=[tile, tile],
            scratch_shapes=[pltpu.VMEM((halo.shape[0], width), f32)],
        ),
        out_shape=[array((rows, width), bf16)] * 2,
        compiler_params=pltpu.CompilerParams(
            dimension_semantics=("arbitrary",), vmem_limit_bytes=20 * 2**20
        ),
        name="conv_mix",
    )(place, same, other, *in_hbm(w), halo, vec)


def reads_kernel(q_ref, gk_ref, gb_ref, wu_ref, v_ref, pos_ref, full_ref, states_ref, o_ref, y_ref):
    width = 2 * HEAD_WIDTH
    each = range(READS_BLOCK // CHUNK)
    t, s, _ = chunk_masks()
    inclusive = t >= s
    fold = functools.partial(spread, first=first_lanes())
    q_all = q_ref[...].astype(f32)
    ask, full = cut(q_all * pos_ref[...]), cut(q_all * full_ref[...])
    gk, gb, wu, v = map(cut, (gk_ref[...], gb_ref[...], wu_ref[...], v_ref[...]))
    grams = [dot(ask[k], jnp.concatenate([fold(gk[k]), fold(gb[k])], axis=0), 1, 1) for k in each]
    key_read = [jnp.where(inclusive, g[:, :width], 0.0) for g in grams]
    beta_read = [jnp.where(inclusive, g[:, width:], 0.0) for g in grams]
    forward = [dot(key_read[k], fold(v[k])) for k in each]
    back = [
        dot(beta_read[k], jnp.concatenate([fold(wu[k][:, :width]), fold(wu[k][:, width:])], axis=1))
        for k in each
    ]
    for k in each:
        start = states_ref[k]
        got = dot(
            full[k] - back[k][:, :width],
            jnp.concatenate([fold(start[:HEAD_WIDTH]), fold(start[HEAD_WIDTH:])], axis=0),
            1,
            1,
        )
        at = slice(k * CHUNK, (k + 1) * CHUNK)
        o_ref[at] = forward[k] - back[k][:, width:] + got[:, :width]
        y_ref[at] = got[:, width:].astype(bf16)


def reads_call(q, gk, gb, wu, v, pos, full, states):
    rows, width = q.shape
    tile = pl.BlockSpec((READS_BLOCK, width), lambda i: (i, 0))
    wide = pl.BlockSpec((READS_BLOCK, 2 * width), lambda i: (i, 0))
    starts = pl.BlockSpec((READS_BLOCK // CHUNK, width, width), lambda i: (i, 0, 0))
    return pl.pallas_call(
        reads_kernel,
        grid=(rows // READS_BLOCK,),
        in_specs=[tile, tile, tile, wide, tile, tile, tile, starts],
        out_specs=[tile, tile],
        out_shape=[array((rows, width), f32), array((rows, width), bf16)],
        compiler_params=pltpu.CompilerParams(
            dimension_semantics=("arbitrary",), vmem_limit_bytes=20 * 2**20
        ),
        name="local_reads",
    )(*in_hbm(q, gk, gb, wu, v, pos, full, states))


def moved(state, piece, first):
    hi = state.astype(bf16)
    lo = (state - hi.astype(f32)).astype(bf16)
    got = dot(jnp.concatenate([hi, lo], axis=0), spread(piece[HEAD_WIDTH:], first))
    return got[: state.shape[0]] + got[state.shape[0] :]


def group_kernel(at_ref, pieces_ref, out_ref, before_ref):
    first = first_lanes()

    def join(total, k):
        piece = pieces_ref[k]
        total = moved(total, piece, first)
        source = total[:HEAD_WIDTH] + piece[:HEAD_WIDTH].astype(f32)
        return jnp.concatenate([source, total[HEAD_WIDTH:]], axis=0)

    total = pieces_ref[0].astype(f32)
    r, l = rows_of(total.shape), lanes_of(total.shape) % HEAD_WIDTH
    before = jnp.where(r - HEAD_WIDTH == l, 1.0, 0.0)
    for k in range(1, pieces_ref.shape[0]):
        before = jnp.where(at_ref[1] == k, total, before)
        total = join(total, k)
    before_ref[...] = before
    for k in range(out_ref.shape[0]):
        out_ref[k] = total.astype(bf16)


def group_call(at, pieces, copies):
    here = pl.BlockSpec(memory_space=pltpu.VMEM)
    return pl.pallas_call(
        group_kernel,
        in_specs=[pl.BlockSpec(memory_space=pltpu.SMEM), here],
        out_specs=[here, here],
        out_shape=[
            jax.ShapeDtypeStruct((copies, *pieces.shape[1:]), bf16),
            jax.ShapeDtypeStruct(pieces.shape[1:], f32),
        ],
        name="group_map",
    )(at, pieces)


def finish_kernel(at_ref, before_ref, far_ref, init_ref, o_ref, y_ref, conv_ref, vec_ref, out_ref, s_ref):
    width = 2 * HEAD_WIDTH
    first = first_lanes()

    @pl.when(pl.program_id(0) == 0)
    def _():
        def advance(i, state):
            piece = far_ref[i]
            return moved(state, piece, first) + piece[:HEAD_WIDTH].astype(f32)

        state = lax.fori_loop(0, at_ref[0], advance, init_ref[...])
        before = before_ref[...]
        state = moved(state, before, first) + before[:HEAD_WIDTH]
        s_ref[...] = spread(state, first)

    low = lanes_of((READS_BLOCK, width)) < HEAD_WIDTH
    reads = o_ref[...] + dot(y_ref[...], s_ref[...], 1, 1)
    centered = reads - head_sums(reads, low) * (1.0 / HEAD_WIDTH)
    variance = head_sums(centered * centered, low) * (1.0 / HEAD_WIDTH)
    mixed = centered * lax.rsqrt(variance + HEAD_WIDTH * 1e-05) * vec_ref[5:6]
    out_ref[:, :width] = conv_ref[...]
    out_ref[:, width:] = mixed.astype(bf16)


def finish_call(at, before, far, init, o, y, conv, vec):
    rows, width = o.shape
    whole = lambda a: pl.BlockSpec(a.shape, lambda i, p: (0,) * a.ndim)
    tile = pl.BlockSpec((READS_BLOCK, width), lambda i, p: (i, 0))
    return pl.pallas_call(
        finish_kernel,
        grid_spec=pltpu.PrefetchScalarGridSpec(
            num_scalar_prefetch=1,
            grid=(rows // READS_BLOCK,),
            in_specs=[whole(before), whole(far), whole(init), tile, tile, tile, whole(vec)],
            out_specs=pl.BlockSpec((READS_BLOCK, 2 * width), lambda i, p: (i, 0)),
            scratch_shapes=[pltpu.VMEM((width, width), bf16)],
        ),
        out_shape=array((rows, 2 * width), bf16),
        compiler_params=pltpu.CompilerParams(
            dimension_semantics=("arbitrary",), vmem_limit_bytes=12 * 2**20
        ),
        name="finish_mix",
    )(at, before, far, init, *in_hbm(o, y, conv), vec)


def outward_kernel(pick_ref, m_ref, *refs):
    *weights, out_ref = refs
    rows, columns = out_ref.shape
    at = pl.multiple_of(pick_ref[0], rows)
    parts = [m_ref[pick_ref[1 + k], pl.ds(at, rows), :] for k in range(len(weights))]
    step = 512
    for first in range(0, columns, step):
        total = None
        for part, w_ref in zip(parts, weights):
            got = dot(part, w_ref[:, first : first + step])
            total = got if total is None else total + got
        out_ref[:, first : first + step] = total.astype(bf16)


def outward_call(pick, gathered, weights):
    rows, columns = gathered.shape[1] // 2, weights[0].shape[1]
    here = pl.BlockSpec(memory_space=pltpu.VMEM)
    return pl.pallas_call(
        outward_kernel,
        in_specs=[pl.BlockSpec(memory_space=pltpu.SMEM)] + [here] * (1 + len(weights)),
        out_specs=here,
        out_shape=jax.ShapeDtypeStruct((rows, columns), bf16),
        compiler_params=pltpu.CompilerParams(vmem_limit_bytes=24 * 2**20),
        name="outward",
    )(pick, gathered, *weights)


def pack_kernel(*refs):
    *parts, out_ref = refs
    for k, ref in enumerate(parts):
        width = ref.shape[1]
        for n in range(out_ref.shape[0]):
            out_ref[n, :, k * width : (k + 1) * width] = ref[...]


def packed(copies, *shards):
    rows, width = shards[0].shape
    return pl.pallas_call(
        pack_kernel,
        out_shape=jax.ShapeDtypeStruct((copies, rows, len(shards) * width), bf16),
        name="pack_shards",
    )(*shards)


def passed_along(block, axis, distance):
    devices = range(lax.axis_size(axis))
    route = [(i - distance, i) for i in devices if i - distance in devices]
    return lax.ppermute(block, axis, route)


def turned(x, distance):
    devices = lax.axis_size("tp")
    return lax.ppermute(x, "tp", [(i, (i + distance) % devices) for i in range(devices)])


def from_everyone(copies, axis, groups=None):
    return lax.all_to_all(copies, axis, 0, 0, tiled=True, axis_index_groups=groups)


def rms_rows(activations, gain_vector):
    values = activations.astype(f32)
    inv_scale = lax.rsqrt(jnp.mean(values * values, axis=-1, keepdims=True) + norm_eps)
    return (values * inv_scale * gain_vector).astype(bf16)


def mixing(
    tokens,
    input_norm_gain,
    earlier_gate,
    later_gate,
    convolution_input,
    convolution_taps,
    receptance,
    key_matrix,
    value_matrix,
    decay_matrix,
    rate_matrix,
    decay_floor,
    rate_offset,
    decay_spike,
    initial_state,
    head_norm_gain,
    convolution_output,
    state_heads_output,
):
    channels = earlier_gate.shape[1]
    heads = channels // HEAD_WIDTH
    devices = lax.axis_size("tp")
    chips = devices // 2
    me = lax.axis_index("tp").astype(jnp.int32)
    chip, core = lax.shift_right_logical(me, 1), me & 1

    def core_swap(x):
        return lax.ppermute(x, "tp", [(i, i ^ 1) for i in range(devices)])

    blocks, seqs = lax.axis_size("sp"), lax.axis_size("fs")
    weights = from_everyone(
        packed(
            seqs,
            key_matrix,
            value_matrix,
            decay_matrix,
            rate_matrix,
            receptance,
            earlier_gate,
            convolution_input,
            later_gate,
        ),
        "fs",
    )
    weights = weights.reshape(-1, 8 * channels)
    weights = lax.all_gather(weights, "sp", axis=0, tiled=True)
    outer = from_everyone(packed(blocks, convolution_output.T, state_heads_output.T), "sp")
    outer = from_everyone(jnp.broadcast_to(outer[None], (seqs, *outer.shape)), "fs")
    outer = jnp.swapaxes(outer, 0, 1).reshape(-1, 2 * channels).T

    normed = rms_rows(tokens[0], input_norm_gain)
    others = [turned(normed, -2), turned(normed, 4), turned(normed, 2)]
    same = jnp.stack([normed, *others])
    other = core_swap(same)
    after, across, before = [turned(outer, k) for k in (-2, 4, 2)]
    vec = jnp.concatenate(
        [
            decay_floor[None],
            rate_offset[None],
            convolution_taps,
            head_norm_gain[None],
            jnp.zeros((2, channels), f32),
        ],
        axis=0,
    )
    place = jnp.stack([chip, core])
    last_rows = jnp.where(core == 0, other[:, -16:], same[:, -16:])
    last_rows = lax.dynamic_index_in_dim(last_rows, (chips - 1 - chip) & (chips - 1), 0, keepdims=False)
    halo = passed_along(last_rows, "sp", 1)
    few = 4
    near_blocks = [list(range(k, k + few)) for k in range(0, blocks, few)]
    far_blocks = [list(range(k, blocks, few)) for k in range(few)]
    *kept, agg = maps_call(place, same, other, weights, decay_spike[0], vec, few)
    near_maps = from_everyone(agg, "sp", near_blocks)
    block = lax.axis_index("sp").astype(jnp.int32)
    at = jnp.stack([lax.shift_right_logical(block, 2), block & (few - 1)])
    total, earlier = group_call(at, near_maps, blocks // few)
    far_maps = from_everyone(total, "sp", far_blocks)
    q, conv = conv_call(place, same, other, weights, halo, vec)
    o, y = reads_call(q, *kept)
    init = jnp.moveaxis(initial_state[0], 0, 1).reshape(HEAD_WIDTH, heads * HEAD_WIDTH)
    mixed = finish_call(at, earlier, far_maps, init, o, y, conv, vec)
    groups = [list(range(side, devices, 2)) for side in range(2)]
    gathered = lax.all_to_all(
        mixed.reshape(chips, -1, 2 * channels), "tp", 0, 0, tiled=True, axis_index_groups=groups
    )
    near = [(chip + k) & (chips - 1) for k in (0, 1, 2, chips - 1)]
    own, ways = normed.shape[0], (outer, after, across, before)
    given = outward_call(jnp.stack([(1 - core) * own, *near]), gathered, ways)
    taken = core_swap(given)
    kept = outward_call(jnp.stack([core * own, *near]), gathered, ways)
    return (kept.astype(f32) + taken.astype(f32)).astype(bf16)[None]


def solution(mesh):
    placed = (
        P("fs", ("sp", "tp"), None),
        P(),
        P(("sp", "fs"), "tp"),
        P(("sp", "fs"), "tp"),
        P(("sp", "fs"), "tp"),
        P(None, "tp"),
        P(("sp", "fs"), "tp"),
        P(("sp", "fs"), "tp"),
        P(("sp", "fs"), "tp"),
        P(("sp", "fs"), "tp"),
        P(("sp", "fs"), "tp"),
        P("tp"),
        P("tp"),
        P("fs", "sp", "tp"),
        P("fs", "tp", None, None),
        P("tp"),
        P("tp", ("sp", "fs")),
        P("tp", ("sp", "fs")),
    )
    return jax.shard_map(
        mixing,
        mesh=mesh,
        in_specs=placed,
        out_specs=P("fs", ("sp", "tp"), None),
        check_vma=False,
    )
```

```python
import functools

import jax
import jax.numpy as jnp
from jax import lax
from jax.experimental import pallas as pl
from jax.experimental.pallas import tpu as pltpu
from jax.sharding import PartitionSpec as P


HEAD_WIDTH = 64
CHUNK = 64
BLOCK = 256
MAPS_BLOCK = 1024
READS_BLOCK = 512
CONV_BLOCK = 1024
HALO = 16
norm_eps = 1e-06
key_eps = 1e-06
f32, bf16 = jnp.float32, jnp.bfloat16


def array(shape, dtype):
    return pltpu.HBM(tuple(shape), dtype)


def in_hbm(*arrays):
    return [pltpu.with_memory_space_constraint(a, pltpu.HBM) for a in arrays]


def dot(a, b, ca=1, cb=0):
    return lax.dot_general(
        a.astype(bf16), b.astype(bf16), (((ca,), (cb,)), ((), ())), preferred_element_type=f32
    )


def lanes_of(shape):
    return lax.broadcasted_iota(jnp.int32, shape, 1)


def rows_of(shape):
    return lax.broadcasted_iota(jnp.int32, shape, 0)


def spread(z, first):
    z = z.astype(bf16)
    return jnp.concatenate([z * first, z * (1 - first)], axis=0)


def head_sums(z, low):
    a = jnp.sum(jnp.where(low, z, 0.0), axis=1, keepdims=True)
    b = jnp.sum(jnp.where(low, 0.0, z), axis=1, keepdims=True)
    return jnp.where(low, a, b)


def own_block(place_ref, same_ref, other_ref, first, pairs=1):
    chips = same_ref.shape[0]
    low_core = place_ref[1] == 0
    rows = []
    for k in range(pairs):
        at = (first + k - place_ref[0]) & (chips - 1)
        mine, theirs = same_ref[at], other_ref[at]
        rows += [jnp.where(low_core, mine, theirs), jnp.where(low_core, theirs, mine)]
    return jnp.concatenate(rows, axis=0)


def chunk_masks():
    shape = (CHUNK, 2 * HEAD_WIDTH)
    return rows_of(shape), lanes_of(shape) % HEAD_WIDTH, lanes_of(shape) < HEAD_WIDTH


def first_lanes():
    return jnp.where(lanes_of((1, 2 * HEAD_WIDTH)) < HEAD_WIDTH, 1.0, 0.0).astype(bf16)


def cut(a):
    return [a[k * CHUNK : (k + 1) * CHUNK] for k in range(a.shape[0] // CHUNK)]


def maps_kernel(
    place_ref,
    same_ref,
    other_ref,
    w_ref,
    spike_ref,
    vec_ref,
    gk_ref,
    gb_ref,
    wu_ref,
    v_ref,
    pos_ref,
    full_ref,
    states_ref,
    last_ref,
    agg_ref,
    st_ref,
):
    step = pl.program_id(0)
    width = 2 * HEAD_WIDTH
    each = range(MAPS_BLOCK // CHUNK)

    @pl.when(step == 0)
    def _():
        r, l = rows_of((width, width)), lanes_of((width, width))
        eye = (r - HEAD_WIDTH == l % HEAD_WIDTH) & (r >= HEAD_WIDTH)
        st_ref[...] = jnp.where(eye, 1.0, 0.0).astype(f32)

    pairs = MAPS_BLOCK // BLOCK
    x = own_block(place_ref, same_ref, other_ref, step * pairs, pairs)

    def section(k):
        two = jnp.dot(x, w_ref[:, 2 * k * width : 2 * (k + 1) * width], preferred_element_type=f32)
        two = two.astype(bf16)
        return two[:, :width], two[:, width:]

    dpre, rpre = (a.astype(f32) for a in section(1))
    keys, vals = section(0)
    v_ref[...] = vals
    keys = keys.astype(f32)

    low = lanes_of((MAPS_BLOCK, width)) < HEAD_WIDTH
    logd = spike_ref[...] - jnp.exp(vec_ref[0:1] + jnp.tanh(dpre))
    rate = jax.nn.sigmoid(vec_ref[1:2] + rpre)
    unit = keys * lax.rsqrt(head_sums(keys * keys, low) + key_eps)
    beta = rate * unit
    r, c = rows_of((BLOCK, BLOCK)), lanes_of((BLOCK, BLOCK))
    tri = jnp.where((r >= c) & (r // CHUNK == c // CHUNK), 1.0, 0.0).astype(bf16)
    hi = logd.astype(bf16)
    rest = logd - hi.astype(f32)
    mid = rest.astype(bf16)
    lo = (rest - mid.astype(f32)).astype(bf16)
    terms = jnp.concatenate([hi, mid, lo], axis=1)
    sums = jnp.concatenate(
        [
            jnp.dot(tri, terms[k : k + BLOCK], preferred_element_type=f32)
            for k in range(0, MAPS_BLOCK, BLOCK)
        ],
        axis=0,
    )
    cum_all = sums[:, :width] + sums[:, width : 2 * width] + sums[:, 2 * width :]
    prev_all = cum_all - logd

    t, s, low_c = chunk_masks()
    strict = t > s
    fold = functools.partial(spread, first=first_lanes())
    same = (rows_of((width, width)) // HEAD_WIDTH) == (lanes_of((width, width)) // HEAD_WIDTH)

    keys, vals, unit, beta, cum, prev = map(cut, (keys, vals, unit, beta, cum_all, prev_all))
    center = [cum[k][CHUNK // 2 : CHUNK // 2 + 1] for k in each]
    close = [cum[k][CHUNK - 1 : CHUNK] for k in each]
    e_neg = [jnp.exp(center[k] - cum[k]) for k in each]
    ask_k = [unit[k] * jnp.exp(prev[k] - center[k]) for k in each]
    give_k = [keys[k] * e_neg[k] for k in each]
    give_b = [beta[k] * e_neg[k] for k in each]
    e_center = [jnp.exp(center[k]) for k in each]
    e_tail = [jnp.exp(close[k] - center[k]) for k in each]
    e_close = [jnp.exp(close[k]) for k in each]
    grams = [dot(ask_k[k], jnp.concatenate([fold(give_k[k]), fold(give_b[k])], axis=0), 1, 1) for k in each]
    key_ask = [jnp.where(strict, g[:, :width], 0.0) for g in grams]
    beta_ask = [jnp.where(strict, g[:, width:], 0.0) for g in grams]
    asked = [dot(key_ask[k], fold(vals[k])) for k in each]

    inv = [jnp.where(t == s, 1.0, jnp.where(t // 2 == s // 2, -beta_ask[k], 0.0)) for k in each]
    size = 2
    while size < CHUNK:
        here = (t // (2 * size) == s // (2 * size)) & (t // size != s // size)
        mixed = [dot(inv[k], fold(jnp.where(here, beta_ask[k], 0.0))) for k in each]
        inv = [inv[k] - dot(mixed[k], fold(inv[k])) for k in each]
        size *= 2

    wu = [
        dot(inv[k], jnp.concatenate([fold(ask_k[k] * e_center[k]), fold(asked[k])], axis=1))
        for k in each
    ]
    outer = [dot(wu[k], give_b[k] * e_tail[k], 0, 0) for k in each]
    outer_v = [dot(vals[k], give_k[k] * e_tail[k], 0, 0) for k in each]
    step_map = [jnp.where(same, -outer[k][:width], 0.0).astype(bf16) for k in each]
    source_full = [outer_v[k] - outer[k][width:] for k in each]
    source = [jnp.where(low_c, f[:HEAD_WIDTH], f[HEAD_WIDTH:]) for f in source_full]

    state = st_ref[...]
    for k in each:
        rounded = state.astype(bf16)
        states_ref[k] = rounded
        state = state * e_close[k] + dot(rounded, step_map[k])
        state = jnp.concatenate([state[:HEAD_WIDTH] + source[k], state[HEAD_WIDTH:]], axis=0)
    st_ref[...] = state

    for k in each:
        at = slice(k * CHUNK, (k + 1) * CHUNK)
        gk_ref[at] = give_k[k].astype(bf16)
        gb_ref[at] = give_b[k].astype(bf16)
        wu_ref[at] = wu[k].astype(bf16)
        pos_ref[at] = jnp.exp(cum[k] - center[k])
        full_ref[at] = jnp.exp(cum[k])

    @pl.when(step == pl.num_programs(0) - 1)
    def _():
        last_ref[...] = x[MAPS_BLOCK - last_ref.shape[0] :]
        for k in range(agg_ref.shape[0]):
            agg_ref[k] = state.astype(bf16)


def token_specs():
    return [pl.BlockSpec(memory_space=pltpu.VMEM)] * 2


def maps_call(place, same, other, w, spike, vec, copies):
    rows, width = spike.shape
    depth = w.shape[0]
    tile = pl.BlockSpec((MAPS_BLOCK, width), lambda i, p: (i, 0))
    wide = pl.BlockSpec((MAPS_BLOCK, 2 * width), lambda i, p: (i, 0))
    pairs = MAPS_BLOCK // CHUNK
    like = lambda n, t: array((rows, n), t)
    return pl.pallas_call(
        maps_kernel,
        grid_spec=pltpu.PrefetchScalarGridSpec(
            num_scalar_prefetch=1,
            grid=(rows // MAPS_BLOCK,),
            in_specs=token_specs()
            + [
                pl.BlockSpec((depth, 4 * width), lambda i, p: (0, 0)),
                tile,
                pl.BlockSpec(vec.shape, lambda i, p: (0, 0)),
            ],
            out_specs=[
                tile,
                tile,
                wide,
                tile,
                tile,
                tile,
                pl.BlockSpec((pairs, width, width), lambda i, p: (i, 0, 0)),
                pl.BlockSpec((HALO, depth), lambda i, p: (0, 0)),
                pl.BlockSpec((copies, width, width), lambda i, p: (0, 0, 0)),
            ],
            scratch_shapes=[pltpu.VMEM((width, width), f32)],
        ),
        out_shape=[
            like(width, bf16),
            like(width, bf16),
            like(2 * width, bf16),
            like(width, bf16),
            like(width, f32),
            like(width, f32),
            array((rows // CHUNK, width, width), bf16),
            array((HALO, depth), bf16),
            array((copies, width, width), bf16),
        ],
        compiler_params=pltpu.CompilerParams(
            dimension_semantics=("arbitrary",), vmem_limit_bytes=28 * 2**20
        ),
        name="state_maps",
    )(place, same, other, *in_hbm(w, spike), vec)


def conv_kernel(place_ref, same_ref, other_ref, w_ref, halo_ref, vec_ref, q_ref, out_ref, tail_ref):
    width = vec_ref.shape[1]

    def project(x, first, last):
        out = jnp.dot(x, w_ref[:, first * width : last * width], preferred_element_type=f32)
        return out.astype(bf16)

    @pl.when(pl.program_id(0) == 0)
    def _():
        two = project(halo_ref[...], 1, 3).astype(f32)
        tail_ref[...] = two[:, :width] * two[:, width:]

    pairs = CONV_BLOCK // BLOCK
    x = own_block(place_ref, same_ref, other_ref, pl.program_id(0) * pairs, pairs)
    two = project(x, 0, 2)
    q_ref[...] = two[:, :width]
    rest = project(x, 2, 4).astype(f32)
    prod, post = two[:, width:].astype(f32) * rest[:, :width], rest[:, width:]
    rows = prod.shape[0]
    tail = tail_ref[...]
    row = rows_of((rows, width))
    last, before = tail[-1:], tail[-2:-1]
    one = jnp.where(row == 0, last, pltpu.roll(prod, 1, 0))
    two = jnp.where(row == 0, before, jnp.where(row == 1, last, pltpu.roll(prod, 2, 0)))
    filtered = vec_ref[2:3] * two + vec_ref[3:4] * one + vec_ref[4:5] * prod
    out_ref[...] = (post * filtered).astype(bf16)
    tail_ref[...] = prod[rows - tail_ref.shape[0] :]


def conv_call(place, same, other, w, halo, vec):
    rows, width = same.shape[0] * same.shape[1] * 2, vec.shape[1]
    depth = w.shape[0]
    tile = pl.BlockSpec((CONV_BLOCK, width), lambda i, p: (i, 0))
    whole = lambda a: pl.BlockSpec(a.shape, lambda i, p: (0,) * a.ndim)
    return pl.pallas_call(
        conv_kernel,
        grid_spec=pltpu.PrefetchScalarGridSpec(
            num_scalar_prefetch=1,
            grid=(rows // CONV_BLOCK,),
            in_specs=token_specs()
            + [pl.BlockSpec((depth, 4 * width), lambda i, p: (0, 1)), whole(halo), whole(vec)],
            out_specs=[tile, tile],
            scratch_shapes=[pltpu.VMEM((halo.shape[0], width), f32)],
        ),
        out_shape=[array((rows, width), bf16)] * 2,
        compiler_params=pltpu.CompilerParams(
            dimension_semantics=("arbitrary",), vmem_limit_bytes=20 * 2**20
        ),
        name="conv_mix",
    )(place, same, other, *in_hbm(w), halo, vec)


def reads_kernel(q_ref, gk_ref, gb_ref, wu_ref, v_ref, pos_ref, full_ref, states_ref, o_ref, y_ref):
    width = 2 * HEAD_WIDTH
    each = range(READS_BLOCK // CHUNK)
    t, s, _ = chunk_masks()
    inclusive = t >= s
    fold = functools.partial(spread, first=first_lanes())
    q_all = q_ref[...].astype(f32)
    ask, full = cut(q_all * pos_ref[...]), cut(q_all * full_ref[...])
    gk, gb, wu, v = map(cut, (gk_ref[...], gb_ref[...], wu_ref[...], v_ref[...]))
    grams = [dot(ask[k], jnp.concatenate([fold(gk[k]), fold(gb[k])], axis=0), 1, 1) for k in each]
    key_read = [jnp.where(inclusive, g[:, :width], 0.0) for g in grams]
    beta_read = [jnp.where(inclusive, g[:, width:], 0.0) for g in grams]
    forward = [dot(key_read[k], fold(v[k])) for k in each]
    back = [
        dot(beta_read[k], jnp.concatenate([fold(wu[k][:, :width]), fold(wu[k][:, width:])], axis=1))
        for k in each
    ]
    for k in each:
        start = states_ref[k]
        got = dot(
            full[k] - back[k][:, :width],
            jnp.concatenate([fold(start[:HEAD_WIDTH]), fold(start[HEAD_WIDTH:])], axis=0),
            1,
            1,
        )
        at = slice(k * CHUNK, (k + 1) * CHUNK)
        o_ref[at] = forward[k] - back[k][:, width:] + got[:, :width]
        y_ref[at] = got[:, width:].astype(bf16)


def reads_call(q, gk, gb, wu, v, pos, full, states):
    rows, width = q.shape
    tile = pl.BlockSpec((READS_BLOCK, width), lambda i: (i, 0))
    wide = pl.BlockSpec((READS_BLOCK, 2 * width), lambda i: (i, 0))
    starts = pl.BlockSpec((READS_BLOCK // CHUNK, width, width), lambda i: (i, 0, 0))
    return pl.pallas_call(
        reads_kernel,
        grid=(rows // READS_BLOCK,),
        in_specs=[tile, tile, tile, wide, tile, tile, tile, starts],
        out_specs=[tile, tile],
        out_shape=[array((rows, width), f32), array((rows, width), bf16)],
        compiler_params=pltpu.CompilerParams(
            dimension_semantics=("arbitrary",), vmem_limit_bytes=20 * 2**20
        ),
        name="local_reads",
    )(*in_hbm(q, gk, gb, wu, v, pos, full, states))


def moved(state, piece, first):
    hi = state.astype(bf16)
    lo = (state - hi.astype(f32)).astype(bf16)
    got = dot(jnp.concatenate([hi, lo], axis=0), spread(piece[HEAD_WIDTH:], first))
    return got[: state.shape[0]] + got[state.shape[0] :]


def group_kernel(at_ref, pieces_ref, out_ref, before_ref):
    first = first_lanes()

    def join(total, k):
        piece = pieces_ref[k]
        total = moved(total, piece, first)
        source = total[:HEAD_WIDTH] + piece[:HEAD_WIDTH].astype(f32)
        return jnp.concatenate([source, total[HEAD_WIDTH:]], axis=0)

    total = pieces_ref[0].astype(f32)
    r, l = rows_of(total.shape), lanes_of(total.shape) % HEAD_WIDTH
    before = jnp.where(r - HEAD_WIDTH == l, 1.0, 0.0)
    for k in range(1, pieces_ref.shape[0]):
        before = jnp.where(at_ref[1] == k, total, before)
        total = join(total, k)
    before_ref[...] = before
    for k in range(out_ref.shape[0]):
        out_ref[k] = total.astype(bf16)


def group_call(at, pieces, copies):
    here = pl.BlockSpec(memory_space=pltpu.VMEM)
    return pl.pallas_call(
        group_kernel,
        in_specs=[pl.BlockSpec(memory_space=pltpu.SMEM), here],
        out_specs=[here, here],
        out_shape=[
            jax.ShapeDtypeStruct((copies, *pieces.shape[1:]), bf16),
            jax.ShapeDtypeStruct(pieces.shape[1:], f32),
        ],
        name="group_map",
    )(at, pieces)


def finish_kernel(at_ref, before_ref, far_ref, init_ref, o_ref, y_ref, conv_ref, vec_ref, out_ref, s_ref):
    width = 2 * HEAD_WIDTH
    first = first_lanes()

    @pl.when(pl.program_id(0) == 0)
    def _():
        def advance(i, state):
            piece = far_ref[i]
            return moved(state, piece, first) + piece[:HEAD_WIDTH].astype(f32)

        state = lax.fori_loop(0, at_ref[0], advance, init_ref[...])
        before = before_ref[...]
        state = moved(state, before, first) + before[:HEAD_WIDTH]
        s_ref[...] = spread(state, first)

    low = lanes_of((READS_BLOCK, width)) < HEAD_WIDTH
    reads = o_ref[...] + dot(y_ref[...], s_ref[...], 1, 1)
    centered = reads - head_sums(reads, low) * (1.0 / HEAD_WIDTH)
    variance = head_sums(centered * centered, low) * (1.0 / HEAD_WIDTH)
    mixed = centered * lax.rsqrt(variance + HEAD_WIDTH * 1e-05) * vec_ref[5:6]
    out_ref[:, :width] = conv_ref[...]
    out_ref[:, width:] = mixed.astype(bf16)


def finish_call(at, before, far, init, o, y, conv, vec):
    rows, width = o.shape
    whole = lambda a: pl.BlockSpec(a.shape, lambda i, p: (0,) * a.ndim)
    tile = pl.BlockSpec((READS_BLOCK, width), lambda i, p: (i, 0))
    return pl.pallas_call(
        finish_kernel,
        grid_spec=pltpu.PrefetchScalarGridSpec(
            num_scalar_prefetch=1,
            grid=(rows // READS_BLOCK,),
            in_specs=[whole(before), whole(far), whole(init), tile, tile, tile, whole(vec)],
            out_specs=pl.BlockSpec((READS_BLOCK, 2 * width), lambda i, p: (i, 0)),
            scratch_shapes=[pltpu.VMEM((width, width), bf16)],
        ),
        out_shape=array((rows, 2 * width), bf16),
        compiler_params=pltpu.CompilerParams(
            dimension_semantics=("arbitrary",), vmem_limit_bytes=12 * 2**20
        ),
        name="finish_mix",
    )(at, before, far, init, *in_hbm(o, y, conv), vec)


def outward_kernel(pick_ref, m_ref, *refs):
    *weights, out_ref = refs
    rows, columns = out_ref.shape
    at = pl.multiple_of(pick_ref[0], rows)
    parts = [m_ref[pick_ref[1 + k], pl.ds(at, rows), :] for k in range(len(weights))]
    step = 512
    for first in range(0, columns, step):
        total = None
        for part, w_ref in zip(parts, weights):
            got = dot(part, w_ref[:, first : first + step])
            total = got if total is None else total + got
        out_ref[:, first : first + step] = total.astype(bf16)


def outward_call(pick, gathered, weights):
    rows, columns = gathered.shape[1] // 2, weights[0].shape[1]
    here = pl.BlockSpec(memory_space=pltpu.VMEM)
    return pl.pallas_call(
        outward_kernel,
        in_specs=[pl.BlockSpec(memory_space=pltpu.SMEM)] + [here] * (1 + len(weights)),
        out_specs=here,
        out_shape=jax.ShapeDtypeStruct((rows, columns), bf16),
        compiler_params=pltpu.CompilerParams(vmem_limit_bytes=24 * 2**20),
        name="outward",
    )(pick, gathered, *weights)


def pack_kernel(*refs):
    *parts, out_ref = refs
    for k, ref in enumerate(parts):
        width = ref.shape[1]
        for n in range(out_ref.shape[0]):
            out_ref[n, :, k * width : (k + 1) * width] = ref[...]


def packed(copies, *shards):
    rows, width = shards[0].shape
    return pl.pallas_call(
        pack_kernel,
        out_shape=jax.ShapeDtypeStruct((copies, rows, len(shards) * width), bf16),
        name="pack_shards",
    )(*shards)


def passed_along(block, axis, distance):
    devices = range(lax.axis_size(axis))
    route = [(i - distance, i) for i in devices if i - distance in devices]
    return lax.ppermute(block, axis, route)


def turned(x, distance):
    devices = lax.axis_size("tp")
    return lax.ppermute(x, "tp", [(i, (i + distance) % devices) for i in range(devices)])


def from_everyone(copies, axis, groups=None):
    return lax.all_to_all(copies, axis, 0, 0, tiled=True, axis_index_groups=groups)


def rms_rows(activations, gain_vector):
    values = activations.astype(f32)
    inv_scale = lax.rsqrt(jnp.mean(values * values, axis=-1, keepdims=True) + norm_eps)
    return (values * inv_scale * gain_vector).astype(bf16)


def mixing(
    tokens,
    input_norm_gain,
    earlier_gate,
    later_gate,
    convolution_input,
    convolution_taps,
    receptance,
    key_matrix,
    value_matrix,
    decay_matrix,
    rate_matrix,
    decay_floor,
    rate_offset,
    decay_spike,
    initial_state,
    head_norm_gain,
    convolution_output,
    state_heads_output,
):
    channels = earlier_gate.shape[1]
    heads = channels // HEAD_WIDTH
    devices = lax.axis_size("tp")
    chips = devices // 2
    me = lax.axis_index("tp").astype(jnp.int32)
    chip, core = lax.shift_right_logical(me, 1), me & 1

    def core_swap(x):
        return lax.ppermute(x, "tp", [(i, i ^ 1) for i in range(devices)])

    blocks, seqs = lax.axis_size("sp"), lax.axis_size("fs")
    weights = from_everyone(
        packed(
            seqs,
            key_matrix,
            value_matrix,
            decay_matrix,
            rate_matrix,
            receptance,
            earlier_gate,
            convolution_input,
            later_gate,
        ),
        "fs",
    )
    weights = weights.reshape(-1, 8 * channels)
    weights = lax.all_gather(weights, "sp", axis=0, tiled=True)
    outer = from_everyone(packed(blocks, convolution_output.T, state_heads_output.T), "sp")
    outer = from_everyone(jnp.broadcast_to(outer[None], (seqs, *outer.shape)), "fs")
    outer = jnp.swapaxes(outer, 0, 1).reshape(-1, 2 * channels).T

    normed = rms_rows(tokens[0], input_norm_gain)
    opposite = turned(normed, 4)
    ahead, behind = turned(normed, -2), turned(normed, 2)
    same = jnp.stack([normed, ahead, opposite, behind])
    other = core_swap(same)
    across = turned(outer, 4)
    after, before = turned(outer, -2), turned(outer, 2)
    vec = jnp.concatenate(
        [
            decay_floor[None],
            rate_offset[None],
            convolution_taps,
            head_norm_gain[None],
            jnp.zeros((2, channels), f32),
        ],
        axis=0,
    )
    place = jnp.stack([chip, core])
    few = 4
    near_blocks = [list(range(k, k + few)) for k in range(0, blocks, few)]
    far_blocks = [list(range(k, blocks, few)) for k in range(few)]
    *kept, last_rows, agg = maps_call(place, same, other, weights, decay_spike[0], vec, few)
    near_maps = from_everyone(agg, "sp", near_blocks)
    halo = passed_along(last_rows, "sp", 1)
    block = lax.axis_index("sp").astype(jnp.int32)
    at = jnp.stack([lax.shift_right_logical(block, 2), block & (few - 1)])
    at, halo = lax.optimization_barrier((at, halo))
    total, earlier = group_call(at, near_maps, blocks // few)
    far_maps = from_everyone(total, "sp", far_blocks)
    q, conv = conv_call(place, same, other, weights, halo, vec)
    o, y = reads_call(q, *kept)
    init = jnp.moveaxis(initial_state[0], 0, 1).reshape(HEAD_WIDTH, heads * HEAD_WIDTH)
    mixed = finish_call(at, earlier, far_maps, init, o, y, conv, vec)
    groups = [list(range(side, devices, 2)) for side in range(2)]
    gathered = lax.all_to_all(
        mixed.reshape(chips, -1, 2 * channels), "tp", 0, 0, tiled=True, axis_index_groups=groups
    )
    near = [(chip + k) & (chips - 1) for k in (0, 1, 2, chips - 1)]
    own, ways = normed.shape[0], (outer, after, across, before)
    given = outward_call(jnp.stack([(1 - core) * own, *near]), gathered, ways)
    taken = core_swap(given)
    kept = outward_call(jnp.stack([core * own, *near]), gathered, ways)
    return (kept.astype(f32) + taken.astype(f32)).astype(bf16)[None]


def solution(mesh):
    placed = (
        P("fs", ("sp", "tp"), None),
        P(),
        P(("sp", "fs"), "tp"),
        P(("sp", "fs"), "tp"),
        P(("sp", "fs"), "tp"),
        P(None, "tp"),
        P(("sp", "fs"), "tp"),
        P(("sp", "fs"), "tp"),
        P(("sp", "fs"), "tp"),
        P(("sp", "fs"), "tp"),
        P(("sp", "fs"), "tp"),
        P("tp"),
        P("tp"),
        P("fs", "sp", "tp"),
        P("fs", "tp", None, None),
        P("tp"),
        P("tp", ("sp", "fs")),
        P("tp", ("sp", "fs")),
    )
    return jax.shard_map(
        mixing,
        mesh=mesh,
        in_specs=placed,
        out_specs=P("fs", ("sp", "tp"), None),
        check_vma=False,
    )
```

```python
import functools

import jax
import jax.numpy as jnp
from jax import lax
from jax.experimental import pallas as pl
from jax.experimental.pallas import tpu as pltpu
from jax.sharding import PartitionSpec as P


HEAD_WIDTH = 64
CHUNK = 64
BLOCK = 256
MAPS_BLOCK = 1024
READS_BLOCK = 512
CONV_BLOCK = 1024
HALO = 16
norm_eps = 1e-06
key_eps = 1e-06
f32, bf16 = jnp.float32, jnp.bfloat16


def array(shape, dtype):
    return pltpu.HBM(tuple(shape), dtype)


def in_hbm(*arrays):
    return [pltpu.with_memory_space_constraint(a, pltpu.HBM) for a in arrays]


def dot(a, b, ca=1, cb=0):
    return lax.dot_general(
        a.astype(bf16), b.astype(bf16), (((ca,), (cb,)), ((), ())), preferred_element_type=f32
    )


def lanes_of(shape):
    return lax.broadcasted_iota(jnp.int32, shape, 1)


def rows_of(shape):
    return lax.broadcasted_iota(jnp.int32, shape, 0)


def spread(z, first):
    z = z.astype(bf16)
    return jnp.concatenate([z * first, z * (1 - first)], axis=0)


def head_sums(z, low):
    a = jnp.sum(jnp.where(low, z, 0.0), axis=1, keepdims=True)
    b = jnp.sum(jnp.where(low, 0.0, z), axis=1, keepdims=True)
    return jnp.where(low, a, b)


def own_block(place_ref, same_ref, other_ref, first, pairs=1):
    chips = same_ref.shape[0]
    low_core = place_ref[1] == 0
    rows = []
    for k in range(pairs):
        at = (first + k - place_ref[0]) & (chips - 1)
        mine, theirs = same_ref[at], other_ref[at]
        rows += [jnp.where(low_core, mine, theirs), jnp.where(low_core, theirs, mine)]
    return jnp.concatenate(rows, axis=0)


def chunk_masks():
    shape = (CHUNK, 2 * HEAD_WIDTH)
    return rows_of(shape), lanes_of(shape) % HEAD_WIDTH, lanes_of(shape) < HEAD_WIDTH


def first_lanes():
    return jnp.where(lanes_of((1, 2 * HEAD_WIDTH)) < HEAD_WIDTH, 1.0, 0.0).astype(bf16)


def cut(a):
    return [a[k * CHUNK : (k + 1) * CHUNK] for k in range(a.shape[0] // CHUNK)]


def maps_kernel(
    place_ref,
    same_ref,
    other_ref,
    w_ref,
    spike_ref,
    vec_ref,
    gk_ref,
    gb_ref,
    wu_ref,
    v_ref,
    pos_ref,
    full_ref,
    states_ref,
    agg_ref,
    st_ref,
):
    step = pl.program_id(0)
    width = 2 * HEAD_WIDTH
    each = range(MAPS_BLOCK // CHUNK)

    @pl.when(step == 0)
    def _():
        r, l = rows_of((width, width)), lanes_of((width, width))
        eye = (r - HEAD_WIDTH == l % HEAD_WIDTH) & (r >= HEAD_WIDTH)
        st_ref[...] = jnp.where(eye, 1.0, 0.0).astype(f32)

    pairs = MAPS_BLOCK // BLOCK
    x = own_block(place_ref, same_ref, other_ref, step * pairs, pairs)

    def section(k):
        two = jnp.dot(x, w_ref[:, 2 * k * width : 2 * (k + 1) * width], preferred_element_type=f32)
        two = two.astype(bf16)
        return two[:, :width], two[:, width:]

    dpre, rpre = (a.astype(f32) for a in section(1))
    keys, vals = section(0)
    v_ref[...] = vals
    keys = keys.astype(f32)

    low = lanes_of((MAPS_BLOCK, width)) < HEAD_WIDTH
    logd = spike_ref[...] - jnp.exp(vec_ref[0:1] + jnp.tanh(dpre))
    rate = jax.nn.sigmoid(vec_ref[1:2] + rpre)
    unit = keys * lax.rsqrt(head_sums(keys * keys, low) + key_eps)
    beta = rate * unit
    r, c = rows_of((BLOCK, BLOCK)), lanes_of((BLOCK, BLOCK))
    tri = jnp.where((r >= c) & (r // CHUNK == c // CHUNK), 1.0, 0.0).astype(bf16)
    hi = logd.astype(bf16)
    rest = logd - hi.astype(f32)
    mid = rest.astype(bf16)
    lo = (rest - mid.astype(f32)).astype(bf16)
    terms = jnp.concatenate([hi, mid, lo], axis=1)
    sums = jnp.concatenate(
        [
            jnp.dot(tri, terms[k : k + BLOCK], preferred_element_type=f32)
            for k in range(0, MAPS_BLOCK, BLOCK)
        ],
        axis=0,
    )
    cum_all = sums[:, :width] + sums[:, width : 2 * width] + sums[:, 2 * width :]
    prev_all = cum_all - logd

    t, s, low_c = chunk_masks()
    strict = t > s
    fold = functools.partial(spread, first=first_lanes())
    same = (rows_of((width, width)) // HEAD_WIDTH) == (lanes_of((width, width)) // HEAD_WIDTH)

    keys, vals, unit, beta, cum, prev = map(cut, (keys, vals, unit, beta, cum_all, prev_all))
    center = [cum[k][CHUNK // 2 : CHUNK // 2 + 1] for k in each]
    close = [cum[k][CHUNK - 1 : CHUNK] for k in each]
    e_neg = [jnp.exp(center[k] - cum[k]) for k in each]
    ask_k = [unit[k] * jnp.exp(prev[k] - center[k]) for k in each]
    give_k = [keys[k] * e_neg[k] for k in each]
    give_b = [beta[k] * e_neg[k] for k in each]
    e_center = [jnp.exp(center[k]) for k in each]
    e_tail = [jnp.exp(close[k] - center[k]) for k in each]
    e_close = [jnp.exp(close[k]) for k in each]
    grams = [dot(ask_k[k], jnp.concatenate([fold(give_k[k]), fold(give_b[k])], axis=0), 1, 1) for k in each]
    key_ask = [jnp.where(strict, g[:, :width], 0.0) for g in grams]
    beta_ask = [jnp.where(strict, g[:, width:], 0.0) for g in grams]
    asked = [dot(key_ask[k], fold(vals[k])) for k in each]

    inv = [jnp.where(t == s, 1.0, jnp.where(t // 2 == s // 2, -beta_ask[k], 0.0)) for k in each]
    size = 2
    while size < CHUNK:
        here = (t // (2 * size) == s // (2 * size)) & (t // size != s // size)
        mixed = [dot(inv[k], fold(jnp.where(here, beta_ask[k], 0.0))) for k in each]
        inv = [inv[k] - dot(mixed[k], fold(inv[k])) for k in each]
        size *= 2

    wu = [
        dot(inv[k], jnp.concatenate([fold(ask_k[k] * e_center[k]), fold(asked[k])], axis=1))
        for k in each
    ]
    outer = [dot(wu[k], give_b[k] * e_tail[k], 0, 0) for k in each]
    outer_v = [dot(vals[k], give_k[k] * e_tail[k], 0, 0) for k in each]
    step_map = [jnp.where(same, -outer[k][:width], 0.0).astype(bf16) for k in each]
    source_full = [outer_v[k] - outer[k][width:] for k in each]
    source = [jnp.where(low_c, f[:HEAD_WIDTH], f[HEAD_WIDTH:]) for f in source_full]

    state = st_ref[...]
    for k in each:
        rounded = state.astype(bf16)
        states_ref[k] = rounded
        state = state * e_close[k] + dot(rounded, step_map[k])
        state = jnp.concatenate([state[:HEAD_WIDTH] + source[k], state[HEAD_WIDTH:]], axis=0)
    st_ref[...] = state

    for k in each:
        at = slice(k * CHUNK, (k + 1) * CHUNK)
        gk_ref[at] = give_k[k].astype(bf16)
        gb_ref[at] = give_b[k].astype(bf16)
        wu_ref[at] = wu[k].astype(bf16)
        pos_ref[at] = jnp.exp(cum[k] - center[k])
        full_ref[at] = jnp.exp(cum[k])

    @pl.when(step == pl.num_programs(0) - 1)
    def _():
        for k in range(agg_ref.shape[0]):
            agg_ref[k] = state.astype(bf16)


def token_specs():
    return [pl.BlockSpec(memory_space=pltpu.VMEM)] * 2


def maps_call(place, same, other, w, spike, vec, copies):
    rows, width = spike.shape
    depth = w.shape[0]
    tile = pl.BlockSpec((MAPS_BLOCK, width), lambda i, p: (i, 0))
    wide = pl.BlockSpec((MAPS_BLOCK, 2 * width), lambda i, p: (i, 0))
    pairs = MAPS_BLOCK // CHUNK
    like = lambda n, t: array((rows, n), t)
    return pl.pallas_call(
        maps_kernel,
        grid_spec=pltpu.PrefetchScalarGridSpec(
            num_scalar_prefetch=1,
            grid=(rows // MAPS_BLOCK,),
            in_specs=token_specs()
            + [
                pl.BlockSpec((depth, 4 * width), lambda i, p: (0, 0)),
                tile,
                pl.BlockSpec(vec.shape, lambda i, p: (0, 0)),
            ],
            out_specs=[
                tile,
                tile,
                wide,
                tile,
                tile,
                tile,
                pl.BlockSpec((pairs, width, width), lambda i, p: (i, 0, 0)),
                pl.BlockSpec((copies, width, width), lambda i, p: (0, 0, 0)),
            ],
            scratch_shapes=[pltpu.VMEM((width, width), f32)],
        ),
        out_shape=[
            like(width, bf16),
            like(width, bf16),
            like(2 * width, bf16),
            like(width, bf16),
            like(width, f32),
            like(width, f32),
            array((rows // CHUNK, width, width), bf16),
            array((copies, width, width), bf16),
        ],
        compiler_params=pltpu.CompilerParams(
            dimension_semantics=("arbitrary",), vmem_limit_bytes=28 * 2**20
        ),
        name="state_maps",
    )(place, same, other, *in_hbm(w, spike), vec)


def conv_kernel(place_ref, same_ref, other_ref, w_ref, halo_ref, vec_ref, q_ref, out_ref, tail_ref):
    width = vec_ref.shape[1]

    def project(x, first, last):
        out = jnp.dot(x, w_ref[:, first * width : last * width], preferred_element_type=f32)
        return out.astype(bf16)

    @pl.when(pl.program_id(0) == 0)
    def _():
        two = project(halo_ref[...], 1, 3).astype(f32)
        tail_ref[...] = two[:, :width] * two[:, width:]

    pairs = CONV_BLOCK // BLOCK
    x = own_block(place_ref, same_ref, other_ref, pl.program_id(0) * pairs, pairs)
    two = project(x, 0, 2)
    q_ref[...] = two[:, :width]
    rest = project(x, 2, 4).astype(f32)
    prod, post = two[:, width:].astype(f32) * rest[:, :width], rest[:, width:]
    rows = prod.shape[0]
    tail = tail_ref[...]
    row = rows_of((rows, width))
    last, before = tail[-1:], tail[-2:-1]
    one = jnp.where(row == 0, last, pltpu.roll(prod, 1, 0))
    two = jnp.where(row == 0, before, jnp.where(row == 1, last, pltpu.roll(prod, 2, 0)))
    filtered = vec_ref[2:3] * two + vec_ref[3:4] * one + vec_ref[4:5] * prod
    out_ref[...] = (post * filtered).astype(bf16)
    tail_ref[...] = prod[rows - tail_ref.shape[0] :]


def conv_call(place, same, other, w, halo, vec):
    rows, width = same.shape[0] * same.shape[1] * 2, vec.shape[1]
    depth = w.shape[0]
    tile = pl.BlockSpec((CONV_BLOCK, width), lambda i, p: (i, 0))
    whole = lambda a: pl.BlockSpec(a.shape, lambda i, p: (0,) * a.ndim)
    return pl.pallas_call(
        conv_kernel,
        grid_spec=pltpu.PrefetchScalarGridSpec(
            num_scalar_prefetch=1,
            grid=(rows // CONV_BLOCK,),
            in_specs=token_specs()
            + [pl.BlockSpec((depth, 4 * width), lambda i, p: (0, 1)), whole(halo), whole(vec)],
            out_specs=[tile, tile],
            scratch_shapes=[pltpu.VMEM((halo.shape[0], width), f32)],
        ),
        out_shape=[array((rows, width), bf16)] * 2,
        compiler_params=pltpu.CompilerParams(
            dimension_semantics=("arbitrary",), vmem_limit_bytes=20 * 2**20
        ),
        name="conv_mix",
    )(place, same, other, *in_hbm(w), halo, vec)


def reads_kernel(q_ref, gk_ref, gb_ref, wu_ref, v_ref, pos_ref, full_ref, states_ref, o_ref, y_ref):
    width = 2 * HEAD_WIDTH
    each = range(READS_BLOCK // CHUNK)
    t, s, _ = chunk_masks()
    inclusive = t >= s
    fold = functools.partial(spread, first=first_lanes())
    q_all = q_ref[...].astype(f32)
    ask, full = cut(q_all * pos_ref[...]), cut(q_all * full_ref[...])
    gk, gb, wu, v = map(cut, (gk_ref[...], gb_ref[...], wu_ref[...], v_ref[...]))
    grams = [dot(ask[k], jnp.concatenate([fold(gk[k]), fold(gb[k])], axis=0), 1, 1) for k in each]
    key_read = [jnp.where(inclusive, g[:, :width], 0.0) for g in grams]
    beta_read = [jnp.where(inclusive, g[:, width:], 0.0) for g in grams]
    forward = [dot(key_read[k], fold(v[k])) for k in each]
    back = [
        dot(beta_read[k], jnp.concatenate([fold(wu[k][:, :width]), fold(wu[k][:, width:])], axis=1))
        for k in each
    ]
    for k in each:
        start = states_ref[k]
        got = dot(
            full[k] - back[k][:, :width],
            jnp.concatenate([fold(start[:HEAD_WIDTH]), fold(start[HEAD_WIDTH:])], axis=0),
            1,
            1,
        )
        at = slice(k * CHUNK, (k + 1) * CHUNK)
        o_ref[at] = forward[k] - back[k][:, width:] + got[:, :width]
        y_ref[at] = got[:, width:].astype(bf16)


def reads_call(q, gk, gb, wu, v, pos, full, states):
    rows, width = q.shape
    tile = pl.BlockSpec((READS_BLOCK, width), lambda i: (i, 0))
    wide = pl.BlockSpec((READS_BLOCK, 2 * width), lambda i: (i, 0))
    starts = pl.BlockSpec((READS_BLOCK // CHUNK, width, width), lambda i: (i, 0, 0))
    return pl.pallas_call(
        reads_kernel,
        grid=(rows // READS_BLOCK,),
        in_specs=[tile, tile, tile, wide, tile, tile, tile, starts],
        out_specs=[tile, tile],
        out_shape=[array((rows, width), f32), array((rows, width), bf16)],
        compiler_params=pltpu.CompilerParams(
            dimension_semantics=("arbitrary",), vmem_limit_bytes=20 * 2**20
        ),
        name="local_reads",
    )(*in_hbm(q, gk, gb, wu, v, pos, full, states))


def moved(state, piece, first):
    hi = state.astype(bf16)
    lo = (state - hi.astype(f32)).astype(bf16)
    got = dot(jnp.concatenate([hi, lo], axis=0), spread(piece[HEAD_WIDTH:], first))
    return got[: state.shape[0]] + got[state.shape[0] :]


def group_kernel(at_ref, pieces_ref, out_ref, before_ref):
    first = first_lanes()

    def join(total, k):
        piece = pieces_ref[k]
        total = moved(total, piece, first)
        source = total[:HEAD_WIDTH] + piece[:HEAD_WIDTH].astype(f32)
        return jnp.concatenate([source, total[HEAD_WIDTH:]], axis=0)

    total = pieces_ref[0].astype(f32)
    r, l = rows_of(total.shape), lanes_of(total.shape) % HEAD_WIDTH
    before = jnp.where(r - HEAD_WIDTH == l, 1.0, 0.0)
    for k in range(1, pieces_ref.shape[0]):
        before = jnp.where(at_ref[1] == k, total, before)
        total = join(total, k)
    before_ref[...] = before
    for k in range(out_ref.shape[0]):
        out_ref[k] = total.astype(bf16)


def group_call(at, pieces, copies):
    here = pl.BlockSpec(memory_space=pltpu.VMEM)
    return pl.pallas_call(
        group_kernel,
        in_specs=[pl.BlockSpec(memory_space=pltpu.SMEM), here],
        out_specs=[here, here],
        out_shape=[
            jax.ShapeDtypeStruct((copies, *pieces.shape[1:]), bf16),
            jax.ShapeDtypeStruct(pieces.shape[1:], f32),
        ],
        name="group_map",
    )(at, pltpu.with_memory_space_constraint(pieces, pltpu.VMEM))


def finish_kernel(at_ref, before_ref, far_ref, init_ref, o_ref, y_ref, conv_ref, vec_ref, out_ref, s_ref):
    width = 2 * HEAD_WIDTH
    first = first_lanes()

    @pl.when(pl.program_id(0) == 0)
    def _():
        def advance(i, state):
            piece = far_ref[i]
            return moved(state, piece, first) + piece[:HEAD_WIDTH].astype(f32)

        state = lax.fori_loop(0, at_ref[0], advance, init_ref[...])
        before = before_ref[...]
        state = moved(state, before, first) + before[:HEAD_WIDTH]
        s_ref[...] = spread(state, first)

    low = lanes_of((READS_BLOCK, width)) < HEAD_WIDTH
    reads = o_ref[...] + dot(y_ref[...], s_ref[...], 1, 1)
    centered = reads - head_sums(reads, low) * (1.0 / HEAD_WIDTH)
    variance = head_sums(centered * centered, low) * (1.0 / HEAD_WIDTH)
    mixed = centered * lax.rsqrt(variance + HEAD_WIDTH * 1e-05) * vec_ref[5:6]
    out_ref[:, :width] = conv_ref[...]
    out_ref[:, width:] = mixed.astype(bf16)


def finish_call(at, before, far, init, o, y, conv, vec):
    rows, width = o.shape
    whole = lambda a: pl.BlockSpec(a.shape, lambda i, p: (0,) * a.ndim)
    tile = pl.BlockSpec((READS_BLOCK, width), lambda i, p: (i, 0))
    return pl.pallas_call(
        finish_kernel,
        grid_spec=pltpu.PrefetchScalarGridSpec(
            num_scalar_prefetch=1,
            grid=(rows // READS_BLOCK,),
            in_specs=[whole(before), whole(far), whole(init), tile, tile, tile, whole(vec)],
            out_specs=pl.BlockSpec((READS_BLOCK, 2 * width), lambda i, p: (i, 0)),
            scratch_shapes=[pltpu.VMEM((width, width), bf16)],
        ),
        out_shape=array((rows, 2 * width), bf16),
        compiler_params=pltpu.CompilerParams(
            dimension_semantics=("arbitrary",), vmem_limit_bytes=12 * 2**20
        ),
        name="finish_mix",
    )(at, before, far, init, *in_hbm(o, y, conv), vec)


def outward_kernel(pick_ref, m_ref, *refs):
    *weights, keep_ref, give_ref = refs
    rows, columns = keep_ref.shape
    first = pick_ref[0] == 0
    step = 512
    for at in range(0, columns, step):
        total = None
        for k, w_ref in enumerate(weights):
            got = dot(m_ref[pick_ref[1 + k]], w_ref[:, at : at + step])
            total = got if total is None else total + got
        total = total.astype(bf16)
        keep_ref[:, at : at + step] = jnp.where(first, total[:rows], total[rows:])
        give_ref[:, at : at + step] = jnp.where(first, total[rows:], total[:rows])


def outward_call(pick, gathered, weights):
    rows, columns = gathered.shape[1] // 2, weights[0].shape[1]
    here = pl.BlockSpec(memory_space=pltpu.VMEM)
    return pl.pallas_call(
        outward_kernel,
        in_specs=[pl.BlockSpec(memory_space=pltpu.SMEM)] + [here] * (1 + len(weights)),
        out_specs=[here, here],
        out_shape=[jax.ShapeDtypeStruct((rows, columns), bf16)] * 2,
        compiler_params=pltpu.CompilerParams(vmem_limit_bytes=24 * 2**20),
        name="outward",
    )(pick, gathered, *weights)


def pack_kernel(*refs):
    *parts, out_ref = refs
    for k, ref in enumerate(parts):
        width = ref.shape[1]
        for n in range(out_ref.shape[0]):
            out_ref[n, :, k * width : (k + 1) * width] = ref[...]


def packed(copies, *shards):
    rows, width = shards[0].shape
    return pl.pallas_call(
        pack_kernel,
        out_shape=jax.ShapeDtypeStruct((copies, rows, len(shards) * width), bf16),
        name="pack_shards",
    )(*shards)


def passed_along(block, axis, distance):
    devices = range(lax.axis_size(axis))
    route = [(i - distance, i) for i in devices if i - distance in devices]
    return lax.ppermute(block, axis, route)


def turned(x, distance):
    devices = lax.axis_size("tp")
    return lax.ppermute(x, "tp", [(i, (i + distance) % devices) for i in range(devices)])


def from_everyone(copies, axis, groups=None):
    return lax.all_to_all(copies, axis, 0, 0, tiled=True, axis_index_groups=groups)


def rms_rows(activations, gain_vector):
    values = activations.astype(f32)
    inv_scale = lax.rsqrt(jnp.mean(values * values, axis=-1, keepdims=True) + norm_eps)
    return (values * inv_scale * gain_vector).astype(bf16)


def mixing(
    tokens,
    input_norm_gain,
    earlier_gate,
    later_gate,
    convolution_input,
    convolution_taps,
    receptance,
    key_matrix,
    value_matrix,
    decay_matrix,
    rate_matrix,
    decay_floor,
    rate_offset,
    decay_spike,
    initial_state,
    head_norm_gain,
    convolution_output,
    state_heads_output,
):
    channels = earlier_gate.shape[1]
    heads = channels // HEAD_WIDTH
    devices = lax.axis_size("tp")
    chips = devices // 2
    me = lax.axis_index("tp").astype(jnp.int32)
    chip, core = lax.shift_right_logical(me, 1), me & 1

    def core_swap(x):
        return lax.ppermute(x, "tp", [(i, i ^ 1) for i in range(devices)])

    blocks, seqs = lax.axis_size("sp"), lax.axis_size("fs")
    weights = from_everyone(
        packed(
            seqs,
            key_matrix,
            value_matrix,
            decay_matrix,
            rate_matrix,
            receptance,
            earlier_gate,
            convolution_input,
            later_gate,
        ),
        "fs",
    )
    weights = weights.reshape(-1, 8 * channels)
    weights = lax.all_gather(weights, "sp", axis=0, tiled=True)
    outer = from_everyone(packed(blocks, convolution_output.T, state_heads_output.T), "sp")
    outer = from_everyone(jnp.broadcast_to(outer[None], (seqs, *outer.shape)), "fs")
    outer = jnp.swapaxes(outer, 0, 1).reshape(-1, 2 * channels).T

    normed = rms_rows(tokens[0], input_norm_gain)
    opposite = turned(normed, 4)
    ahead, behind = turned(normed, -2), turned(normed, 2)
    same = jnp.stack([normed, ahead, opposite, behind])
    other = core_swap(same)
    across = turned(outer, 4)
    after, before = turned(outer, -2), turned(outer, 2)
    vec = jnp.concatenate(
        [
            decay_floor[None],
            rate_offset[None],
            convolution_taps,
            head_norm_gain[None],
            jnp.zeros((2, channels), f32),
        ],
        axis=0,
    )
    init = jnp.moveaxis(initial_state[0], 0, 1).reshape(HEAD_WIDTH, heads * HEAD_WIDTH)
    vec, init = lax.optimization_barrier((vec, init))
    place = jnp.stack([chip, core])
    last_rows = jnp.where(core == 0, other[:, -HALO:], same[:, -HALO:])
    last_rows = lax.dynamic_index_in_dim(last_rows, (chips - 1 - chip) & (chips - 1), 0, keepdims=False)
    halo = passed_along(last_rows, "sp", 1)
    few = 4
    near_blocks = [list(range(k, k + few)) for k in range(0, blocks, few)]
    far_blocks = [list(range(k, blocks, few)) for k in range(few)]
    *kept, agg = maps_call(place, same, other, weights, decay_spike[0], vec, few)
    near_maps = from_everyone(agg, "sp", near_blocks)
    block = lax.axis_index("sp").astype(jnp.int32)
    at = jnp.stack([lax.shift_right_logical(block, 2), block & (few - 1)])
    total, earlier = group_call(at, near_maps, blocks // few)
    far_maps = from_everyone(total, "sp", far_blocks)
    q, conv = conv_call(place, same, other, weights, halo, vec)
    o, y = reads_call(q, *kept)
    mixed = finish_call(at, earlier, far_maps, init, o, y, conv, vec)
    groups = [list(range(side, devices, 2)) for side in range(2)]
    gathered = lax.all_to_all(
        mixed.reshape(chips, -1, 2 * channels), "tp", 0, 0, tiled=True, axis_index_groups=groups
    )
    near = [(chip + k) & (chips - 1) for k in (0, 1, 2, chips - 1)]
    kept, given = outward_call(jnp.stack([core, *near]), gathered, (outer, after, across, before))
    taken = core_swap(given)
    return (kept.astype(f32) + taken.astype(f32)).astype(bf16)[None]


def solution(mesh):
    placed = (
        P("fs", ("sp", "tp"), None),
        P(),
        P(("sp", "fs"), "tp"),
        P(("sp", "fs"), "tp"),
        P(("sp", "fs"), "tp"),
        P(None, "tp"),
        P(("sp", "fs"), "tp"),
        P(("sp", "fs"), "tp"),
        P(("sp", "fs"), "tp"),
        P(("sp", "fs"), "tp"),
        P(("sp", "fs"), "tp"),
        P("tp"),
        P("tp"),
        P("fs", "sp", "tp"),
        P("fs", "tp", None, None),
        P("tp"),
        P("tp", ("sp", "fs")),
        P("tp", ("sp", "fs")),
    )
    return jax.shard_map(
        mixing,
        mesh=mesh,
        in_specs=placed,
        out_specs=P("fs", ("sp", "tp"), None),
        check_vma=False,
    )
```

```python
import functools

import jax
import jax.numpy as jnp
from jax import lax
from jax.experimental import pallas as pl
from jax.experimental.pallas import tpu as pltpu
from jax.sharding import PartitionSpec as P


HEAD_WIDTH = 64
CHUNK = 64
BLOCK = 256
MAPS_BLOCK = 1024
READS_BLOCK = 512
CONV_BLOCK = 1024
HALO = 16
norm_eps = 1e-06
key_eps = 1e-06
f32, bf16 = jnp.float32, jnp.bfloat16


def array(shape, dtype):
    return pltpu.HBM(tuple(shape), dtype)


def in_hbm(*arrays):
    return [pltpu.with_memory_space_constraint(a, pltpu.HBM) for a in arrays]


def in_vmem(a):
    return pltpu.with_memory_space_constraint(a, pltpu.VMEM)


def dot(a, b, ca=1, cb=0):
    return lax.dot_general(
        a.astype(bf16), b.astype(bf16), (((ca,), (cb,)), ((), ())), preferred_element_type=f32
    )


def lanes_of(shape):
    return lax.broadcasted_iota(jnp.int32, shape, 1)


def rows_of(shape):
    return lax.broadcasted_iota(jnp.int32, shape, 0)


def spread(z, first):
    z = z.astype(bf16)
    return jnp.concatenate([z * first, z * (1 - first)], axis=0)


def head_sums(z, low):
    a = jnp.sum(jnp.where(low, z, 0.0), axis=1, keepdims=True)
    b = jnp.sum(jnp.where(low, 0.0, z), axis=1, keepdims=True)
    return jnp.where(low, a, b)


def own_block(place_ref, same_ref, other_ref, first, pairs=1):
    chips = same_ref.shape[0]
    low_core = place_ref[1] == 0
    rows = []
    for k in range(pairs):
        at = (first + k - place_ref[0]) & (chips - 1)
        mine, theirs = same_ref[at], other_ref[at]
        rows += [jnp.where(low_core, mine, theirs), jnp.where(low_core, theirs, mine)]
    return jnp.concatenate(rows, axis=0)


def chunk_masks():
    shape = (CHUNK, 2 * HEAD_WIDTH)
    return rows_of(shape), lanes_of(shape) % HEAD_WIDTH, lanes_of(shape) < HEAD_WIDTH


def first_lanes():
    return jnp.where(lanes_of((1, 2 * HEAD_WIDTH)) < HEAD_WIDTH, 1.0, 0.0).astype(bf16)


def cut(a):
    return [a[k * CHUNK : (k + 1) * CHUNK] for k in range(a.shape[0] // CHUNK)]


def maps_kernel(
    place_ref,
    same_ref,
    other_ref,
    w_ref,
    spike_ref,
    vec_ref,
    gk_ref,
    gb_ref,
    wu_ref,
    v_ref,
    pos_ref,
    full_ref,
    states_ref,
    agg_ref,
    st_ref,
):
    step = pl.program_id(0)
    width = 2 * HEAD_WIDTH
    each = range(MAPS_BLOCK // CHUNK)

    @pl.when(step == 0)
    def _():
        r, l = rows_of((width, width)), lanes_of((width, width))
        eye = (r - HEAD_WIDTH == l % HEAD_WIDTH) & (r >= HEAD_WIDTH)
        st_ref[...] = jnp.where(eye, 1.0, 0.0).astype(f32)

    pairs = MAPS_BLOCK // BLOCK
    x = own_block(place_ref, same_ref, other_ref, step * pairs, pairs)

    def section(k):
        two = jnp.dot(x, w_ref[:, 2 * k * width : 2 * (k + 1) * width], preferred_element_type=f32)
        two = two.astype(bf16)
        return two[:, :width], two[:, width:]

    dpre, rpre = (a.astype(f32) for a in section(1))
    keys, vals = section(0)
    v_ref[...] = vals
    keys = keys.astype(f32)

    low = lanes_of((MAPS_BLOCK, width)) < HEAD_WIDTH
    logd = spike_ref[...] - jnp.exp(vec_ref[0:1] + jnp.tanh(dpre))
    rate = jax.nn.sigmoid(vec_ref[1:2] + rpre)
    unit = keys * lax.rsqrt(head_sums(keys * keys, low) + key_eps)
    beta = rate * unit
    r, c = rows_of((BLOCK, BLOCK)), lanes_of((BLOCK, BLOCK))
    tri = jnp.where((r >= c) & (r // CHUNK == c // CHUNK), 1.0, 0.0).astype(bf16)
    hi = logd.astype(bf16)
    rest = logd - hi.astype(f32)
    mid = rest.astype(bf16)
    lo = (rest - mid.astype(f32)).astype(bf16)
    terms = jnp.concatenate([hi, mid, lo], axis=1)
    sums = jnp.concatenate(
        [
            jnp.dot(tri, terms[k : k + BLOCK], preferred_element_type=f32)
            for k in range(0, MAPS_BLOCK, BLOCK)
        ],
        axis=0,
    )
    cum_all = sums[:, :width] + sums[:, width : 2 * width] + sums[:, 2 * width :]
    prev_all = cum_all - logd

    t, s, low_c = chunk_masks()
    strict = t > s
    fold = functools.partial(spread, first=first_lanes())
    same = (rows_of((width, width)) // HEAD_WIDTH) == (lanes_of((width, width)) // HEAD_WIDTH)

    keys, vals, unit, beta, cum, prev = map(cut, (keys, vals, unit, beta, cum_all, prev_all))
    center = [cum[k][CHUNK // 2 : CHUNK // 2 + 1] for k in each]
    close = [cum[k][CHUNK - 1 : CHUNK] for k in each]
    e_neg = [jnp.exp(center[k] - cum[k]) for k in each]
    ask_k = [unit[k] * jnp.exp(prev[k] - center[k]) for k in each]
    give_k = [keys[k] * e_neg[k] for k in each]
    give_b = [beta[k] * e_neg[k] for k in each]
    e_center = [jnp.exp(center[k]) for k in each]
    e_tail = [jnp.exp(close[k] - center[k]) for k in each]
    e_close = [jnp.exp(close[k]) for k in each]
    grams = [dot(ask_k[k], jnp.concatenate([fold(give_k[k]), fold(give_b[k])], axis=0), 1, 1) for k in each]
    key_ask = [jnp.where(strict, g[:, :width], 0.0) for g in grams]
    beta_ask = [jnp.where(strict, g[:, width:], 0.0) for g in grams]
    asked = [dot(key_ask[k], fold(vals[k])) for k in each]

    inv = [jnp.where(t == s, 1.0, jnp.where(t // 2 == s // 2, -beta_ask[k], 0.0)) for k in each]
    size = 2
    while size < CHUNK:
        here = (t // (2 * size) == s // (2 * size)) & (t // size != s // size)
        mixed = [dot(inv[k], fold(jnp.where(here, beta_ask[k], 0.0))) for k in each]
        inv = [inv[k] - dot(mixed[k], fold(inv[k])) for k in each]
        size *= 2

    wu = [
        dot(inv[k], jnp.concatenate([fold(ask_k[k] * e_center[k]), fold(asked[k])], axis=1))
        for k in each
    ]
    outer = [dot(wu[k], give_b[k] * e_tail[k], 0, 0) for k in each]
    outer_v = [dot(vals[k], give_k[k] * e_tail[k], 0, 0) for k in each]
    step_map = [jnp.where(same, -outer[k][:width], 0.0).astype(bf16) for k in each]
    source_full = [outer_v[k] - outer[k][width:] for k in each]
    source = [jnp.where(low_c, f[:HEAD_WIDTH], f[HEAD_WIDTH:]) for f in source_full]

    state = st_ref[...]
    for k in each:
        rounded = state.astype(bf16)
        states_ref[k] = rounded
        state = state * e_close[k] + dot(rounded, step_map[k])
        state = jnp.concatenate([state[:HEAD_WIDTH] + source[k], state[HEAD_WIDTH:]], axis=0)
    st_ref[...] = state

    for k in each:
        at = slice(k * CHUNK, (k + 1) * CHUNK)
        gk_ref[at] = give_k[k].astype(bf16)
        gb_ref[at] = give_b[k].astype(bf16)
        wu_ref[at] = wu[k].astype(bf16)
        pos_ref[at] = jnp.exp(cum[k] - center[k])
        full_ref[at] = jnp.exp(cum[k])

    @pl.when(step == pl.num_programs(0) - 1)
    def _():
        for k in range(agg_ref.shape[0]):
            agg_ref[k] = state.astype(bf16)


def token_specs():
    return [pl.BlockSpec(memory_space=pltpu.VMEM)] * 2


def maps_call(place, same, other, w, spike, vec, copies):
    rows, width = spike.shape
    depth = w.shape[0]
    tile = pl.BlockSpec((MAPS_BLOCK, width), lambda i, p: (i, 0))
    wide = pl.BlockSpec((MAPS_BLOCK, 2 * width), lambda i, p: (i, 0))
    pairs = MAPS_BLOCK // CHUNK
    like = lambda n, t: array((rows, n), t)
    return pl.pallas_call(
        maps_kernel,
        grid_spec=pltpu.PrefetchScalarGridSpec(
            num_scalar_prefetch=1,
            grid=(rows // MAPS_BLOCK,),
            in_specs=token_specs()
            + [
                pl.BlockSpec((depth, 4 * width), lambda i, p: (0, 0)),
                tile,
                pl.BlockSpec(vec.shape, lambda i, p: (0, 0)),
            ],
            out_specs=[
                tile,
                tile,
                wide,
                tile,
                tile,
                tile,
                pl.BlockSpec((pairs, width, width), lambda i, p: (i, 0, 0)),
                pl.BlockSpec((copies, width, width), lambda i, p: (0, 0, 0)),
            ],
            scratch_shapes=[pltpu.VMEM((width, width), f32)],
        ),
        out_shape=[
            like(width, bf16),
            like(width, bf16),
            like(2 * width, bf16),
            like(width, bf16),
            like(width, f32),
            like(width, f32),
            array((rows // CHUNK, width, width), bf16),
            array((copies, width, width), bf16),
        ],
        compiler_params=pltpu.CompilerParams(
            dimension_semantics=("arbitrary",), vmem_limit_bytes=28 * 2**20
        ),
        name="state_maps",
    )(place, same, other, *in_hbm(w, spike), vec)


def conv_kernel(place_ref, same_ref, other_ref, w_ref, halo_ref, vec_ref, q_ref, out_ref, tail_ref):
    width = vec_ref.shape[1]

    def project(x, first, last):
        out = jnp.dot(x, w_ref[:, first * width : last * width], preferred_element_type=f32)
        return out.astype(bf16)

    @pl.when(pl.program_id(0) == 0)
    def _():
        two = project(halo_ref[...], 1, 3).astype(f32)
        tail_ref[...] = two[:, :width] * two[:, width:]

    pairs = CONV_BLOCK // BLOCK
    x = own_block(place_ref, same_ref, other_ref, pl.program_id(0) * pairs, pairs)
    two = project(x, 0, 2)
    q_ref[...] = two[:, :width]
    rest = project(x, 2, 4).astype(f32)
    prod, post = two[:, width:].astype(f32) * rest[:, :width], rest[:, width:]
    rows = prod.shape[0]
    tail = tail_ref[...]
    row = rows_of((rows, width))
    last, before = tail[-1:], tail[-2:-1]
    one = jnp.where(row == 0, last, pltpu.roll(prod, 1, 0))
    two = jnp.where(row == 0, before, jnp.where(row == 1, last, pltpu.roll(prod, 2, 0)))
    filtered = vec_ref[2:3] * two + vec_ref[3:4] * one + vec_ref[4:5] * prod
    out_ref[...] = (post * filtered).astype(bf16)
    tail_ref[...] = prod[rows - tail_ref.shape[0] :]


def conv_call(place, same, other, w, halo, vec):
    rows, width = same.shape[0] * same.shape[1] * 2, vec.shape[1]
    depth = w.shape[0]
    tile = pl.BlockSpec((CONV_BLOCK, width), lambda i, p: (i, 0))
    whole = lambda a: pl.BlockSpec(a.shape, lambda i, p: (0,) * a.ndim)
    return pl.pallas_call(
        conv_kernel,
        grid_spec=pltpu.PrefetchScalarGridSpec(
            num_scalar_prefetch=1,
            grid=(rows // CONV_BLOCK,),
            in_specs=token_specs()
            + [pl.BlockSpec((depth, 4 * width), lambda i, p: (0, 1)), whole(halo), whole(vec)],
            out_specs=[tile, tile],
            scratch_shapes=[pltpu.VMEM((halo.shape[0], width), f32)],
        ),
        out_shape=[array((rows, width), bf16)] * 2,
        compiler_params=pltpu.CompilerParams(
            dimension_semantics=("arbitrary",), vmem_limit_bytes=20 * 2**20
        ),
        name="conv_mix",
    )(place, same, other, *in_hbm(w), halo, vec)


def reads_kernel(q_ref, gk_ref, gb_ref, wu_ref, v_ref, pos_ref, full_ref, states_ref, o_ref, y_ref):
    width = 2 * HEAD_WIDTH
    each = range(READS_BLOCK // CHUNK)
    t, s, _ = chunk_masks()
    inclusive = t >= s
    fold = functools.partial(spread, first=first_lanes())
    q_all = q_ref[...].astype(f32)
    ask, full = cut(q_all * pos_ref[...]), cut(q_all * full_ref[...])
    gk, gb, wu, v = map(cut, (gk_ref[...], gb_ref[...], wu_ref[...], v_ref[...]))
    grams = [dot(ask[k], jnp.concatenate([fold(gk[k]), fold(gb[k])], axis=0), 1, 1) for k in each]
    key_read = [jnp.where(inclusive, g[:, :width], 0.0) for g in grams]
    beta_read = [jnp.where(inclusive, g[:, width:], 0.0) for g in grams]
    forward = [dot(key_read[k], fold(v[k])) for k in each]
    back = [
        dot(beta_read[k], jnp.concatenate([fold(wu[k][:, :width]), fold(wu[k][:, width:])], axis=1))
        for k in each
    ]
    for k in each:
        start = states_ref[k]
        got = dot(
            full[k] - back[k][:, :width],
            jnp.concatenate([fold(start[:HEAD_WIDTH]), fold(start[HEAD_WIDTH:])], axis=0),
            1,
            1,
        )
        at = slice(k * CHUNK, (k + 1) * CHUNK)
        o_ref[at] = forward[k] - back[k][:, width:] + got[:, :width]
        y_ref[at] = got[:, width:].astype(bf16)


def reads_call(q, gk, gb, wu, v, pos, full, states):
    rows, width = q.shape
    tile = pl.BlockSpec((READS_BLOCK, width), lambda i: (i, 0))
    wide = pl.BlockSpec((READS_BLOCK, 2 * width), lambda i: (i, 0))
    starts = pl.BlockSpec((READS_BLOCK // CHUNK, width, width), lambda i: (i, 0, 0))
    return pl.pallas_call(
        reads_kernel,
        grid=(rows // READS_BLOCK,),
        in_specs=[tile, tile, tile, wide, tile, tile, tile, starts],
        out_specs=[tile, tile],
        out_shape=[pltpu.VMEM((rows, width), f32), pltpu.VMEM((rows, width), bf16)],
        compiler_params=pltpu.CompilerParams(
            dimension_semantics=("arbitrary",), vmem_limit_bytes=20 * 2**20
        ),
        name="local_reads",
    )(*in_hbm(q, gk, gb, wu, v, pos, full, states))


def moved(state, piece, first):
    hi = state.astype(bf16)
    lo = (state - hi.astype(f32)).astype(bf16)
    got = dot(jnp.concatenate([hi, lo], axis=0), spread(piece[HEAD_WIDTH:], first))
    return got[: state.shape[0]] + got[state.shape[0] :]


def group_kernel(at_ref, pieces_ref, out_ref, before_ref):
    first = first_lanes()

    def join(total, k):
        piece = pieces_ref[k]
        total = moved(total, piece, first)
        source = total[:HEAD_WIDTH] + piece[:HEAD_WIDTH].astype(f32)
        return jnp.concatenate([source, total[HEAD_WIDTH:]], axis=0)

    total = pieces_ref[0].astype(f32)
    r, l = rows_of(total.shape), lanes_of(total.shape) % HEAD_WIDTH
    before = jnp.where(r - HEAD_WIDTH == l, 1.0, 0.0)
    for k in range(1, pieces_ref.shape[0]):
        before = jnp.where(at_ref[1] == k, total, before)
        total = join(total, k)
    before_ref[...] = before
    for k in range(out_ref.shape[0]):
        out_ref[k] = total.astype(bf16)


def group_call(at, pieces, copies):
    here = pl.BlockSpec(memory_space=pltpu.VMEM)
    return pl.pallas_call(
        group_kernel,
        in_specs=[pl.BlockSpec(memory_space=pltpu.SMEM), here],
        out_specs=[here, here],
        out_shape=[
            jax.ShapeDtypeStruct((copies, *pieces.shape[1:]), bf16),
            jax.ShapeDtypeStruct(pieces.shape[1:], f32),
        ],
        name="group_map",
    )(at, pltpu.with_memory_space_constraint(pieces, pltpu.VMEM))


def finish_kernel(at_ref, before_ref, far_ref, init_ref, o_ref, y_ref, conv_ref, vec_ref, out_ref, s_ref):
    width = 2 * HEAD_WIDTH
    first = first_lanes()

    @pl.when(pl.program_id(0) == 0)
    def _():
        def advance(i, state):
            piece = far_ref[i]
            return moved(state, piece, first) + piece[:HEAD_WIDTH].astype(f32)

        state = lax.fori_loop(0, at_ref[0], advance, init_ref[...])
        before = before_ref[...]
        state = moved(state, before, first) + before[:HEAD_WIDTH]
        s_ref[...] = spread(state, first)

    low = lanes_of((READS_BLOCK, width)) < HEAD_WIDTH
    reads = o_ref[...] + dot(y_ref[...], s_ref[...], 1, 1)
    centered = reads - head_sums(reads, low) * (1.0 / HEAD_WIDTH)
    variance = head_sums(centered * centered, low) * (1.0 / HEAD_WIDTH)
    mixed = centered * lax.rsqrt(variance + HEAD_WIDTH * 1e-05) * vec_ref[5:6]
    out_ref[:, :width] = conv_ref[...]
    out_ref[:, width:] = mixed.astype(bf16)


def finish_call(at, before, far, init, o, y, conv, vec):
    rows, width = o.shape
    whole = lambda a: pl.BlockSpec(a.shape, lambda i, p: (0,) * a.ndim)
    tile = pl.BlockSpec((READS_BLOCK, width), lambda i, p: (i, 0))
    return pl.pallas_call(
        finish_kernel,
        grid_spec=pltpu.PrefetchScalarGridSpec(
            num_scalar_prefetch=1,
            grid=(rows // READS_BLOCK,),
            in_specs=[whole(before), whole(far), whole(init), tile, tile, tile, whole(vec)],
            out_specs=pl.BlockSpec((READS_BLOCK, 2 * width), lambda i, p: (i, 0)),
            scratch_shapes=[pltpu.VMEM((width, width), bf16)],
        ),
        out_shape=array((rows, 2 * width), bf16),
        compiler_params=pltpu.CompilerParams(
            dimension_semantics=("arbitrary",), vmem_limit_bytes=12 * 2**20
        ),
        name="finish_mix",
    )(at, before, far, init, in_vmem(o), in_vmem(y), *in_hbm(conv), vec)


def outward_kernel(pick_ref, m_ref, *refs):
    *weights, keep_ref, give_ref = refs
    rows, columns = keep_ref.shape
    first = pick_ref[0] == 0
    step = 512
    for at in range(0, columns, step):
        total = None
        for k, w_ref in enumerate(weights):
            got = dot(m_ref[pick_ref[1 + k]], w_ref[:, at : at + step])
            total = got if total is None else total + got
        total = total.astype(bf16)
        keep_ref[:, at : at + step] = jnp.where(first, total[:rows], total[rows:])
        give_ref[:, at : at + step] = jnp.where(first, total[rows:], total[:rows])


def outward_call(pick, gathered, weights):
    rows, columns = gathered.shape[1] // 2, weights[0].shape[1]
    here = pl.BlockSpec(memory_space=pltpu.VMEM)
    return pl.pallas_call(
        outward_kernel,
        in_specs=[pl.BlockSpec(memory_space=pltpu.SMEM)] + [here] * (1 + len(weights)),
        out_specs=[here, here],
        out_shape=[jax.ShapeDtypeStruct((rows, columns), bf16)] * 2,
        compiler_params=pltpu.CompilerParams(vmem_limit_bytes=24 * 2**20),
        name="outward",
    )(pick, gathered, *weights)


def pack_kernel(*refs):
    *parts, out_ref = refs
    for k, ref in enumerate(parts):
        width = ref.shape[1]
        for n in range(out_ref.shape[0]):
            out_ref[n, :, k * width : (k + 1) * width] = ref[...]


def packed(copies, *shards):
    rows, width = shards[0].shape
    return pl.pallas_call(
        pack_kernel,
        out_shape=jax.ShapeDtypeStruct((copies, rows, len(shards) * width), bf16),
        name="pack_shards",
    )(*shards)


def passed_along(block, axis, distance):
    devices = range(lax.axis_size(axis))
    route = [(i - distance, i) for i in devices if i - distance in devices]
    return lax.ppermute(block, axis, route)


def turned(x, distance):
    devices = lax.axis_size("tp")
    return lax.ppermute(x, "tp", [(i, (i + distance) % devices) for i in range(devices)])


def from_everyone(copies, axis, groups=None):
    return lax.all_to_all(copies, axis, 0, 0, tiled=True, axis_index_groups=groups)


def rms_rows(activations, gain_vector):
    values = activations.astype(f32)
    inv_scale = lax.rsqrt(jnp.mean(values * values, axis=-1, keepdims=True) + norm_eps)
    return (values * inv_scale * gain_vector).astype(bf16)


def mixing(
    tokens,
    input_norm_gain,
    earlier_gate,
    later_gate,
    convolution_input,
    convolution_taps,
    receptance,
    key_matrix,
    value_matrix,
    decay_matrix,
    rate_matrix,
    decay_floor,
    rate_offset,
    decay_spike,
    initial_state,
    head_norm_gain,
    convolution_output,
    state_heads_output,
):
    channels = earlier_gate.shape[1]
    heads = channels // HEAD_WIDTH
    devices = lax.axis_size("tp")
    chips = devices // 2
    me = lax.axis_index("tp").astype(jnp.int32)
    chip, core = lax.shift_right_logical(me, 1), me & 1

    def core_swap(x):
        return lax.ppermute(x, "tp", [(i, i ^ 1) for i in range(devices)])

    blocks, seqs = lax.axis_size("sp"), lax.axis_size("fs")
    weights = from_everyone(
        packed(
            seqs,
            key_matrix,
            value_matrix,
            decay_matrix,
            rate_matrix,
            receptance,
            earlier_gate,
            convolution_input,
            later_gate,
        ),
        "fs",
    )
    weights = weights.reshape(-1, 8 * channels)
    weights = lax.all_gather(weights, "sp", axis=0, tiled=True)
    outer = from_everyone(packed(blocks, convolution_output.T, state_heads_output.T), "sp")
    outer = from_everyone(jnp.broadcast_to(outer[None], (seqs, *outer.shape)), "fs")
    outer = jnp.swapaxes(outer, 0, 1).reshape(-1, 2 * channels).T

    normed = rms_rows(tokens[0], input_norm_gain)
    opposite = turned(normed, 4)
    ahead, behind = turned(normed, -2), turned(normed, 2)
    same = jnp.stack([normed, ahead, opposite, behind])
    other = core_swap(same)
    across = turned(outer, 4)
    after, before = turned(outer, -2), turned(outer, 2)
    vec = jnp.concatenate(
        [
            decay_floor[None],
            rate_offset[None],
            convolution_taps,
            head_norm_gain[None],
            jnp.zeros((2, channels), f32),
        ],
        axis=0,
    )
    init = jnp.moveaxis(initial_state[0], 0, 1).reshape(HEAD_WIDTH, heads * HEAD_WIDTH)
    vec, init = lax.optimization_barrier((vec, init))
    place = jnp.stack([chip, core])
    last_rows = jnp.where(core == 0, other[:, -HALO:], same[:, -HALO:])
    last_rows = lax.dynamic_index_in_dim(last_rows, (chips - 1 - chip) & (chips - 1), 0, keepdims=False)
    halo = passed_along(last_rows, "sp", 1)
    few = 4
    near_blocks = [list(range(k, k + few)) for k in range(0, blocks, few)]
    far_blocks = [list(range(k, blocks, few)) for k in range(few)]
    *kept, agg = maps_call(place, same, other, weights, decay_spike[0], vec, few)
    near_maps = from_everyone(agg, "sp", near_blocks)
    block = lax.axis_index("sp").astype(jnp.int32)
    at = jnp.stack([lax.shift_right_logical(block, 2), block & (few - 1)])
    total, earlier = group_call(at, near_maps, blocks // few)
    far_maps = from_everyone(total, "sp", far_blocks)
    q, conv = conv_call(place, same, other, weights, halo, vec)
    o, y = reads_call(q, *kept)
    mixed = finish_call(at, earlier, far_maps, init, o, y, conv, vec)
    groups = [list(range(side, devices, 2)) for side in range(2)]
    gathered = lax.all_to_all(
        mixed.reshape(chips, -1, 2 * channels), "tp", 0, 0, tiled=True, axis_index_groups=groups
    )
    near = [(chip + k) & (chips - 1) for k in (0, 1, 2, chips - 1)]
    kept, given = outward_call(jnp.stack([core, *near]), gathered, (outer, after, across, before))
    taken = core_swap(given)
    return (kept.astype(f32) + taken.astype(f32)).astype(bf16)[None]


def solution(mesh):
    placed = (
        P("fs", ("sp", "tp"), None),
        P(),
        P(("sp", "fs"), "tp"),
        P(("sp", "fs"), "tp"),
        P(("sp", "fs"), "tp"),
        P(None, "tp"),
        P(("sp", "fs"), "tp"),
        P(("sp", "fs"), "tp"),
        P(("sp", "fs"), "tp"),
        P(("sp", "fs"), "tp"),
        P(("sp", "fs"), "tp"),
        P("tp"),
        P("tp"),
        P("fs", "sp", "tp"),
        P("fs", "tp", None, None),
        P("tp"),
        P("tp", ("sp", "fs")),
        P("tp", ("sp", "fs")),
    )
    return jax.shard_map(
        mixing,
        mesh=mesh,
        in_specs=placed,
        out_specs=P("fs", ("sp", "tp"), None),
        check_vma=False,
    )
```
